256 devices in a mesh: sp: 16 (over y, x), dp: 16 (over z, core).
Axes of the slice: x: 4, y: 4, z: 8, core: 2. Of those that a mesh axis runs over, the one named last changes fastest.
Arguments:
- value_half: bfloat16 [16, 4096, 2048], P('dp', 'sp'), may hold values from -6 to 6
- gate_half: bfloat16 [16, 4096, 2048], P('dp', 'sp'), may hold values from -6 to 6
- upstream: bfloat16 [16, 4096, 2048], P('dp', 'sp'), may hold values from -6 to 6
- conv_taps: float32 [31, 2048], P(None, 'sp'), may hold values from -1 to 1
- norm_gain: float32 [2048], replicated, may hold values from 0.1 to 1.9
- out_weight: bfloat16 [2048, 2048], P('dp'), may hold values from -0.125 to 0.125
Outputs:
- grad_value: bfloat16 [16, 4096, 2048], P('dp', 'sp')
- grad_gate: bfloat16 [16, 4096, 2048], P('dp', 'sp')
- grad_taps: float32 [31, 2048], P(None, 'sp')
- grad_gain: float32 [2048], replicated
- grad_weight: float32 [2048, 2048], P('dp')
The draws below stay inside these ranges and needn't reach their ends.
All inputs are finite; a program needn't handle non-finite values.
Results may differ from the reference program's by a relative error of at most 0.0062.
Values may be sent and summed in bfloat16 or wider, within the bound.
A program may use at most 128 MiB of HBM per device.

```python
import jax
import jax.numpy as jnp
from jax import lax

D = 2048
KERNEL = 31
LENGTH = 4096
BATCH = 16


def spiked(drawn, rng, source, target, parts, factor):
    owner, partner = [(jnp.arange(drawn.shape[dim]) // (drawn.shape[dim] // parts)).reshape([-1 if axis == dim else 1 for axis in range(drawn.ndim)]) for dim in (source, target)]
    chosen = jax.random.permutation(rng, parts)[partner]
    strong = (owner == chosen) | (owner == (partner + parts // 2) % parts)
    return jnp.where(strong, factor * drawn, drawn)


def block_levels(stream_key, dims, pieces, low, largest):
    level = 1.0
    for axis_at, blocks in pieces:
        draws = jax.random.uniform(jax.random.fold_in(jax.random.fold_in(stream_key, 6), axis_at), (blocks,), jnp.float32, low / len(pieces), largest / len(pieces))
        level = level * jnp.repeat(jnp.exp(draws), dims[axis_at] // blocks).reshape((-1,) + (1,) * (len(dims) - 1 - axis_at))
    return level


def normal_values(own_key, shape, scale, bound, pieces=(), held_as=jnp.bfloat16):
    drawn = scale * jax.random.normal(own_key, shape, jnp.float32)
    if pieces:
        drawn = drawn * block_levels(own_key, shape, pieces, -0.22, 0.18)
    return jnp.clip(drawn, -bound, bound).astype(held_as)


def bell_draw_with(rng, shape, spread, limit, cuts, heavy, dtype=jnp.bfloat16):
    drawn = spread * jax.random.normal(rng, shape, jnp.float32)
    if cuts:
        drawn = drawn * block_levels(rng, shape, cuts, -0.22, 0.18)
    return jnp.clip(spiked(drawn, jax.random.fold_in(rng, 3), *heavy), -limit, limit).astype(dtype)


def setup_inputs(seed: int = 0) -> dict:
    splits = jax.random.split(jax.random.key(seed), 7)
    return {
        "value_half": normal_values(splits[0], (BATCH, LENGTH, D), 1.0, 6.0, ((0, 16), (1, 16))),
        "gate_half": normal_values(splits[1], (BATCH, LENGTH, D), 1.0, 6.0, ((0, 16), (1, 16))),
        "upstream": bell_draw_with(splits[2], (BATCH, LENGTH, D), 1.0, 6.0, ((0, 16), (1, 16)), (0, 2, 16, 2.0)),
        "conv_taps": normal_values(splits[3], (KERNEL, D), 0.18, 1.0, ((1, 16),), jnp.float32),
        "norm_gain": jnp.clip(1.0 + 0.18 * jax.random.normal(splits[4], (D,), jnp.float32), 0.1, 1.9),
        "out_weight": normal_values(splits[5], (D, D), D ** -0.5, 0.125, ((0, 16),)),
    }


NORM_EPS = 1e-05

def one_sequence(sequence, conv_taps, norm_gain, out_weight):
    value_half, gate_half, upstream = sequence
    tap_count = conv_taps.shape[0]
    length = value_half.shape[0]
    sig_gate = jax.nn.sigmoid(gate_half.astype(jnp.float32))
    value_wide = value_half.astype(jnp.float32)
    glu = (value_wide * sig_gate).astype(jnp.bfloat16)
    glu_wide = lax.optimization_barrier(glu).astype(jnp.float32)
    padded = jnp.pad(glu_wide, ((tap_count - 1, 0), (0, 0)))
    conv_out = jnp.zeros_like(glu_wide)
    for offset in range(tap_count):
        conv_out = conv_out + conv_taps[offset] * padded[offset:offset + length]
    conv_out = lax.optimization_barrier(conv_out.astype(jnp.bfloat16)).astype(jnp.float32)
    row_mean = lax.optimization_barrier(jnp.mean(conv_out, axis=-1, keepdims=True))
    centered = conv_out - row_mean
    inv_scale = lax.rsqrt(lax.optimization_barrier(jnp.mean(centered * centered, axis=-1, keepdims=True)) + NORM_EPS)
    normed = centered * inv_scale
    scaled = normed * norm_gain
    sig_scaled = jax.nn.sigmoid(scaled)
    activated = (scaled * sig_scaled).astype(jnp.bfloat16)
    grad_act = jnp.dot(upstream, out_weight, preferred_element_type=jnp.float32)
    grad_scaled = grad_act * sig_scaled * (1.0 + scaled * (1.0 - sig_scaled))
    gain_term = lax.optimization_barrier(jnp.sum(grad_scaled * normed, axis=0))
    grad_normed = grad_scaled * norm_gain
    grad_conv_out = inv_scale * (grad_normed - lax.optimization_barrier(jnp.mean(grad_normed, axis=-1, keepdims=True)) - normed * lax.optimization_barrier(jnp.mean(grad_normed * normed, axis=-1, keepdims=True)))
    grad_conv_out = lax.optimization_barrier(grad_conv_out.astype(jnp.bfloat16)).astype(jnp.float32)
    grad_padded = jnp.pad(grad_conv_out, ((0, tap_count - 1), (0, 0)))
    grad_glu = jnp.zeros_like(grad_conv_out)
    tap_terms = []
    for offset in range(tap_count):
        first = tap_count - 1 - offset
        grad_glu = grad_glu + conv_taps[offset] * grad_padded[first:first + length]
        tap_terms.append(lax.optimization_barrier(jnp.sum(grad_conv_out * padded[offset:offset + length], axis=0)))
    grad_glu = lax.optimization_barrier(grad_glu.astype(jnp.bfloat16)).astype(jnp.float32)
    grad_value = (grad_glu * sig_gate).astype(jnp.bfloat16)
    grad_gate = (grad_glu * value_wide * sig_gate * (1.0 - sig_gate)).astype(jnp.bfloat16)
    return (grad_value, grad_gate, activated, jnp.stack(tap_terms), gain_term)

def reference(value_half, gate_half, upstream, conv_taps, norm_gain, out_weight):

    def mapped(sequence):
        return one_sequence(sequence, conv_taps, norm_gain, out_weight)
    grad_value, grad_gate, activated, tap_terms, gain_terms = lax.map(mapped, (value_half, gate_half, upstream))
    model_width = value_half.shape[2]
    grad_weight = lax.dot_general(upstream.reshape(-1, model_width), activated.reshape(-1, model_width), (((0,), (0,)), ((), ())), preferred_element_type=jnp.float32)
    grad_taps = lax.optimization_barrier(jnp.sum(tap_terms, axis=0))
    grad_gain = lax.optimization_barrier(jnp.sum(gain_terms, axis=0))
    return (grad_value, grad_gate, grad_taps, grad_gain, grad_weight)
```

```python
import functools

import jax
import jax.numpy as jnp
from jax import lax
from jax.experimental import pallas as pl
from jax.experimental.pallas import tpu as pltpu
from jax.sharding import Mesh
from jax.sharding import PartitionSpec as P

DP = ("dp_0", "dp_1")
SP = ("sp_0", "sp_1")
NORM_EPS = 1e-05
MESH = pl.DeviceIdType.MESH
F32 = jnp.float32
BF16 = jnp.bfloat16

TOK = 256
CH = 2048
NC = CH // 128
TAPS = 31
NZ = 8
ORDER = (4, 3, 5, 2, 6, 1, 7, 0)
STAGES = ((0, 4), (4, 8))
N_SEND = 220


def kernel(
    v_hbm, g_hbm, u_hbm, w_hbm, taps_ref, gain_ref,
    gg_ref, gw_ref, dt_ref, dn_ref,
    v_s, g_s, u_s, usib, wbuf, tapsb, glu, conv, act, actsib, ut,
    pbuf, r1, r2, q, s1, s2, vz, rz, fg, gacc, gpad, mean_s, inv_s,
    halo_out, halo_in, ghalo_out, ghalo_in, dn, tg, tr, tz, tsib, tfin, gfull,
    local_sem, send_sem, recv_sem,
):
    cy, cx, cz, cc = (lax.axis_index(a) for a in ("sp_0", "sp_1", "dp_0", "dp_1"))
    sp = cy * 4 + cx
    other = 1 - cc
    sibling = {"dp_1": other}

    def zdev(d):
        return {"dp_0": lax.rem(cz + d + NZ, NZ)}

    def spdev(d):
        s = lax.rem(sp + d + 16, 16)
        return {"sp_0": s // 4, "sp_1": lax.rem(s, 4)}

    used = [0]
    started = []

    def send(src, dst, device):
        i = used[0]
        used[0] += 1
        copy = pltpu.make_async_remote_copy(
            src_ref=src, dst_ref=dst, send_sem=send_sem.at[i], recv_sem=recv_sem.at[i],
            device_id=device, device_id_type=MESH,
        )
        copy.start()
        started.append(copy)
        return copy

    loads = [
        pltpu.make_async_copy(w_hbm, wbuf.at[0, cc], local_sem.at[0]),
        pltpu.make_async_copy(v_hbm.at[0], v_s, local_sem.at[1]),
        pltpu.make_async_copy(g_hbm.at[0], g_s, local_sem.at[2]),
        pltpu.make_async_copy(u_hbm.at[0], u_s, local_sem.at[3]),
    ]
    for load in loads:
        load.start()

    barrier = pltpu.get_barrier_semaphore()
    pl.semaphore_signal(barrier, inc=1, device_id=sibling, device_id_type=MESH)
    for d in range(1, NZ):
        pl.semaphore_signal(barrier, inc=1, device_id=zdev(d), device_id_type=MESH)
    for d in range(1, 16):
        pl.semaphore_signal(barrier, inc=1, device_id=spdev(d), device_id_type=MESH)

    tapsb[sp, :TAPS] = taps_ref[...]
    tapsb[sp, TAPS:] = jnp.zeros((1, 128), F32)
    loads[0].wait()
    pl.semaphore_wait(barrier, 23)

    w_copies = {}

    def w_send(step, sub):
        rows = pl.ds(64 * sub, 64)
        lanes = (slice(0, 1024), slice(1024, 2048)) if step == 4 else (slice(None), slice(None))
        for way, sign in ((0, 1), (1, -1)):
            src = (-sign * (step - 1)) % NZ
            dst = (-sign * step) % NZ
            w_copies[step, sub, way] = send(
                wbuf.at[src, cc, rows, lanes[way]], wbuf.at[dst, cc, rows, lanes[way]], zdev(sign)
            )

    w_pair = {}

    def w_share(rel, sub):
        rows = pl.ds(64 * sub, 64)
        w_pair[rel, sub] = send(wbuf.at[rel, cc, rows], wbuf.at[rel, cc, rows], sibling)

    def w_event(step, sub):
        for way in (0, 1):
            w_copies[step, sub, way].wait_recv()
        if step < 4:
            w_send(step + 1, sub)
        for rel in sorted({step, (-step) % NZ}):
            w_share(rel, sub)

    w_send(1, 0)
    w_send(1, 1)
    taps_copies = [send(tapsb.at[sp], tapsb.at[sp], spdev(d)) for d in range(1, 16)]
    for load in loads[1:]:
        load.wait()
    u_copy = send(u_s, usib, sibling)
    w_share(0, 0)
    w_share(0, 1)

    def glu_rows(r):
        rows = pl.ds(r, 32)
        for c in range(NC):
            lanes = slice(128 * c, 128 * c + 128)
            wide = v_s[rows, lanes].astype(F32) * jax.nn.sigmoid(g_s[rows, lanes].astype(F32))
            narrow = wide.astype(BF16)
            glu[c, pl.ds(r + 32, 32), :] = narrow.astype(F32)
            yield lanes, narrow

    for lanes, narrow in glu_rows(TOK - 32):
        halo_out[:, lanes] = narrow
    halo_copy = send(halo_out, halo_in, spdev(1))

    def glu_step(i, carry):
        for _ in glu_rows(pl.multiple_of(i * 32, 32)):
            pass
        return carry

    lax.fori_loop(0, TOK // 32 - 1, glu_step, 0)

    u_copy.wait_recv()

    def transpose_step(k, carry):
        zb = lax.rem(cz + k, NZ)
        cols = pl.ds(pl.multiple_of(zb * 256 + cc * 128, 128), 128)
        ut[k, :, 0:256] = u_s[:, cols].T
        ut[k, :, 256:512] = usib[:, cols].T
        return carry

    lax.fori_loop(0, NZ, transpose_step, 0)

    for copy in taps_copies:
        copy.wait_recv()
    halo_copy.wait_recv()
    keep = (sp > 0).astype(F32)
    for c in range(NC):
        glu[c, 0:32, :] = halo_in[:, 128 * c : 128 * c + 128].astype(F32) * keep

    mean_s[...] = jnp.zeros_like(mean_s)

    def conv_chunk(c, carry):
        taps = [jnp.broadcast_to(tapsb[c, j : j + 1, :], (8, 128)) for j in range(TAPS)]

        def rows_step(i, carry):
            for k in range(4):
                r = pl.multiple_of(i * 32, 32) + 8 * k
                parts = [None] * 4
                for j in range(TAPS):
                    term = taps[j] * glu[c, pl.ds(r + 2 + j, 8), :]
                    parts[j % 4] = term if parts[j % 4] is None else parts[j % 4] + term
                total = (parts[0] + parts[1]) + (parts[2] + parts[3])
                total = total.astype(BF16).astype(F32)
                conv[c, pl.ds(r, 8), :] = total
                mean_s[pl.ds(r, 8), :] += total
            return carry

        return lax.fori_loop(0, TOK // 32, rows_step, carry)

    lax.fori_loop(0, 8, conv_chunk, 0)
    w_event(1, 0)
    lax.fori_loop(8, NC, conv_chunk, 0)

    def norm_step(i, carry):
        rows = pl.ds(pl.multiple_of(i * 32, 32), 32)
        mu = jnp.broadcast_to(jnp.sum(mean_s[rows, :], axis=1, keepdims=True) * (1.0 / CH), (32, 128))
        squares = jnp.zeros((32, 128), F32)
        for c in range(NC):
            centered = conv[c, rows, :] - mu
            squares = squares + centered * centered
        inv = lax.rsqrt(jnp.sum(squares, axis=1, keepdims=True) * (1.0 / CH) + NORM_EPS)
        inv = jnp.broadcast_to(inv, (32, 128))
        mean_s[rows, :] = mu
        inv_s[rows, :] = inv
        for c in range(NC):
            lanes = slice(128 * c, 128 * c + 128)
            scaled = (conv[c, rows, :] - mu) * inv * gain_ref[:, lanes]
            act[rows, lanes] = (scaled * jax.nn.sigmoid(scaled)).astype(BF16)
        return carry

    lax.fori_loop(0, 4, norm_step, 0)
    act_copies = [send(act.at[0:128], actsib.at[0:128], sibling)]
    lax.fori_loop(4, 8, norm_step, 0)
    act_copies.append(send(act.at[128:256], actsib.at[128:256], sibling))
    w_event(1, 1)
    for copy in act_copies:
        copy.wait_recv()

    axes = ((("sp_1", cx), ("sp_0", cy)), (("sp_0", cy), ("sp_1", cx)))

    def near(axis, d):
        name, at = axis
        return {name: lax.rem(at + d + 4, 4)}

    def part(axis, d):
        return lax.rem(axis[1] + d + 4, 4)

    def partial_sums(stage):
        for k in range(*STAGES[stage]):
            lhs = ut[ORDER[k]]
            for n in range(4):
                lanes = slice(512 * n, 512 * n + 512)
                total = jnp.dot(lhs[:, 0:256], act[:, lanes], preferred_element_type=F32)
                total = total + jnp.dot(lhs[:, 256:512], actsib[:, lanes], preferred_element_type=F32)
                narrow = total.astype(BF16)
                for h in range(2):
                    for p in range(4):
                        first = 64 * h + 16 * p
                        pbuf[h, p, k, :, lanes] = narrow[first : first + 16, :]

    rs_copies = {}

    def rs1_send(stage):
        zs = pl.ds(STAGES[stage][0], STAGES[stage][1] - STAGES[stage][0])
        for h in range(2):
            axis = axes[h][0]
            far = part(axis, 2)
            for way, sign, lanes in ((0, 1, slice(0, 1024)), (1, -1, slice(1024, 2048))):
                rs_copies[1, stage, h, way] = send(
                    pbuf.at[h, far, zs, :, lanes], r1.at[h, way, zs], near(axis, sign)
                )

    def rs1_mid(stage):
        zs = pl.ds(STAGES[stage][0], STAGES[stage][1] - STAGES[stage][0])
        for h in range(2):
            axis = axes[h][0]
            for way, sign, lanes in ((0, 1, slice(0, 1024)), (1, -1, slice(1024, 2048))):
                rs_copies[1, stage, h, way].wait_recv()
                to = part(axis, sign)

                def add(k, carry, h=h, to=to, way=way, lanes=lanes):
                    pbuf[h, to, k, :, lanes] = (
                        pbuf[h, to, k, :, lanes].astype(F32) + r1[h, way, k].astype(F32)
                    ).astype(BF16)
                    return carry

                lax.fori_loop(*STAGES[stage], add, 0)
                rs_copies[2, stage, h, way] = send(pbuf.at[h, to, zs], r2.at[h, way, zs], near(axis, sign))

    def rs1_fin(stage):
        zs = pl.ds(STAGES[stage][0], STAGES[stage][1] - STAGES[stage][0])
        for h in range(2):
            mine = part(axes[h][0], 0)
            axis = axes[h][1]
            for way in (0, 1):
                rs_copies[2, stage, h, way].wait_recv()

            def add(k, carry, h=h, mine=mine):
                for p in range(4):
                    lanes = slice(512 * p, 512 * p + 512)
                    q[h, p, k] = (
                        pbuf[h, mine, k, :, lanes].astype(F32)
                        + r2[h, 0, k, :, lanes].astype(F32)
                        + r2[h, 1, k, :, lanes].astype(F32)
                    ).astype(BF16)
                return carry

            lax.fori_loop(*STAGES[stage], add, 0)
            far = part(axis, 2)
            for way, sign, lanes in ((0, 1, slice(0, 256)), (1, -1, slice(256, 512))):
                rs_copies[3, stage, h, way] = send(
                    q.at[h, far, zs, :, lanes], s1.at[h, way, zs], near(axis, sign)
                )

    def rs2_mid(stage):
        zs = pl.ds(STAGES[stage][0], STAGES[stage][1] - STAGES[stage][0])
        for h in range(2):
            axis = axes[h][1]
            for way, sign, lanes in ((0, 1, slice(0, 256)), (1, -1, slice(256, 512))):
                rs_copies[3, stage, h, way].wait_recv()
                to = part(axis, sign)
                for k in range(*STAGES[stage]):
                    q[h, to, k, :, lanes] = (
                        q[h, to, k, :, lanes].astype(F32) + s1[h, way, k].astype(F32)
                    ).astype(BF16)
                rs_copies[4, stage, h, way] = send(q.at[h, to, zs], s2.at[h, way, zs], near(axis, sign))

    z_copies = {}

    def rs2_fin(stage):
        for h in range(2):
            mine = part(axes[h][1], 0)
            for way in (0, 1):
                rs_copies[4, stage, h, way].wait_recv()
            for k in range(*STAGES[stage]):
                vz[k, h] = (
                    q[h, mine, k].astype(F32) + s2[h, 0, k].astype(F32) + s2[h, 1, k].astype(F32)
                ).astype(BF16)
        for k in range(*STAGES[stage]):
            if ORDER[k]:
                z_copies[k] = send(vz.at[k], rz.at[k], zdev(ORDER[k]))

    gather_copies = []

    def rs3():
        total = vz[ORDER.index(0)].astype(F32)
        for k in range(NZ):
            if ORDER[k]:
                z_copies[k].wait_recv()
                total = total + rz[k].astype(F32)
        fg[sp] = total.astype(BF16)
        for d in range(1, 16):
            gather_copies.append(send(fg.at[sp], fg.at[sp], spdev(d)))

    def grad_block(rels, first=False):
        for rel in rels:
            for sub in (0, 1):
                w_pair[rel, sub].wait_recv()
        lhs = []
        for rel in rels:
            zb = lax.rem(cz + rel, NZ)
            lhs.append(u_s[:, pl.ds(pl.multiple_of(zb * 256, 256), 256)])

        def step(n, carry):
            lanes = pl.ds(pl.multiple_of(n * 512, 512), 512)
            total = None
            for left, rel in zip(lhs, rels):
                right = wbuf[rel, :, :, lanes].reshape(256, 512)
                term = jnp.dot(left, right, preferred_element_type=F32)
                total = term if total is None else total + term
            if first:
                gacc[:, lanes] = total
            else:
                gacc[:, lanes] += total
            return carry

        lax.fori_loop(0, 4, step, 0)

    partial_sums(0)
    rs1_send(0)
    partial_sums(1)
    rs1_send(1)
    w_event(2, 0)
    rs1_mid(0)
    grad_block((0, 1, 7), first=True)
    rs1_mid(1)
    w_event(2, 1)
    rs1_fin(0)
    w_event(3, 0)
    rs2_mid(0)
    rs1_fin(1)
    grad_block((2, 6))
    rs2_fin(0)
    w_event(3, 1)
    rs2_mid(1)
    grad_block((3, 5))
    w_event(4, 0)
    rs2_fin(1)
    w_event(4, 1)
    grad_block((4,))

    dn[...] = jnp.zeros_like(dn)

    def back_rows(r):
        rows = pl.ds(r, 32)
        mu = mean_s[rows, :]
        inv = inv_s[rows, :]
        sum1 = jnp.zeros((32, 128), F32)
        sum2 = jnp.zeros((32, 128), F32)
        for c in range(NC):
            lanes = slice(128 * c, 128 * c + 128)
            gain = gain_ref[:, lanes]
            normed = (conv[c, rows, :] - mu) * inv
            scaled = normed * gain
            sig = jax.nn.sigmoid(scaled)
            grad_scaled = gacc[rows, lanes] * sig * (1.0 + scaled * (1.0 - sig))
            gain_term = grad_scaled * normed
            dn[c] += (gain_term[0:8] + gain_term[8:16]) + (gain_term[16:24] + gain_term[24:32])
            grad_normed = grad_scaled * gain
            gacc[rows, lanes] = grad_normed
            sum1 = sum1 + grad_normed
            sum2 = sum2 + grad_normed * normed
        m1 = jnp.broadcast_to(jnp.sum(sum1, axis=1, keepdims=True) * (1.0 / CH), (32, 128))
        m2 = jnp.broadcast_to(jnp.sum(sum2, axis=1, keepdims=True) * (1.0 / CH), (32, 128))
        for c in range(NC):
            lanes = slice(128 * c, 128 * c + 128)
            normed = (conv[c, rows, :] - mu) * inv
            narrow = (inv * (gacc[rows, lanes] - m1 - normed * m2)).astype(BF16)
            gpad[c, rows, :] = narrow.astype(F32)
            yield lanes, narrow

    for lanes, narrow in back_rows(0):
        ghalo_out[:, lanes] = narrow
    ghalo_copy = send(ghalo_out, ghalo_in, spdev(-1))

    def back_step(i, carry):
        for _ in back_rows(pl.multiple_of(i * 32, 32)):
            pass
        return carry

    lax.fori_loop(1, TOK // 32, back_step, 0)

    def taps_chunk(c, carry):
        def rows_step(i, sums):
            r = pl.multiple_of(i * 8, 8)
            g = gpad[c, pl.ds(r, 8), :]
            return tuple(sums[j] + g * glu[c, pl.ds(r + 2 + j, 8), :] for j in range(TAPS))

        sums = lax.fori_loop(0, TOK // 8, rows_step, tuple(jnp.zeros((8, 128), F32) for _ in range(TAPS)))
        for j in range(TAPS):
            tg[c, j : j + 1, :] = jnp.sum(sums[j], axis=0, keepdims=True)
        tg[c, TAPS:, :] = jnp.sum(dn[c], axis=0, keepdims=True)
        return carry

    lax.fori_loop(0, NC, taps_chunk, 0)
    part_copies = [send(tg.at[lax.rem(sp + d, 16)], tr.at[d], spdev(d)) for d in range(1, 16)]

    rs3()

    ghalo_copy.wait_recv()
    keep_g = (sp < 15).astype(F32)
    for c in range(NC):
        gpad[c, TOK:, :] = ghalo_in[:, 128 * c : 128 * c + 128].astype(F32) * keep_g

    def grad_chunk(c, carry):
        taps = [jnp.broadcast_to(tapsb[c, j : j + 1, :], (8, 128)) for j in range(TAPS)]
        lanes = pl.ds(pl.multiple_of(c * 128, 128), 128)

        def rows_step(i, carry):
            base = pl.multiple_of(i * 32, 32)
            tiles = []
            for k in range(4):
                r = base + 8 * k
                parts = [None] * 4
                for j in range(TAPS):
                    term = taps[j] * gpad[c, pl.ds(r + 30 - j, 8), :]
                    parts[j % 4] = term if parts[j % 4] is None else parts[j % 4] + term
                tiles.append((parts[0] + parts[1]) + (parts[2] + parts[3]))
            gg_ref[pl.ds(base, 32), lanes] = jnp.concatenate(tiles, axis=0).astype(BF16)
            return carry

        return lax.fori_loop(0, TOK // 32, rows_step, carry)

    lax.fori_loop(0, 8, grad_chunk, 0)

    total = tg[sp]
    for d in range(1, 16):
        part_copies[d - 1].wait_recv()
        total = total + tr[d]
    tz[cz] = total
    tz_copies = [send(tz.at[cz], tz.at[cz], zdev(d)) for d in range(1, NZ)]

    lax.fori_loop(8, NC, grad_chunk, 0)

    for copy in tz_copies:
        copy.wait_recv()
    total = tz[0]
    for k in range(1, NZ):
        total = total + tz[k]
    tfin[...] = total
    pair_copy = send(tfin, tsib, sibling)
    pair_copy.wait_recv()
    total = tfin[...] + tsib[...]
    dt_ref[...] = total
    gfull[sp] = jnp.broadcast_to(total[TAPS:, :], (8, 128))
    gain_copies = [send(gfull.at[sp], gfull.at[sp], spdev(d)) for d in range(1, 16)]

    for copy in gather_copies:
        copy.wait_recv()
    for s in range(16):
        y, x = divmod(s, 4)
        gw_ref[16 * x : 16 * x + 16, 512 * y : 512 * y + 512] = fg[s, 0]
        gw_ref[64 + 16 * y : 80 + 16 * y, 512 * x : 512 * x + 512] = fg[s, 1]
    for copy in gain_copies:
        copy.wait_recv()
    dn_ref[...] = gfull[...]
    for copy in started:
        copy.wait_send()


def body(value_half, gate_half, upstream, conv_taps, norm_gain, out_weight):
    vmem = pl.BlockSpec(memory_space=pltpu.VMEM)
    hbm = pl.BlockSpec(memory_space=pl.ANY)
    grad_glu, grad_rows, taps, gain = pl.pallas_call(
        kernel,
        out_shape=(
            jax.ShapeDtypeStruct((TOK, CH), BF16),
            jax.ShapeDtypeStruct((128, CH), BF16),
            jax.ShapeDtypeStruct((32, 128), F32),
            jax.ShapeDtypeStruct((16, 8, 128), F32),
        ),
        in_specs=[hbm] * 4 + [vmem] * 2,
        out_specs=[vmem] * 4,
        scratch_shapes=[
            pltpu.VMEM((TOK, CH), BF16),
            pltpu.VMEM((TOK, CH), BF16),
            pltpu.VMEM((TOK, CH), BF16),
            pltpu.VMEM((TOK, CH), BF16),
            pltpu.VMEM((NZ, 2, 128, CH), BF16),
            pltpu.VMEM((NC, 32, 128), F32),
            pltpu.VMEM((NC, TOK + 32, 128), F32),
            pltpu.VMEM((NC, TOK, 128), F32),
            pltpu.VMEM((TOK, CH), BF16),
            pltpu.VMEM((TOK, CH), BF16),
            pltpu.VMEM((NZ, 128, 512), BF16),
            pltpu.VMEM((2, 4, NZ, 16, CH), BF16),
            pltpu.VMEM((2, 2, NZ, 16, 1024), BF16),
            pltpu.VMEM((2, 2, NZ, 16, 2048), BF16),
            pltpu.VMEM((2, 4, NZ, 16, 512), BF16),
            pltpu.VMEM((2, 2, NZ, 16, 256), BF16),
            pltpu.VMEM((2, 2, NZ, 16, 512), BF16),
            pltpu.VMEM((NZ, 2, 16, 512), BF16),
            pltpu.VMEM((NZ, 2, 16, 512), BF16),
            pltpu.VMEM((16, 2, 16, 512), BF16),
            pltpu.VMEM((TOK, CH), F32),
            pltpu.VMEM((NC, TOK + 32, 128), F32),
            pltpu.VMEM((TOK, 128), F32),
            pltpu.VMEM((TOK, 128), F32),
            pltpu.VMEM((32, CH), BF16),
            pltpu.VMEM((32, CH), BF16),
            pltpu.VMEM((32, CH), BF16),
            pltpu.VMEM((32, CH), BF16),
            pltpu.VMEM((NC, 8, 128), F32),
            pltpu.VMEM((NC, 32, 128), F32),
            pltpu.VMEM((16, 32, 128), F32),
            pltpu.VMEM((NZ, 32, 128), F32),
            pltpu.VMEM((32, 128), F32),
            pltpu.VMEM((32, 128), F32),
            pltpu.VMEM((16, 8, 128), F32),
            pltpu.SemaphoreType.DMA((4,)),
            pltpu.SemaphoreType.DMA((N_SEND,)),
            pltpu.SemaphoreType.DMA((N_SEND,)),
        ],
        compiler_params=pltpu.CompilerParams(
            collective_id=0, has_side_effects=True, vmem_limit_bytes=66_000_000
        ),
    )(value_half, gate_half, upstream, out_weight, conv_taps, norm_gain[None])
    sig_gate = jax.nn.sigmoid(gate_half.astype(F32))
    wide = grad_glu.astype(F32)[None]
    grad_value = (wide * sig_gate).astype(BF16)
    grad_gate = (wide * value_half.astype(F32) * sig_gate * (1.0 - sig_gate)).astype(BF16)
    return grad_value, grad_gate, taps[:TAPS], gain[:, 0, :].reshape(CH), grad_rows.astype(F32)


def solution(mesh):
    torus = Mesh(mesh.devices.reshape(4, 4, 8, 2), ("sp_0", "sp_1", "dp_0", "dp_1"))
    placed = (P(DP, SP, None), P(DP, SP, None), P(DP, SP, None), P(None, SP), P(), P(DP, None))
    return jax.shard_map(
        body,
        mesh=torus,
        in_specs=placed,
        out_specs=(P(DP, SP, None), P(DP, SP, None), P(None, SP), P(), P(DP, None)),
        check_vma=False,
    )
```

```python
import functools

import jax
import jax.numpy as jnp
from jax import lax
from jax.experimental import pallas as pl
from jax.experimental.pallas import tpu as pltpu
from jax.sharding import Mesh
from jax.sharding import PartitionSpec as P

DP = ("dp_0", "dp_1")
SP = ("sp_0", "sp_1")
NORM_EPS = 1e-05
MESH = pl.DeviceIdType.MESH
F32 = jnp.float32
BF16 = jnp.bfloat16

TOK = 256
CH = 2048
NC = CH // 128
TAPS = 31
NZ = 8
N_SEND = 220


def kernel(
    v_hbm, g_hbm, u_hbm, w_hbm, taps_ref, gain_ref,
    gv_hbm, gt_hbm, gw_ref, dt_ref, dn_ref,
    v_s, g_s, u_s, usib, wbuf, tapsb, glu, conv, act, actsib, ut,
    pbuf, r1, r2, q, s1, s2, vz, rz, fg, gacc, gpad, mean_s, inv_s, gate_a, gate_b, gv_s, gt_s,
    halo_out, halo_in, ghalo_out, ghalo_in, dn, tg, tr, tz, tsib, tfin, gfull,
    local_sem, send_sem, recv_sem,
):
    cy, cx, cz, cc = (lax.axis_index(a) for a in ("sp_0", "sp_1", "dp_0", "dp_1"))
    sp = cy * 4 + cx
    other = 1 - cc
    sibling = {"dp_1": other}

    def zdev(d):
        return {"dp_0": lax.rem(cz + d + NZ, NZ)}

    def spdev(d):
        s = lax.rem(sp + d + 16, 16)
        return {"sp_0": s // 4, "sp_1": lax.rem(s, 4)}

    used = [0]
    started = []

    def send(src, dst, device):
        i = used[0]
        used[0] += 1
        copy = pltpu.make_async_remote_copy(
            src_ref=src, dst_ref=dst, send_sem=send_sem.at[i], recv_sem=recv_sem.at[i],
            device_id=device, device_id_type=MESH,
        )
        copy.start()
        started.append(copy)
        return copy

    loads = [
        pltpu.make_async_copy(w_hbm, wbuf.at[0, cc], local_sem.at[0]),
        pltpu.make_async_copy(v_hbm.at[0], v_s, local_sem.at[1]),
        pltpu.make_async_copy(g_hbm.at[0], g_s, local_sem.at[2]),
        pltpu.make_async_copy(u_hbm.at[0], u_s, local_sem.at[3]),
    ]
    for load in loads:
        load.start()

    barrier = pltpu.get_barrier_semaphore()
    pl.semaphore_signal(barrier, inc=1, device_id=sibling, device_id_type=MESH)
    for d in range(1, NZ):
        pl.semaphore_signal(barrier, inc=1, device_id=zdev(d), device_id_type=MESH)
    for d in range(1, 16):
        pl.semaphore_signal(barrier, inc=1, device_id=spdev(d), device_id_type=MESH)

    tapsb[sp, :TAPS] = taps_ref[...]
    tapsb[sp, TAPS:] = jnp.zeros((1, 128), F32)
    loads[0].wait()
    pl.semaphore_wait(barrier, 23)

    parity = lax.rem(cy + cx, 2)
    w_copies = {}
    w_quarters = {}
    w_pair = {}

    def w_send(step, sub):
        rows = pl.ds(pl.multiple_of(64 * parity + 32 * sub, 32), 32)
        lanes = (slice(0, 1024), slice(1024, 2048)) if step == 4 else (slice(None), slice(None))
        for way, sign in ((0, 1), (1, -1)):
            src = (-sign * (step - 1)) % NZ
            dst = (-sign * step) % NZ
            w_copies[step, sub, way] = send(
                wbuf.at[src, cc, rows, lanes[way]], wbuf.at[dst, cc, rows, lanes[way]], zdev(sign)
            )

    def w_share(rel):
        if rel:
            for turn in range(4):
                w_quarters[rel, turn].wait_recv()
        w_pair[rel] = send(wbuf.at[rel, cc], wbuf.at[rel, cc], sibling)

    def w_event(step, sub):
        for way in (0, 1):
            w_copies[step, sub, way].wait_recv()
        if step < 4:
            w_send(step + 1, sub)
        name, at = (("sp_1", cx), ("sp_0", cy))[sub]
        for rel in sorted({step, (-step) % NZ}):
            for turn, sign in ((2 * sub, 1), (2 * sub + 1, -1)):
                rows = pl.ds(pl.multiple_of(64 * parity + 16 * turn, 16), 16)
                w_quarters[rel, turn] = send(
                    wbuf.at[rel, cc, rows], wbuf.at[rel, cc, rows], {name: lax.rem(at + sign + 4, 4)}
                )

    taps_copies = [send(tapsb.at[sp], tapsb.at[sp], spdev(d)) for d in range(1, 16)]
    w_send(1, 0)
    w_send(1, 1)
    for load in loads[1:]:
        load.wait()
    u_copy = send(u_s, usib, sibling)
    w_share(0)

    def glu_rows(r):
        rows = pl.ds(r, 32)
        for c in range(NC):
            lanes = slice(128 * c, 128 * c + 128)
            value = v_s[rows, lanes].astype(F32)
            sig = jax.nn.sigmoid(g_s[rows, lanes].astype(F32))
            wide = value * sig
            gate_a[c, rows, :] = sig
            gate_b[c, rows, :] = wide * (1.0 - sig)
            narrow = wide.astype(BF16)
            glu[c, pl.ds(r + 32, 32), :] = narrow.astype(F32)
            yield lanes, narrow

    for lanes, narrow in glu_rows(TOK - 32):
        halo_out[:, lanes] = narrow
    halo_copy = send(halo_out, halo_in, spdev(1))

    def glu_step(i, carry):
        for _ in glu_rows(pl.multiple_of(i * 32, 32)):
            pass
        return carry

    lax.fori_loop(0, TOK // 32 - 1, glu_step, 0)

    for copy in taps_copies:
        copy.wait_recv()

    mean_s[...] = jnp.zeros_like(mean_s)

    def conv_chunk(first, last, c, carry):
        taps = [jnp.broadcast_to(tapsb[c, j : j + 1, :], (8, 128)) for j in range(TAPS)]

        def rows_step(i, carry):
            for k in range(8):
                r = pl.multiple_of(i * 64, 64) + 8 * k
                parts = [None] * 2
                for j in range(TAPS):
                    term = taps[j] * glu[c, pl.ds(r + 2 + j, 8), :]
                    parts[j % 2] = term if parts[j % 2] is None else parts[j % 2] + term
                total = (parts[0] + parts[1]).astype(BF16).astype(F32)
                conv[c, pl.ds(r, 8), :] = total
                mean_s[pl.ds(r, 8), :] += total
            return carry

        return lax.fori_loop(first, last, rows_step, carry)

    body_rows = functools.partial(conv_chunk, 1, TOK // 64)
    w_event(1, 0)
    lax.fori_loop(0, 8, body_rows, 0)
    w_event(1, 1)
    lax.fori_loop(8, NC, body_rows, 0)
    w_event(2, 0)
    halo_copy.wait_recv()
    keep = (sp > 0).astype(F32)
    for c in range(NC):
        glu[c, 0:32, :] = halo_in[:, 128 * c : 128 * c + 128].astype(F32) * keep
    lax.fori_loop(0, NC, functools.partial(conv_chunk, 0, 1), 0)

    def norm_step(i, carry):
        rows = pl.ds(pl.multiple_of(i * 32, 32), 32)
        mu = jnp.broadcast_to(jnp.sum(mean_s[rows, :], axis=1, keepdims=True) * (1.0 / CH), (32, 128))
        squares = jnp.zeros((32, 128), F32)
        for c in range(NC):
            centered = conv[c, rows, :] - mu
            squares = squares + centered * centered
        inv = lax.rsqrt(jnp.sum(squares, axis=1, keepdims=True) * (1.0 / CH) + NORM_EPS)
        inv = jnp.broadcast_to(inv, (32, 128))
        mean_s[rows, :] = mu
        inv_s[rows, :] = inv
        for c in range(NC):
            lanes = slice(128 * c, 128 * c + 128)
            scaled = (conv[c, rows, :] - mu) * inv * gain_ref[:, lanes]
            act[rows, lanes] = (scaled * jax.nn.sigmoid(scaled)).astype(BF16)
        return carry

    act_copies = []
    for part_at in range(4):
        lax.fori_loop(2 * part_at, 2 * part_at + 2, norm_step, 0)
        rows = pl.ds(64 * part_at, 64)
        act_copies.append(send(act.at[rows], actsib.at[rows], sibling))
    w_event(2, 1)
    u_copy.wait_recv()

    def transpose_step(k, carry):
        zb = lax.rem(cz + k, NZ)
        cols = pl.ds(pl.multiple_of(zb * 256 + cc * 128, 128), 128)
        ut[k, :, 0:256] = u_s[:, cols].T
        ut[k, :, 256:512] = usib[:, cols].T
        return carry

    lax.fori_loop(0, NZ, transpose_step, 0)

    w_share(1)
    w_share(7)
    for copy in act_copies:
        copy.wait_recv()

    axes = ((("sp_1", cx), ("sp_0", cy)), (("sp_0", cy), ("sp_1", cx)))

    def near(axis, d):
        name, at = axis
        return {name: lax.rem(at + d + 4, 4)}

    def part(axis, d):
        return lax.rem(axis[1] + d + 4, 4)

    def partial_sums(stage):
        for k in range(NZ):
            lhs = ut[k]
            for n in range(2):
                lanes = slice(1024 * stage + 512 * n, 1024 * stage + 512 * n + 512)
                total = jnp.dot(lhs[:, 0:256], act[:, lanes], preferred_element_type=F32)
                total = total + jnp.dot(lhs[:, 256:512], actsib[:, lanes], preferred_element_type=F32)
                narrow = total.astype(BF16)
                for h in range(2):
                    for p in range(4):
                        first = 64 * h + 16 * p
                        pbuf[stage, h, p, k, :, 512 * n : 512 * n + 512] = narrow[first : first + 16, :]

    rs_copies = {}

    def rs1_send(stage):
        for h in range(2):
            axis = axes[h][0]
            far = part(axis, 2)
            for way, sign, lanes in ((0, 1, slice(0, 512)), (1, -1, slice(512, 1024))):
                rs_copies[1, stage, h, way] = send(
                    pbuf.at[stage, h, far, :, :, lanes], r1.at[stage, h, way], near(axis, sign)
                )

    def rs1_mid(stage):
        for h in range(2):
            axis = axes[h][0]
            for way, sign, lanes in ((0, 1, slice(0, 512)), (1, -1, slice(512, 1024))):
                rs_copies[1, stage, h, way].wait_recv()
                to = part(axis, sign)

                def add(k, carry, h=h, to=to, way=way, lanes=lanes):
                    pbuf[stage, h, to, k, :, lanes] = (
                        pbuf[stage, h, to, k, :, lanes].astype(F32) + r1[stage, h, way, k].astype(F32)
                    ).astype(BF16)
                    return carry

                lax.fori_loop(0, NZ, add, 0)
                rs_copies[2, stage, h, way] = send(
                    pbuf.at[stage, h, to], r2.at[stage, h, way], near(axis, sign)
                )

    def rs1_fin(stage):
        for h in range(2):
            mine = part(axes[h][0], 0)
            axis = axes[h][1]
            for way in (0, 1):
                rs_copies[2, stage, h, way].wait_recv()

            def add(k, carry, h=h, mine=mine):
                for p in range(4):
                    lanes = slice(256 * p, 256 * p + 256)
                    q[stage, h, p, k] = (
                        pbuf[stage, h, mine, k, :, lanes].astype(F32)
                        + r2[stage, h, 0, k, :, lanes].astype(F32)
                        + r2[stage, h, 1, k, :, lanes].astype(F32)
                    ).astype(BF16)
                return carry

            lax.fori_loop(0, NZ, add, 0)
            far = part(axis, 2)
            for way, sign, lanes in ((0, 1, slice(0, 128)), (1, -1, slice(128, 256))):
                rs_copies[3, stage, h, way] = send(
                    q.at[stage, h, far, :, :, lanes], s1.at[stage, h, way], near(axis, sign)
                )

    def rs2_mid(stage):
        for h in range(2):
            axis = axes[h][1]
            for way, sign, lanes in ((0, 1, slice(0, 128)), (1, -1, slice(128, 256))):
                rs_copies[3, stage, h, way].wait_recv()
                to = part(axis, sign)
                for k in range(NZ):
                    q[stage, h, to, k, :, lanes] = (
                        q[stage, h, to, k, :, lanes].astype(F32) + s1[stage, h, way, k].astype(F32)
                    ).astype(BF16)
                rs_copies[4, stage, h, way] = send(
                    q.at[stage, h, to], s2.at[stage, h, way], near(axis, sign)
                )

    z_copies = {}

    def rs2_fin(stage):
        for h in range(2):
            mine = part(axes[h][1], 0)
            for way in (0, 1):
                rs_copies[4, stage, h, way].wait_recv()
            for k in range(NZ):
                vz[stage, k, h] = (
                    q[stage, h, mine, k].astype(F32)
                    + s2[stage, h, 0, k].astype(F32)
                    + s2[stage, h, 1, k].astype(F32)
                ).astype(BF16)
        for k in (4, 3, 5, 2, 6, 1, 7):
            z_copies[stage, k] = send(vz.at[stage, k], rz.at[stage, k], zdev(k))

    gather_copies = []

    def rs3(stage):
        total = vz[stage, 0].astype(F32)
        for k in range(1, NZ):
            z_copies[stage, k].wait_recv()
            total = total + rz[stage, k].astype(F32)
        fg[stage, sp] = total.astype(BF16)
        for d in range(1, 16):
            gather_copies.append(send(fg.at[stage, sp], fg.at[stage, sp], spdev(d)))

    def grad_block(rels, first=False):
        for rel in rels:
            w_pair[rel].wait_recv()
        lhs = []
        for rel in rels:
            zb = lax.rem(cz + rel, NZ)
            lhs.append(u_s[:, pl.ds(pl.multiple_of(zb * 256, 256), 256)])

        def step(n, carry):
            lanes = pl.ds(pl.multiple_of(n * 512, 512), 512)
            total = None
            for left, rel in zip(lhs, rels):
                right = wbuf[rel, :, :, lanes].reshape(256, 512)
                term = jnp.dot(left, right, preferred_element_type=F32)
                total = term if total is None else total + term
            if first:
                gacc[:, lanes] = total
            else:
                gacc[:, lanes] += total
            return carry

        lax.fori_loop(0, 4, step, 0)

    partial_sums(0)
    rs1_send(0)
    w_event(3, 0)
    partial_sums(1)
    rs1_send(1)
    w_event(3, 1)
    w_event(4, 0)
    grad_block((0, 1, 7), first=True)
    w_event(4, 1)
    rs1_mid(0)
    w_share(2)
    w_share(6)
    rs1_mid(1)
    w_share(3)
    w_share(5)
    grad_block((2, 6))
    w_share(4)
    grad_block((3, 5))
    rs1_fin(0)
    grad_block((4,))

    dn[...] = jnp.zeros_like(dn)

    def back_rows(r):
        rows = pl.ds(r, 32)
        mu = mean_s[rows, :]
        inv = inv_s[rows, :]
        sum1 = jnp.zeros((32, 128), F32)
        sum2 = jnp.zeros((32, 128), F32)
        for c in range(NC):
            lanes = slice(128 * c, 128 * c + 128)
            gain = gain_ref[:, lanes]
            normed = (conv[c, rows, :] - mu) * inv
            scaled = normed * gain
            sig = jax.nn.sigmoid(scaled)
            grad_scaled = gacc[rows, lanes] * sig * (1.0 + scaled * (1.0 - sig))
            gain_term = grad_scaled * normed
            dn[c] += (gain_term[0:8] + gain_term[8:16]) + (gain_term[16:24] + gain_term[24:32])
            grad_normed = grad_scaled * gain
            gacc[rows, lanes] = grad_normed
            sum1 = sum1 + grad_normed
            sum2 = sum2 + grad_normed * normed
        m1 = jnp.broadcast_to(jnp.sum(sum1, axis=1, keepdims=True) * (1.0 / CH), (32, 128))
        m2 = jnp.broadcast_to(jnp.sum(sum2, axis=1, keepdims=True) * (1.0 / CH), (32, 128))
        for c in range(NC):
            lanes = slice(128 * c, 128 * c + 128)
            normed = (conv[c, rows, :] - mu) * inv
            narrow = (inv * (gacc[rows, lanes] - m1 - normed * m2)).astype(BF16)
            gpad[c, rows, :] = narrow.astype(F32)
            yield lanes, narrow

    for lanes, narrow in back_rows(0):
        ghalo_out[:, lanes] = narrow
    ghalo_copy = send(ghalo_out, ghalo_in, spdev(-1))

    def back_step(i, carry):
        for _ in back_rows(pl.multiple_of(i * 32, 32)):
            pass
        return carry

    lax.fori_loop(1, TOK // 32, back_step, 0)

    def taps_chunk(c, carry):
        def rows_step(i, sums):
            sums = list(sums)
            for k in range(4):
                r = pl.multiple_of(i * 32, 32) + 8 * k
                g = gpad[c, pl.ds(r, 8), :]
                for j in range(TAPS):
                    sums[j] = sums[j] + g * glu[c, pl.ds(r + 2 + j, 8), :]
            return tuple(sums)

        sums = lax.fori_loop(0, TOK // 32, rows_step, tuple(jnp.zeros((8, 128), F32) for _ in range(TAPS)))
        for j in range(TAPS):
            tg[c, j : j + 1, :] = jnp.sum(sums[j], axis=0, keepdims=True)
        tg[c, TAPS:, :] = jnp.sum(dn[c], axis=0, keepdims=True)
        return carry

    rs1_fin(1)
    lax.fori_loop(0, 4, taps_chunk, 0)
    rs2_mid(0)
    lax.fori_loop(4, 8, taps_chunk, 0)
    rs2_mid(1)
    lax.fori_loop(8, 12, taps_chunk, 0)
    rs2_fin(0)
    lax.fori_loop(12, NC, taps_chunk, 0)
    part_copies = [send(tg.at[lax.rem(sp + d, 16)], tr.at[d], spdev(d)) for d in range(1, 16)]
    rs2_fin(1)

    ghalo_copy.wait_recv()
    keep_g = (sp < 15).astype(F32)
    for c in range(NC):
        gpad[c, TOK:, :] = ghalo_in[:, 128 * c : 128 * c + 128].astype(F32) * keep_g

    def grad_chunk(c, carry):
        taps = [jnp.broadcast_to(tapsb[c, j : j + 1, :], (8, 128)) for j in range(TAPS)]
        lanes = pl.ds(pl.multiple_of(c * 128, 128), 128)

        def rows_step(i, carry):
            base = pl.multiple_of(i * 64, 64)
            for pair in range(4):
                values, gates = [], []
                for k in (2 * pair, 2 * pair + 1):
                    r = base + 8 * k
                    parts = [None] * 2
                    for j in range(TAPS):
                        term = taps[j] * gpad[c, pl.ds(r + 30 - j, 8), :]
                        parts[j % 2] = term if parts[j % 2] is None else parts[j % 2] + term
                    total = (parts[0] + parts[1]).astype(BF16).astype(F32)
                    values.append(total * gate_a[c, pl.ds(r, 8), :])
                    gates.append(total * gate_b[c, pl.ds(r, 8), :])
                rows = pl.ds(base + 16 * pair, 16)
                gv_s[rows, lanes] = jnp.concatenate(values, axis=0).astype(BF16)
                gt_s[rows, lanes] = jnp.concatenate(gates, axis=0).astype(BF16)
            return carry

        return lax.fori_loop(0, TOK // 64, rows_step, carry)

    stores = []

    def grad_group(at):
        lax.fori_loop(4 * at, 4 * at + 4, grad_chunk, 0)
        lanes = pl.ds(512 * at, 512)
        for narrow, wide in ((gv_s, gv_hbm), (gt_s, gt_hbm)):
            copy = pltpu.make_async_copy(
                narrow.at[:, lanes], wide.at[0, :, lanes], local_sem.at[4 + len(stores)]
            )
            copy.start()
            stores.append(copy)

    grad_group(0)
    total = tg[sp]
    for d in range(1, 16):
        part_copies[d - 1].wait_recv()
        total = total + tr[d]
    tz[cz] = total
    tz_copies = [send(tz.at[cz], tz.at[cz], zdev(d)) for d in range(1, NZ)]
    grad_group(1)
    rs3(0)
    grad_group(2)
    rs3(1)
    grad_group(3)

    for copy in tz_copies:
        copy.wait_recv()
    total = tz[0]
    for k in range(1, NZ):
        total = total + tz[k]
    tfin[...] = total
    pair_copy = send(tfin, tsib, sibling)
    pair_copy.wait_recv()
    total = tfin[...] + tsib[...]
    dt_ref[...] = total[:TAPS]
    gfull[sp] = jnp.broadcast_to(total[TAPS:, :], (8, 128))
    gain_copies = [send(gfull.at[sp], gfull.at[sp], spdev(d)) for d in range(1, 16)]

    for copy in gather_copies:
        copy.wait_recv()
    for s in range(16):
        y, x = divmod(s, 4)
        for t in range(2):
            lane = 1024 * t + 256 * y
            gw_ref[16 * x : 16 * x + 16, lane : lane + 256] = fg[t, s, 0]
            lane = 1024 * t + 256 * x
            gw_ref[64 + 16 * y : 80 + 16 * y, lane : lane + 256] = fg[t, s, 1]
    for copy in gain_copies:
        copy.wait_recv()
    for c in range(NC):
        dn_ref[:, 128 * c : 128 * c + 128] = gfull[c, 0:1, :]
    for copy in stores:
        copy.wait()
    for copy in started:
        copy.wait_send()


def body(value_half, gate_half, upstream, conv_taps, norm_gain, out_weight):
    vmem = pl.BlockSpec(memory_space=pltpu.VMEM)
    hbm = pl.BlockSpec(memory_space=pl.ANY)
    grad_value, grad_gate, grad_rows, taps, gain = pl.pallas_call(
        kernel,
        out_shape=(
            jax.ShapeDtypeStruct((1, TOK, CH), BF16),
            jax.ShapeDtypeStruct((1, TOK, CH), BF16),
            jax.ShapeDtypeStruct((128, CH), BF16),
            jax.ShapeDtypeStruct((TAPS, 128), F32),
            jax.ShapeDtypeStruct((1, CH), F32),
        ),
        in_specs=[hbm] * 4 + [vmem] * 2,
        out_specs=[hbm] * 2 + [vmem] * 3,
        scratch_shapes=[
            pltpu.VMEM((TOK, CH), BF16),
            pltpu.VMEM((TOK, CH), BF16),
            pltpu.VMEM((TOK, CH), BF16),
            pltpu.VMEM((TOK, CH), BF16),
            pltpu.VMEM((NZ, 2, 128, CH), BF16),
            pltpu.VMEM((NC, 32, 128), F32),
            pltpu.VMEM((NC, TOK + 32, 128), F32),
            pltpu.VMEM((NC, TOK, 128), F32),
            pltpu.VMEM((TOK, CH), BF16),
            pltpu.VMEM((TOK, CH), BF16),
            pltpu.VMEM((NZ, 128, 512), BF16),
            pltpu.VMEM((2, 2, 4, NZ, 16, 1024), BF16),
            pltpu.VMEM((2, 2, 2, NZ, 16, 512), BF16),
            pltpu.VMEM((2, 2, 2, NZ, 16, 1024), BF16),
            pltpu.VMEM((2, 2, 4, NZ, 16, 256), BF16),
            pltpu.VMEM((2, 2, 2, NZ, 16, 128), BF16),
            pltpu.VMEM((2, 2, 2, NZ, 16, 256), BF16),
            pltpu.VMEM((2, NZ, 2, 16, 256), BF16),
            pltpu.VMEM((2, NZ, 2, 16, 256), BF16),
            pltpu.VMEM((2, 16, 2, 16, 256), BF16),
            pltpu.VMEM((TOK, CH), F32),
            pltpu.VMEM((NC, TOK + 32, 128), F32),
            pltpu.VMEM((TOK, 128), F32),
            pltpu.VMEM((TOK, 128), F32),
            pltpu.VMEM((NC, TOK, 128), F32),
            pltpu.VMEM((NC, TOK, 128), F32),
            pltpu.VMEM((TOK, CH), BF16),
            pltpu.VMEM((TOK, CH), BF16),
            pltpu.VMEM((32, CH), BF16),
            pltpu.VMEM((32, CH), BF16),
            pltpu.VMEM((32, CH), BF16),
            pltpu.VMEM((32, CH), BF16),
            pltpu.VMEM((NC, 8, 128), F32),
            pltpu.VMEM((NC, 32, 128), F32),
            pltpu.VMEM((16, 32, 128), F32),
            pltpu.VMEM((NZ, 32, 128), F32),
            pltpu.VMEM((32, 128), F32),
            pltpu.VMEM((32, 128), F32),
            pltpu.VMEM((16, 8, 128), F32),
            pltpu.SemaphoreType.DMA((12,)),
            pltpu.SemaphoreType.DMA((N_SEND,)),
            pltpu.SemaphoreType.DMA((N_SEND,)),
        ],
        compiler_params=pltpu.CompilerParams(
            collective_id=0, has_side_effects=True, vmem_limit_bytes=66_000_000
        ),
    )(value_half, gate_half, upstream, out_weight, conv_taps, norm_gain[None])
    return grad_value, grad_gate, taps, gain.reshape(CH), grad_rows.astype(F32)


def solution(mesh):
    torus = Mesh(mesh.devices.reshape(4, 4, 8, 2), ("sp_0", "sp_1", "dp_0", "dp_1"))
    placed = (P(DP, SP, None), P(DP, SP, None), P(DP, SP, None), P(None, SP), P(), P(DP, None))
    return jax.shard_map(
        body,
        mesh=torus,
        in_specs=placed,
        out_specs=(P(DP, SP, None), P(DP, SP, None), P(None, SP), P(), P(DP, None)),
        check_vma=False,
    )
```

```python
import functools

import jax
import jax.numpy as jnp
from jax import lax
from jax.experimental import pallas as pl
from jax.experimental.pallas import tpu as pltpu
from jax.sharding import Mesh
from jax.sharding import PartitionSpec as P

DP = ("dp_0", "dp_1")
SP = ("sp_0", "sp_1")
NORM_EPS = 1e-05
MESH = pl.DeviceIdType.MESH
F32 = jnp.float32
BF16 = jnp.bfloat16

TOK = 256
CH = 2048
NC = CH // 128
TAPS = 31
ROW_ORDER = (0, 1, 3, 2)
NZ = 8
NS = 4
N_SEND = 320


def kernel(
    v_hbm, g_hbm, u_hbm, w_hbm, taps_ref, gain_ref,
    gv_hbm, gt_hbm, gw_ref, dt_ref, dn_ref,
    v_s, g_s, u_s, usib, wbuf, tapsb, glu, conv, act, actsib, ut,
    pbuf, r1, r2, q, s1, s2, vz, rz, fg, gacc, gpad, mean_s, inv_s, gate_a, gate_b, gv_s, gt_s,
    halo_out, halo_in, ghalo_out, ghalo_in, dn, tg, tr, tz, tsib, tfin, gfull, dr, dz, dfin, dsib,
    local_sem, send_sem, recv_sem,
):
    cy, cx, cz, cc = (lax.axis_index(a) for a in ("sp_0", "sp_1", "dp_0", "dp_1"))
    sp = cy * 4 + cx
    other = 1 - cc
    sibling = {"dp_1": other}

    def zdev(d):
        return {"dp_0": lax.rem(cz + d + NZ, NZ)}

    def spdev(d):
        s = lax.rem(sp + d + 16, 16)
        return {"sp_0": s // 4, "sp_1": lax.rem(s, 4)}

    used = [0]
    started = []

    def send(src, dst, device):
        i = used[0]
        used[0] += 1
        copy = pltpu.make_async_remote_copy(
            src_ref=src, dst_ref=dst, send_sem=send_sem.at[i], recv_sem=recv_sem.at[i],
            device_id=device, device_id_type=MESH,
        )
        copy.start()
        started.append(copy)
        return copy

    loads = [
        pltpu.make_async_copy(w_hbm, wbuf.at[0, cc], local_sem.at[0]),
        pltpu.make_async_copy(v_hbm.at[0], v_s, local_sem.at[1]),
        pltpu.make_async_copy(g_hbm.at[0], g_s, local_sem.at[2]),
        pltpu.make_async_copy(u_hbm.at[0], u_s, local_sem.at[3]),
    ]
    for load in loads:
        load.start()

    barrier = pltpu.get_barrier_semaphore()
    pl.semaphore_signal(barrier, inc=1, device_id=sibling, device_id_type=MESH)
    for d in range(1, NZ):
        pl.semaphore_signal(barrier, inc=1, device_id=zdev(d), device_id_type=MESH)
    for d in range(1, 16):
        pl.semaphore_signal(barrier, inc=1, device_id=spdev(d), device_id_type=MESH)

    tapsb[sp, :TAPS] = taps_ref[...]
    tapsb[sp, TAPS:] = jnp.zeros((1, 128), F32)
    loads[0].wait()
    pl.semaphore_wait(barrier, 23)

    parity = lax.rem(cy + cx, 2)
    w_copies = {}
    w_quarters = {}
    w_pair = {}

    def arrived(copies, key):
        copy = copies.pop(key, None)
        if copy is not None:
            copy.wait_recv()

    def w_send(half, step, sub):
        at = parity if half == 0 else 1 - parity
        rows = pl.ds(pl.multiple_of(64 * at + 32 * sub, 32), 32)
        lanes = (slice(0, 1024), slice(1024, 2048)) if step == 4 else (slice(None), slice(None))
        for way, sign in ((0, 1), (1, -1)):
            src = (-sign * (step - 1)) % NZ
            dst = (-sign * step) % NZ
            w_copies[half, step, sub, way] = send(
                wbuf.at[src, cc, rows, lanes[way]], wbuf.at[dst, cc, rows, lanes[way]], zdev(sign)
            )

    def w_share(rel):
        for turn in range(4):
            arrived(w_quarters, (rel, turn))
        w_pair[rel] = send(wbuf.at[rel, cc], wbuf.at[rel, cc], sibling)

    def w_event(step, sub):
        for way in (0, 1):
            arrived(w_copies, (0, step, sub, way))
        if step < 4:
            w_send(0, step + 1, sub)
        name, at = (("sp_1", cx), ("sp_0", cy))[sub]
        if step < 3:
            for rel in (step, NZ - step):
                for turn, sign in ((2 * sub, 1), (2 * sub + 1, -1)):
                    rows = pl.ds(pl.multiple_of(64 * parity + 16 * turn, 16), 16)
                    w_quarters[rel, turn] = send(
                        wbuf.at[rel, cc, rows], wbuf.at[rel, cc, rows], {name: lax.rem(at + sign + 4, 4)}
                    )

    def w_rest(step, sub):
        if step == 2:
            for rel in (2, 6):
                for turn in (2 * sub, 2 * sub + 1):
                    arrived(w_quarters, (rel, turn))
        else:
            for way in (0, 1):
                arrived(w_copies, (1, step, sub, way))
        if step < 4:
            w_send(1, step + 1, sub)

    taps_copies = {
        dy: [
            send(tapsb.at[sp], tapsb.at[sp], {"sp_0": lax.rem(cy + dy, 4), "sp_1": lax.rem(cx + dx, 4)})
            for dx in range(4)
            if dx or dy
        ]
        for dy in ROW_ORDER
    }
    w_send(0, 1, 0)
    w_send(0, 1, 1)
    for load in loads[1:]:
        load.wait()
    u_copy = send(u_s, usib, sibling)
    w_share(0)

    def glu_rows(r):
        rows = pl.ds(r, 32)
        for c in range(NC):
            lanes = slice(128 * c, 128 * c + 128)
            value = v_s[rows, lanes].astype(F32)
            sig = jax.nn.sigmoid(g_s[rows, lanes].astype(F32))
            wide = value * sig
            gate_a[c, rows, :] = sig
            gate_b[c, rows, :] = wide * (1.0 - sig)
            narrow = wide.astype(BF16)
            glu[c, pl.ds(r + 32, 32), :] = narrow.astype(F32)
            yield lanes, narrow

    for lanes, narrow in glu_rows(TOK - 32):
        halo_out[:, lanes] = narrow
    halo_copy = send(halo_out, halo_in, spdev(1))

    def glu_step(i, carry):
        for _ in glu_rows(pl.multiple_of(i * 32, 32)):
            pass
        return carry

    lax.fori_loop(0, TOK // 32 - 1, glu_step, 0)

    u_copy.wait_recv()

    def transpose_step(k, carry):
        zb = lax.rem(cz + k, NZ)
        cols = pl.ds(pl.multiple_of(zb * 256 + cc * 128, 128), 128)
        ut[k, :, 0:256] = u_s[:, cols].T
        ut[k, :, 256:512] = usib[:, cols].T
        return carry

    lax.fori_loop(0, NZ, transpose_step, 0)

    mean_s[...] = jnp.zeros_like(mean_s)

    def conv_chunk(first, last, c, carry):
        taps = [jnp.broadcast_to(tapsb[c, j : j + 1, :], (8, 128)) for j in range(TAPS)]

        def rows_step(i, carry):
            for k in range(8):
                r = pl.multiple_of(i * 64, 64) + 8 * k
                parts = [None] * 2
                for j in range(TAPS):
                    term = taps[j] * glu[c, pl.ds(r + 2 + j, 8), :]
                    parts[j % 2] = term if parts[j % 2] is None else parts[j % 2] + term
                total = (parts[0] + parts[1]).astype(BF16).astype(F32)
                conv[c, pl.ds(r, 8), :] = total
                mean_s[pl.ds(r, 8), :] += total
            return carry

        return lax.fori_loop(first, last, rows_step, carry)

    body_rows = functools.partial(conv_chunk, 1, TOK // 64)

    def conv_group(dy):
        for copy in taps_copies[dy]:
            copy.wait_recv()
        row = lax.rem(cy - dy + 4, 4)
        lax.fori_loop(4 * row, 4 * row + 4, body_rows, 0)

    conv_group(ROW_ORDER[0])
    w_event(1, 0)
    conv_group(ROW_ORDER[1])
    conv_group(ROW_ORDER[2])
    w_event(1, 1)
    conv_group(ROW_ORDER[3])
    halo_copy.wait_recv()
    keep = (sp > 0).astype(F32)
    for c in range(NC):
        glu[c, 0:32, :] = halo_in[:, 128 * c : 128 * c + 128].astype(F32) * keep
    lax.fori_loop(0, NC, functools.partial(conv_chunk, 0, 1), 0)

    def norm_step(i, carry):
        rows = pl.ds(pl.multiple_of(i * 32, 32), 32)
        mu = jnp.broadcast_to(jnp.sum(mean_s[rows, :], axis=1, keepdims=True) * (1.0 / CH), (32, 128))
        squares = jnp.zeros((32, 128), F32)
        for c in range(NC):
            centered = conv[c, rows, :] - mu
            squares = squares + centered * centered
        inv = lax.rsqrt(jnp.sum(squares, axis=1, keepdims=True) * (1.0 / CH) + NORM_EPS)
        inv = jnp.broadcast_to(inv, (32, 128))
        mean_s[rows, :] = mu
        inv_s[rows, :] = inv
        for c in range(NC):
            lanes = slice(128 * c, 128 * c + 128)
            scaled = (conv[c, rows, :] - mu) * inv * gain_ref[:, lanes]
            act[rows, lanes] = (scaled * jax.nn.sigmoid(scaled)).astype(BF16)
        return carry

    act_copies = []

    def norm_part(at):
        lax.fori_loop(2 * at, 2 * at + 2, norm_step, 0)
        rows = pl.ds(64 * at, 64)
        act_copies.append(send(act.at[rows], actsib.at[rows], sibling))

    norm_part(0)
    norm_part(1)
    w_event(2, 0)
    norm_part(2)
    norm_part(3)
    w_share(1)
    w_share(7)
    for copy in act_copies:
        copy.wait_recv()

    axes = ((("sp_1", cx), ("sp_0", cy)), (("sp_0", cy), ("sp_1", cx)))

    def near(axis, d):
        name, at = axis
        return {name: lax.rem(at + d + 4, 4)}

    def part(axis, d):
        return lax.rem(axis[1] + d + 4, 4)

    def partial_sums(stage):
        lanes = slice(512 * stage, 512 * stage + 512)
        for k in range(NZ):
            lhs = ut[k]
            total = jnp.dot(lhs[:, 0:256], act[:, lanes], preferred_element_type=F32)
            total = total + jnp.dot(lhs[:, 256:512], actsib[:, lanes], preferred_element_type=F32)
            narrow = total.astype(BF16)
            for h in range(2):
                for p in range(4):
                    first = 64 * h + 16 * p
                    pbuf[stage, h, p, k] = narrow[first : first + 16, :]

    rs_copies = {}

    def rs1_send(stage):
        for h in range(2):
            axis = axes[h][0]
            far = part(axis, 2)
            for way, sign, lanes in ((0, 1, slice(0, 256)), (1, -1, slice(256, 512))):
                rs_copies[1, stage, h, way] = send(
                    pbuf.at[stage, h, far, :, :, lanes], r1.at[stage, h, way], near(axis, sign)
                )

    def rs1_mid(stage):
        for h in range(2):
            axis = axes[h][0]
            for way, sign, lanes in ((0, 1, slice(0, 256)), (1, -1, slice(256, 512))):
                rs_copies[1, stage, h, way].wait_recv()
                to = part(axis, sign)

                def add(k, carry, h=h, to=to, way=way, lanes=lanes):
                    pbuf[stage, h, to, k, :, lanes] = (
                        pbuf[stage, h, to, k, :, lanes].astype(F32) + r1[stage, h, way, k].astype(F32)
                    ).astype(BF16)
                    return carry

                lax.fori_loop(0, NZ, add, 0)
                rs_copies[2, stage, h, way] = send(
                    pbuf.at[stage, h, to], r2.at[stage, h, way], near(axis, sign)
                )

    def rs1_fin(stage):
        for h in range(2):
            mine = part(axes[h][0], 0)
            axis = axes[h][1]
            for way in (0, 1):
                rs_copies[2, stage, h, way].wait_recv()

            def add(k, carry, h=h, mine=mine):
                for p in range(4):
                    lanes = slice(128 * p, 128 * p + 128)
                    q[stage, h, p, k] = (
                        pbuf[stage, h, mine, k, :, lanes].astype(F32)
                        + r2[stage, h, 0, k, :, lanes].astype(F32)
                        + r2[stage, h, 1, k, :, lanes].astype(F32)
                    ).astype(BF16)
                return carry

            lax.fori_loop(0, NZ, add, 0)
            far = part(axis, 2)
            for way, sign in ((0, 1), (1, -1)):
                rs_copies[3, stage, h, way] = send(
                    q.at[stage, h, far, pl.ds(4 * way, 4)], s1.at[stage, h, way], near(axis, sign)
                )

    def rs2_mid(stage):
        for h in range(2):
            axis = axes[h][1]
            for way, sign in ((0, 1), (1, -1)):
                rs_copies[3, stage, h, way].wait_recv()
                to = part(axis, sign)
                for k in range(4):
                    q[stage, h, to, 4 * way + k] = (
                        q[stage, h, to, 4 * way + k].astype(F32) + s1[stage, h, way, k].astype(F32)
                    ).astype(BF16)
                rs_copies[4, stage, h, way] = send(
                    q.at[stage, h, to], s2.at[stage, h, way], near(axis, sign)
                )

    z_copies = {}

    def rs2_fin(stage):
        for h in range(2):
            mine = part(axes[h][1], 0)
            for way in (0, 1):
                rs_copies[4, stage, h, way].wait_recv()
            for k in range(NZ):
                vz[stage, k, h] = (
                    q[stage, h, mine, k].astype(F32)
                    + s2[stage, h, 0, k].astype(F32)
                    + s2[stage, h, 1, k].astype(F32)
                ).astype(BF16)
        for k in (4, 3, 5, 2, 6, 1, 7):
            z_copies[stage, k] = send(vz.at[stage, k], rz.at[stage, k], zdev(k))

    gather_copies = []

    def rs3(stage):
        total = vz[stage, 0].astype(F32)
        for k in range(1, NZ):
            z_copies[stage, k].wait_recv()
            total = total + rz[stage, k].astype(F32)
        fg[stage, sp] = total.astype(BF16)
        for d in range(1, 16):
            gather_copies.append(send(fg.at[stage, sp], fg.at[stage, sp], spdev(d)))

    def grad_block(rels, first=False):
        for rel in rels:
            w_pair[rel].wait_recv()
        lhs = []
        for rel in rels:
            zb = lax.rem(cz + rel, NZ)
            lhs.append(u_s[:, pl.ds(pl.multiple_of(zb * 256, 256), 256)])

        def step(n, carry):
            lanes = pl.ds(pl.multiple_of(n * 512, 512), 512)
            total = None
            for left, rel in zip(lhs, rels):
                right = wbuf[rel, :, :, lanes].reshape(256, 512)
                term = jnp.dot(left, right, preferred_element_type=F32)
                total = term if total is None else total + term
            if first:
                gacc[:, lanes] = total
            else:
                gacc[:, lanes] += total
            return carry

        lax.fori_loop(0, 4, step, 0)

    partial_sums(0)
    rs1_send(0)
    w_event(2, 1)
    partial_sums(1)
    rs1_send(1)
    w_rest(2, 0)
    partial_sums(2)
    rs1_send(2)
    w_event(3, 0)
    partial_sums(3)
    rs1_send(3)
    grad_block((0, 1, 7), first=True)
    rs1_mid(0)
    w_rest(2, 1)
    w_event(3, 1)
    rs1_mid(1)
    w_share(2)
    w_share(6)
    grad_block((2, 6))
    w_rest(3, 0)
    w_event(4, 0)
    w_event(4, 1)
    w_rest(3, 1)
    rs1_fin(0)
    rs1_mid(2)
    w_share(3)
    w_share(5)
    rs1_fin(1)
    rs1_mid(3)
    rs2_mid(0)
    grad_block((3, 5))
    w_rest(4, 0)
    w_rest(4, 1)
    w_share(4)
    rs2_mid(1)
    rs1_fin(2)
    grad_block((4,))

    dn[...] = jnp.zeros_like(dn)

    def back_rows(r):
        rows = pl.ds(r, 32)
        mu = mean_s[rows, :]
        inv = inv_s[rows, :]
        sum1 = jnp.zeros((32, 128), F32)
        sum2 = jnp.zeros((32, 128), F32)
        for c in range(NC):
            lanes = slice(128 * c, 128 * c + 128)
            gain = gain_ref[:, lanes]
            normed = (conv[c, rows, :] - mu) * inv
            scaled = normed * gain
            sig = jax.nn.sigmoid(scaled)
            grad_scaled = gacc[rows, lanes] * sig * (1.0 + scaled * (1.0 - sig))
            gain_term = grad_scaled * normed
            dn[c] += (gain_term[0:8] + gain_term[8:16]) + (gain_term[16:24] + gain_term[24:32])
            grad_normed = grad_scaled * gain
            gacc[rows, lanes] = grad_normed
            sum1 = sum1 + grad_normed
            sum2 = sum2 + grad_normed * normed
        m1 = jnp.broadcast_to(jnp.sum(sum1, axis=1, keepdims=True) * (1.0 / CH), (32, 128))
        m2 = jnp.broadcast_to(jnp.sum(sum2, axis=1, keepdims=True) * (1.0 / CH), (32, 128))
        for c in range(NC):
            lanes = slice(128 * c, 128 * c + 128)
            normed = (conv[c, rows, :] - mu) * inv
            narrow = (inv * (gacc[rows, lanes] - m1 - normed * m2)).astype(BF16)
            gpad[c, rows, :] = narrow.astype(F32)
            yield lanes, narrow

    for lanes, narrow in back_rows(0):
        ghalo_out[:, lanes] = narrow
    ghalo_copy = send(ghalo_out, ghalo_in, spdev(-1))

    def back_step(i, carry):
        for _ in back_rows(pl.multiple_of(i * 32, 32)):
            pass
        return carry

    lax.fori_loop(1, TOK // 32, back_step, 0)

    def rest_of_plane(d):
        return lax.rem(sp + d, 16)

    gain_copies = [send(dn.at[rest_of_plane(d)], dr.at[d], spdev(d)) for d in range(1, 16)]

    def gain_sum():
        total = dn[sp]
        for d in range(1, 16):
            gain_copies[d - 1].wait_recv()
            total = total + dr[d]
        dz[cz] = total
        return [send(dz.at[cz], dz.at[cz], zdev(d)) for d in range(1, NZ)]

    def gain_pair(copies):
        for copy in copies:
            copy.wait_recv()
        total = dz[0]
        for k in range(1, NZ):
            total = total + dz[k]
        dfin[...] = total
        return send(dfin, dsib, sibling)

    def gain_out(copy):
        copy.wait_recv()
        gfull[sp] = dfin[...] + dsib[...]
        return [send(gfull.at[sp], gfull.at[sp], spdev(d)) for d in range(1, 16)]

    def taps_chunk(c, carry):
        def rows_step(i, sums):
            sums = list(sums)
            for k in range(4):
                r = pl.multiple_of(i * 32, 32) + 8 * k
                g = gpad[c, pl.ds(r, 8), :]
                for j in range(TAPS):
                    sums[j] = sums[j] + g * glu[c, pl.ds(r + 2 + j, 8), :]
            return tuple(sums)

        sums = lax.fori_loop(0, TOK // 32, rows_step, tuple(jnp.zeros((8, 128), F32) for _ in range(TAPS)))
        for j in range(TAPS):
            tg[c, j : j + 1, :] = jnp.sum(sums[j], axis=0, keepdims=True)
        tg[c, TAPS:, :] = jnp.zeros((1, 128), F32)
        return carry

    part_copies = []

    def taps_group(dy):
        row = lax.rem(cy + dy, 4)
        lax.fori_loop(4 * row, 4 * row + 4, taps_chunk, 0)
        for dx in range(4):
            if dx or dy:
                x = lax.rem(cx + dx, 4)
                part_copies.append(
                    send(tg.at[4 * row + x], tr.at[4 * dy + dx], {"sp_0": row, "sp_1": x})
                )

    rs2_fin(0)
    rs2_mid(2)
    rs1_fin(3)
    taps_group(2)
    rs2_fin(1)
    taps_group(1)
    gain_z = gain_sum()
    rs2_mid(3)
    rs2_fin(2)
    taps_group(3)
    rs2_fin(3)
    rs3(0)
    taps_group(0)
    gain_last = gain_pair(gain_z)
    rs3(1)

    ghalo_copy.wait_recv()
    keep_g = (sp < 15).astype(F32)
    for c in range(NC):
        gpad[c, TOK:, :] = ghalo_in[:, 128 * c : 128 * c + 128].astype(F32) * keep_g

    def grad_chunk(c, carry):
        taps = [jnp.broadcast_to(tapsb[c, j : j + 1, :], (8, 128)) for j in range(TAPS)]
        lanes = pl.ds(pl.multiple_of(c * 128, 128), 128)

        def rows_step(i, carry):
            base = pl.multiple_of(i * 64, 64)
            for pair in range(4):
                values, gates = [], []
                for k in (2 * pair, 2 * pair + 1):
                    r = base + 8 * k
                    parts = [None] * 2
                    for j in range(TAPS):
                        term = taps[j] * gpad[c, pl.ds(r + 30 - j, 8), :]
                        parts[j % 2] = term if parts[j % 2] is None else parts[j % 2] + term
                    total = (parts[0] + parts[1]).astype(BF16).astype(F32)
                    values.append(total * gate_a[c, pl.ds(r, 8), :])
                    gates.append(total * gate_b[c, pl.ds(r, 8), :])
                rows = pl.ds(base + 16 * pair, 16)
                gv_s[rows, lanes] = jnp.concatenate(values, axis=0).astype(BF16)
                gt_s[rows, lanes] = jnp.concatenate(gates, axis=0).astype(BF16)
            return carry

        return lax.fori_loop(0, TOK // 64, rows_step, carry)

    stores = []

    def grad_group(at):
        lax.fori_loop(4 * at, 4 * at + 4, grad_chunk, 0)
        lanes = pl.ds(512 * at, 512)
        for narrow, wide in ((gv_s, gv_hbm), (gt_s, gt_hbm)):
            copy = pltpu.make_async_copy(
                narrow.at[:, lanes], wide.at[0, :, lanes], local_sem.at[4 + len(stores)]
            )
            copy.start()
            stores.append(copy)

    grad_group(0)
    gain_copies2 = gain_out(gain_last)
    rs3(2)
    grad_group(1)
    total = tg[sp]
    for copy in part_copies:
        copy.wait_recv()
    for d in range(1, 16):
        total = total + tr[d]
    tz[cz] = total
    tz_copies = [send(tz.at[cz], tz.at[cz], zdev(d)) for d in range(1, NZ)]
    rs3(3)
    grad_group(2)
    grad_group(3)

    for copy in tz_copies:
        copy.wait_recv()
    total = tz[0]
    for k in range(1, NZ):
        total = total + tz[k]
    tfin[...] = total
    pair_copy = send(tfin, tsib, sibling)

    for copy in gather_copies:
        copy.wait_recv()
    for s in range(16):
        y, x = divmod(s, 4)
        for t in range(NS):
            lane = 512 * t + 128 * y
            gw_ref[16 * x : 16 * x + 16, lane : lane + 128] = fg[t, s, 0]
            lane = 512 * t + 128 * x
            gw_ref[64 + 16 * y : 80 + 16 * y, lane : lane + 128] = fg[t, s, 1]
    for copy in gain_copies2:
        copy.wait_recv()
    for c in range(NC):
        dn_ref[:, 128 * c : 128 * c + 128] = jnp.sum(gfull[c], axis=0, keepdims=True)
    pair_copy.wait_recv()
    dt_ref[...] = (tfin[...] + tsib[...])[:TAPS]
    for copy in stores:
        copy.wait()
    for copy in started:
        copy.wait_send()


def write_out(gv, gt, gw, dt, dn, gv_out, gt_out, gw_out, dt_out, dn_out, gv_s, gt_s, gw_s, gw_wide, dt_s, dn_s, sem):
    copies = []
    for i, (source, held, target) in enumerate(
        ((gw, gw_s, gw_out), (gv, gv_s, gv_out), (gt, gt_s, gt_out), (dt, dt_s, dt_out), (dn, dn_s, dn_out))
    ):
        copy = pltpu.make_async_copy(source, held, sem.at[0, i])
        copy.start()
        copies.append((copy, held, target))
    outs = []
    for i, (copy, held, target) in enumerate(copies):
        copy.wait()
        if i == 0:
            gw_wide[...] = gw_s[...].astype(F32)
            held = gw_wide
        out = pltpu.make_async_copy(held, target, sem.at[1, i])
        out.start()
        outs.append(out)
    for out in outs:
        out.wait()


def body(value_half, gate_half, upstream, conv_taps, norm_gain, out_weight):
    vmem = pl.BlockSpec(memory_space=pltpu.VMEM)
    hbm = pl.BlockSpec(memory_space=pl.ANY)
    grad_value, grad_gate, grad_rows, taps, gain = pl.pallas_call(
        kernel,
        out_shape=(
            jax.ShapeDtypeStruct((1, TOK, CH), BF16),
            jax.ShapeDtypeStruct((1, TOK, CH), BF16),
            jax.ShapeDtypeStruct((128, CH), BF16),
            jax.ShapeDtypeStruct((TAPS, 128), F32),
            jax.ShapeDtypeStruct((1, CH), F32),
        ),
        in_specs=[hbm] * 4 + [vmem] * 2,
        out_specs=[hbm] * 2 + [vmem] * 3,
        scratch_shapes=[
            pltpu.VMEM((TOK, CH), BF16),
            pltpu.VMEM((TOK, CH), BF16),
            pltpu.VMEM((TOK, CH), BF16),
            pltpu.VMEM((TOK, CH), BF16),
            pltpu.VMEM((NZ, 2, 128, CH), BF16),
            pltpu.VMEM((NC, 32, 128), F32),
            pltpu.VMEM((NC, TOK + 32, 128), F32),
            pltpu.VMEM((NC, TOK, 128), F32),
            pltpu.VMEM((TOK, CH), BF16),
            pltpu.VMEM((TOK, CH), BF16),
            pltpu.VMEM((NZ, 128, 512), BF16),
            pltpu.VMEM((NS, 2, 4, NZ, 16, 512), BF16),
            pltpu.VMEM((NS, 2, 2, NZ, 16, 256), BF16),
            pltpu.VMEM((NS, 2, 2, NZ, 16, 512), BF16),
            pltpu.VMEM((NS, 2, 4, NZ, 16, 128), BF16),
            pltpu.VMEM((NS, 2, 2, 4, 16, 128), BF16),
            pltpu.VMEM((NS, 2, 2, NZ, 16, 128), BF16),
            pltpu.VMEM((NS, NZ, 2, 16, 128), BF16),
            pltpu.VMEM((NS, NZ, 2, 16, 128), BF16),
            pltpu.VMEM((NS, 16, 2, 16, 128), BF16),
            pltpu.VMEM((TOK, CH), F32),
            pltpu.VMEM((NC, TOK + 32, 128), F32),
            pltpu.VMEM((TOK, 128), F32),
            pltpu.VMEM((TOK, 128), F32),
            pltpu.VMEM((NC, TOK, 128), F32),
            pltpu.VMEM((NC, TOK, 128), F32),
            pltpu.VMEM((TOK, CH), BF16),
            pltpu.VMEM((TOK, CH), BF16),
            pltpu.VMEM((32, CH), BF16),
            pltpu.VMEM((32, CH), BF16),
            pltpu.VMEM((32, CH), BF16),
            pltpu.VMEM((32, CH), BF16),
            pltpu.VMEM((NC, 8, 128), F32),
            pltpu.VMEM((NC, 32, 128), F32),
            pltpu.VMEM((16, 32, 128), F32),
            pltpu.VMEM((NZ, 32, 128), F32),
            pltpu.VMEM((32, 128), F32),
            pltpu.VMEM((32, 128), F32),
            pltpu.VMEM((16, 8, 128), F32),
            pltpu.VMEM((16, 8, 128), F32),
            pltpu.VMEM((NZ, 8, 128), F32),
            pltpu.VMEM((8, 128), F32),
            pltpu.VMEM((8, 128), F32),
            pltpu.SemaphoreType.DMA((12,)),
            pltpu.SemaphoreType.DMA((N_SEND,)),
            pltpu.SemaphoreType.DMA((N_SEND,)),
        ],
        compiler_params=pltpu.CompilerParams(
            collective_id=0, has_side_effects=True, vmem_limit_bytes=66_000_000
        ),
    )(value_half, gate_half, upstream, out_weight, conv_taps, norm_gain[None])
    grad_value, grad_gate, grad_rows, taps, gain = pl.pallas_call(
        write_out,
        out_shape=(
            jax.ShapeDtypeStruct((1, TOK, CH), BF16),
            jax.ShapeDtypeStruct((1, TOK, CH), BF16),
            jax.ShapeDtypeStruct((128, CH), F32),
            jax.ShapeDtypeStruct((TAPS, 128), F32),
            jax.ShapeDtypeStruct((1, CH), F32),
        ),
        in_specs=[hbm] * 5,
        out_specs=[hbm] * 5,
        scratch_shapes=[
            pltpu.VMEM((1, TOK, CH), BF16),
            pltpu.VMEM((1, TOK, CH), BF16),
            pltpu.VMEM((128, CH), BF16),
            pltpu.VMEM((128, CH), F32),
            pltpu.VMEM((TAPS, 128), F32),
            pltpu.VMEM((1, CH), F32),
            pltpu.SemaphoreType.DMA((2, 5)),
        ],
        compiler_params=pltpu.CompilerParams(vmem_limit_bytes=60_000_000),
    )(grad_value, grad_gate, grad_rows, taps, gain)
    return grad_value, grad_gate, taps, gain.reshape(CH), grad_rows


def solution(mesh):
    torus = Mesh(mesh.devices.reshape(4, 4, 8, 2), ("sp_0", "sp_1", "dp_0", "dp_1"))
    placed = (P(DP, SP, None), P(DP, SP, None), P(DP, SP, None), P(None, SP), P(), P(DP, None))
    return jax.shard_map(
        body,
        mesh=torus,
        in_specs=placed,
        out_specs=(P(DP, SP, None), P(DP, SP, None), P(None, SP), P(), P(DP, None)),
        check_vma=False,
    )
```

```python
import functools

import jax
import jax.numpy as jnp
from jax import lax
from jax.experimental import pallas as pl
from jax.experimental.pallas import tpu as pltpu
from jax.sharding import Mesh
from jax.sharding import PartitionSpec as P

DP = ("dp_0", "dp_1")
SP = ("sp_0", "sp_1")
NORM_EPS = 1e-05
MESH = pl.DeviceIdType.MESH
F32 = jnp.float32
BF16 = jnp.bfloat16

TOK = 256
CH = 2048
NC = CH // 128
TAPS = 31
ROW_ORDER = (0, 1, 3, 2)
NZ = 8
NS = 4
N_SEND = 320


def kernel(
    v_hbm, g_hbm, u_hbm, w_hbm, taps_hbm, gain_hbm,
    gv_hbm, gt_hbm, gw_hbm, dt_hbm, dn_hbm,
    gain_ref, gw_ref, dt_ref, dn_ref,
    v_s, g_s, u_s, usib, wbuf, tapsb, glu, conv, act, actsib, ut,
    pbuf, r1, r2, q, s1, s2, vz, rz, fg, gacc, gpad, mean_s, inv_s, gate_a, gate_b, gv_s, gt_s,
    halo_out, halo_in, ghalo_out, ghalo_in, dn, tg, tr, tz, tsib, tfin, gfull, dr, dz, dfin, dsib,
    local_sem, send_sem, recv_sem,
):
    cy, cx, cz, cc = (lax.axis_index(a) for a in ("sp_0", "sp_1", "dp_0", "dp_1"))
    sp = cy * 4 + cx
    other = 1 - cc
    sibling = {"dp_1": other}

    def zdev(d):
        return {"dp_0": lax.rem(cz + d + NZ, NZ)}

    def spdev(d):
        s = lax.rem(sp + d + 16, 16)
        return {"sp_0": s // 4, "sp_1": lax.rem(s, 4)}

    used = [0]
    started = []

    def send(src, dst, device):
        i = used[0]
        used[0] += 1
        copy = pltpu.make_async_remote_copy(
            src_ref=src, dst_ref=dst, send_sem=send_sem.at[i], recv_sem=recv_sem.at[i],
            device_id=device, device_id_type=MESH,
        )
        copy.start()
        started.append(copy)
        return copy

    loads = [
        pltpu.make_async_copy(w_hbm, wbuf.at[0, cc], local_sem.at[0]),
        pltpu.make_async_copy(v_hbm.at[0], v_s, local_sem.at[1]),
        pltpu.make_async_copy(g_hbm.at[0], g_s, local_sem.at[2]),
        pltpu.make_async_copy(u_hbm.at[0], u_s, local_sem.at[3]),
        pltpu.make_async_copy(taps_hbm, tapsb.at[sp, pl.ds(0, TAPS)], local_sem.at[12]),
        pltpu.make_async_copy(gain_hbm, gain_ref, local_sem.at[13]),
    ]
    for at in (1, 2, 4, 5, 0, 3):
        loads[at].start()

    barrier = pltpu.get_barrier_semaphore()
    pl.semaphore_signal(barrier, inc=1, device_id=sibling, device_id_type=MESH)
    for d in range(1, NZ):
        pl.semaphore_signal(barrier, inc=1, device_id=zdev(d), device_id_type=MESH)
    for d in range(1, 16):
        pl.semaphore_signal(barrier, inc=1, device_id=spdev(d), device_id_type=MESH)

    for load in loads[1:3]:
        load.wait()
    def glu_rows(r):
        rows = pl.ds(r, 32)
        for c in range(NC):
            lanes = slice(128 * c, 128 * c + 128)
            value = v_s[rows, lanes].astype(F32)
            sig = jax.nn.sigmoid(g_s[rows, lanes].astype(F32))
            wide = value * sig
            gate_a[c, rows, :] = sig
            gate_b[c, rows, :] = wide * (1.0 - sig)
            narrow = wide.astype(BF16)
            glu[c, pl.ds(r + 32, 32), :] = narrow.astype(F32)
            yield lanes, narrow

    for lanes, narrow in glu_rows(TOK - 32):
        halo_out[:, lanes] = narrow

    def glu_step(i, carry):
        for _ in glu_rows(pl.multiple_of(i * 32, 32)):
            pass
        return carry

    lax.fori_loop(0, TOK // 32 - 1, glu_step, 0)

    for load in loads[3:]:
        load.wait()
    tapsb[sp, TAPS:] = jnp.zeros((1, 128), F32)
    loads[0].wait()
    pl.semaphore_wait(barrier, 23)

    parity = lax.rem(cy + cx, 2)
    w_copies = {}
    w_quarters = {}
    w_pair = {}

    def arrived(copies, key):
        copy = copies.pop(key, None)
        if copy is not None:
            copy.wait_recv()

    def w_send(half, step, sub):
        at = parity if half == 0 else 1 - parity
        rows = pl.ds(pl.multiple_of(64 * at + 32 * sub, 32), 32)
        lanes = (slice(0, 1024), slice(1024, 2048)) if step == 4 else (slice(None), slice(None))
        for way, sign in ((0, 1), (1, -1)):
            src = (-sign * (step - 1)) % NZ
            dst = (-sign * step) % NZ
            w_copies[half, step, sub, way] = send(
                wbuf.at[src, cc, rows, lanes[way]], wbuf.at[dst, cc, rows, lanes[way]], zdev(sign)
            )

    def w_share(rel):
        for turn in range(4):
            arrived(w_quarters, (rel, turn))
        w_pair[rel] = send(wbuf.at[rel, cc], wbuf.at[rel, cc], sibling)

    def w_event(step, sub):
        for way in (0, 1):
            arrived(w_copies, (0, step, sub, way))
        if step < 4:
            w_send(0, step + 1, sub)
        name, at = (("sp_1", cx), ("sp_0", cy))[sub]
        if step < 3:
            for rel in (step, NZ - step):
                for turn, sign in ((2 * sub, 1), (2 * sub + 1, -1)):
                    rows = pl.ds(pl.multiple_of(64 * parity + 16 * turn, 16), 16)
                    w_quarters[rel, turn] = send(
                        wbuf.at[rel, cc, rows], wbuf.at[rel, cc, rows], {name: lax.rem(at + sign + 4, 4)}
                    )

    def w_rest(step, sub):
        if step == 2:
            for rel in (2, 6):
                for turn in (2 * sub, 2 * sub + 1):
                    arrived(w_quarters, (rel, turn))
        else:
            for way in (0, 1):
                arrived(w_copies, (1, step, sub, way))
        if step < 4:
            w_send(1, step + 1, sub)

    taps_copies = {
        dy: [
            send(tapsb.at[sp], tapsb.at[sp], {"sp_0": lax.rem(cy + dy, 4), "sp_1": lax.rem(cx + dx, 4)})
            for dx in range(4)
            if dx or dy
        ]
        for dy in ROW_ORDER
    }
    w_send(0, 1, 0)
    w_send(0, 1, 1)
    halo_copy = send(halo_out, halo_in, spdev(1))
    u_copy = send(u_s, usib, sibling)
    w_share(0)

    u_copy.wait_recv()

    def transpose_step(k, carry):
        zb = lax.rem(cz + k, NZ)
        cols = pl.ds(pl.multiple_of(zb * 256 + cc * 128, 128), 128)
        ut[k, :, 0:256] = u_s[:, cols].T
        ut[k, :, 256:512] = usib[:, cols].T
        return carry

    lax.fori_loop(0, NZ, transpose_step, 0)

    def correlate(taps, read):
        sums = {}
        for o in range(8 * 7 + TAPS):
            x = read(o)
            for k in range(8):
                j = o - 8 * k
                if 0 <= j < TAPS:
                    term = taps[j] * x
                    key = k, j % 2
                    sums[key] = sums[key] + term if key in sums else term
                    if j == TAPS - 1:
                        yield k, sums.pop((k, 0)) + sums.pop((k, 1))

    mean_s[...] = jnp.zeros_like(mean_s)

    def conv_chunk(first, last, c, carry):
        taps = [jnp.broadcast_to(tapsb[c, j : j + 1, :], (8, 128)) for j in range(TAPS)]

        def rows_step(i, carry):
            base = pl.multiple_of(i * 64, 64)
            for k, total in correlate(taps, lambda o: glu[c, pl.ds(base + 2 + o, 8), :]):
                total = total.astype(BF16).astype(F32)
                conv[c, pl.ds(base + 8 * k, 8), :] = total
                mean_s[pl.ds(base + 8 * k, 8), :] += total
            return carry

        return lax.fori_loop(first, last, rows_step, carry)

    body_rows = functools.partial(conv_chunk, 1, TOK // 64)

    def conv_group(dy):
        for copy in taps_copies[dy]:
            copy.wait_recv()
        row = lax.rem(cy - dy + 4, 4)
        lax.fori_loop(4 * row, 4 * row + 4, body_rows, 0)

    conv_group(ROW_ORDER[0])
    w_event(1, 0)
    conv_group(ROW_ORDER[1])
    conv_group(ROW_ORDER[2])
    w_event(1, 1)
    conv_group(ROW_ORDER[3])
    halo_copy.wait_recv()
    keep = (sp > 0).astype(F32)
    for c in range(NC):
        glu[c, 0:32, :] = halo_in[:, 128 * c : 128 * c + 128].astype(F32) * keep
    lax.fori_loop(0, NC, functools.partial(conv_chunk, 0, 1), 0)

    def norm_step(i, carry):
        rows = pl.ds(pl.multiple_of(i * 32, 32), 32)
        mu = jnp.broadcast_to(jnp.sum(mean_s[rows, :], axis=1, keepdims=True) * (1.0 / CH), (32, 128))
        squares = jnp.zeros((32, 128), F32)
        for c in range(NC):
            centered = conv[c, rows, :] - mu
            squares = squares + centered * centered
        inv = lax.rsqrt(jnp.sum(squares, axis=1, keepdims=True) * (1.0 / CH) + NORM_EPS)
        inv = jnp.broadcast_to(inv, (32, 128))
        mean_s[rows, :] = mu
        inv_s[rows, :] = inv
        for c in range(NC):
            lanes = slice(128 * c, 128 * c + 128)
            scaled = (conv[c, rows, :] - mu) * inv * gain_ref[:, lanes]
            act[rows, lanes] = (scaled * jax.nn.sigmoid(scaled)).astype(BF16)
        return carry

    act_copies = []

    def norm_part(at):
        lax.fori_loop(2 * at, 2 * at + 2, norm_step, 0)
        rows = pl.ds(64 * at, 64)
        act_copies.append(send(act.at[rows], actsib.at[rows], sibling))

    norm_part(0)
    norm_part(1)
    w_event(2, 0)
    norm_part(2)
    norm_part(3)
    axes = ((("sp_1", cx), ("sp_0", cy)), (("sp_0", cy), ("sp_1", cx)))

    def near(axis, d):
        name, at = axis
        return {name: lax.rem(at + d + 4, 4)}

    def part(axis, d):
        return lax.rem(axis[1] + d + 4, 4)

    def partial_sums(stage):
        lanes = slice(512 * stage, 512 * stage + 512)
        for k in range(NZ):
            lhs = ut[k]
            total = jnp.dot(lhs[:, 0:256], act[:, lanes], preferred_element_type=F32)
            total = total + jnp.dot(lhs[:, 256:512], actsib[:, lanes], preferred_element_type=F32)
            narrow = total.astype(BF16)
            for h in range(2):
                for p in range(4):
                    first = 64 * h + 16 * p
                    pbuf[stage, h, p, k] = narrow[first : first + 16, :]

    rs_copies = {}

    def rs1_send(stage):
        for h in range(2):
            axis = axes[h][0]
            far = part(axis, 2)
            for way, sign, lanes in ((0, 1, slice(0, 256)), (1, -1, slice(256, 512))):
                rs_copies[1, stage, h, way] = send(
                    pbuf.at[stage, h, far, :, :, lanes], r1.at[stage, h, way], near(axis, sign)
                )

    def rs1_mid(stage):
        for h in range(2):
            axis = axes[h][0]
            for way, sign, lanes in ((0, 1, slice(0, 256)), (1, -1, slice(256, 512))):
                rs_copies[1, stage, h, way].wait_recv()
                to = part(axis, sign)

                def add(k, carry, h=h, to=to, way=way, lanes=lanes):
                    pbuf[stage, h, to, k, :, lanes] = (
                        pbuf[stage, h, to, k, :, lanes].astype(F32) + r1[stage, h, way, k].astype(F32)
                    ).astype(BF16)
                    return carry

                lax.fori_loop(0, NZ, add, 0)
                rs_copies[2, stage, h, way] = send(
                    pbuf.at[stage, h, to], r2.at[stage, h, way], near(axis, sign)
                )

    def rs1_fin(stage):
        for h in range(2):
            mine = part(axes[h][0], 0)
            axis = axes[h][1]
            for way in (0, 1):
                rs_copies[2, stage, h, way].wait_recv()

            def add(k, carry, h=h, mine=mine):
                for p in range(4):
                    lanes = slice(128 * p, 128 * p + 128)
                    q[stage, h, p, k] = (
                        pbuf[stage, h, mine, k, :, lanes].astype(F32)
                        + r2[stage, h, 0, k, :, lanes].astype(F32)
                        + r2[stage, h, 1, k, :, lanes].astype(F32)
                    ).astype(BF16)
                return carry

            lax.fori_loop(0, NZ, add, 0)
            far = part(axis, 2)
            for way, sign in ((0, 1), (1, -1)):
                rs_copies[3, stage, h, way] = send(
                    q.at[stage, h, far, pl.ds(4 * way, 4)], s1.at[stage, h, way], near(axis, sign)
                )

    def rs2_mid(stage):
        for h in range(2):
            axis = axes[h][1]
            for way, sign in ((0, 1), (1, -1)):
                rs_copies[3, stage, h, way].wait_recv()
                to = part(axis, sign)
                for k in range(4):
                    q[stage, h, to, 4 * way + k] = (
                        q[stage, h, to, 4 * way + k].astype(F32) + s1[stage, h, way, k].astype(F32)
                    ).astype(BF16)
                rs_copies[4, stage, h, way] = send(
                    q.at[stage, h, to], s2.at[stage, h, way], near(axis, sign)
                )

    z_copies = {}

    def rs2_fin(stage):
        for h in range(2):
            mine = part(axes[h][1], 0)
            for way in (0, 1):
                rs_copies[4, stage, h, way].wait_recv()
            for k in range(NZ):
                vz[stage, k, h] = (
                    q[stage, h, mine, k].astype(F32)
                    + s2[stage, h, 0, k].astype(F32)
                    + s2[stage, h, 1, k].astype(F32)
                ).astype(BF16)
        for k in (4, 3, 5, 2, 6, 1, 7):
            z_copies[stage, k] = send(vz.at[stage, k], rz.at[stage, k], zdev(k))

    gather_copies = []

    def rs3(stage):
        total = vz[stage, 0].astype(F32)
        for k in range(1, NZ):
            z_copies[stage, k].wait_recv()
            total = total + rz[stage, k].astype(F32)
        fg[stage, sp] = total.astype(BF16)
        for d in range(1, 16):
            gather_copies.append(send(fg.at[stage, sp], fg.at[stage, sp], spdev(d)))

    def grad_block(rels, first=False):
        for rel in rels:
            w_pair[rel].wait_recv()
        lhs = []
        for rel in rels:
            zb = lax.rem(cz + rel, NZ)
            lhs.append(u_s[:, pl.ds(pl.multiple_of(zb * 256, 256), 256)])

        def step(n, carry):
            lanes = pl.ds(pl.multiple_of(n * 512, 512), 512)
            total = None
            for left, rel in zip(lhs, rels):
                right = wbuf[rel, :, :, lanes].reshape(256, 512)
                term = jnp.dot(left, right, preferred_element_type=F32)
                total = term if total is None else total + term
            if first:
                gacc[:, lanes] = total
            else:
                gacc[:, lanes] += total
            return carry

        lax.fori_loop(0, 4, step, 0)

    grad_block((0,), first=True)
    w_event(2, 1)
    w_share(1)
    w_share(7)
    for copy in act_copies:
        copy.wait_recv()
    partial_sums(0)
    rs1_send(0)
    partial_sums(1)
    rs1_send(1)
    w_rest(2, 0)
    partial_sums(2)
    rs1_send(2)
    partial_sums(3)
    rs1_send(3)
    w_event(3, 0)
    w_rest(2, 1)
    rs1_mid(0)
    w_event(3, 1)
    w_share(2)
    w_share(6)
    rs1_mid(1)
    grad_block((1, 7))
    w_rest(3, 0)
    grad_block((2, 6))
    w_rest(3, 1)
    w_share(3)
    w_share(5)
    rs1_fin(0)
    rs1_mid(2)
    grad_block((3, 5))
    rs1_fin(1)
    rs1_mid(3)
    rs2_mid(0)
    w_event(4, 0)
    w_event(4, 1)
    w_rest(4, 0)
    w_rest(4, 1)
    w_share(4)
    rs1_fin(2)
    rs2_mid(1)
    grad_block((4,))

    dn[...] = jnp.zeros_like(dn)

    def back_rows(r):
        rows = pl.ds(r, 32)
        mu = mean_s[rows, :]
        inv = inv_s[rows, :]
        sum1 = jnp.zeros((32, 128), F32)
        sum2 = jnp.zeros((32, 128), F32)
        for c in range(NC):
            lanes = slice(128 * c, 128 * c + 128)
            gain = gain_ref[:, lanes]
            normed = (conv[c, rows, :] - mu) * inv
            scaled = normed * gain
            sig = jax.nn.sigmoid(scaled)
            grad_scaled = gacc[rows, lanes] * sig * (1.0 + scaled * (1.0 - sig))
            gain_term = grad_scaled * normed
            dn[c] += (gain_term[0:8] + gain_term[8:16]) + (gain_term[16:24] + gain_term[24:32])
            grad_normed = grad_scaled * gain
            gacc[rows, lanes] = grad_normed
            sum1 = sum1 + grad_normed
            sum2 = sum2 + grad_normed * normed
        m1 = jnp.broadcast_to(jnp.sum(sum1, axis=1, keepdims=True) * (1.0 / CH), (32, 128))
        m2 = jnp.broadcast_to(jnp.sum(sum2, axis=1, keepdims=True) * (1.0 / CH), (32, 128))
        for c in range(NC):
            lanes = slice(128 * c, 128 * c + 128)
            normed = (conv[c, rows, :] - mu) * inv
            narrow = (inv * (gacc[rows, lanes] - m1 - normed * m2)).astype(BF16)
            gpad[c, rows, :] = narrow.astype(F32)
            yield lanes, narrow

    for lanes, narrow in back_rows(0):
        ghalo_out[:, lanes] = narrow
    ghalo_copy = send(ghalo_out, ghalo_in, spdev(-1))

    def back_step(i, carry):
        for _ in back_rows(pl.multiple_of(i * 32, 32)):
            pass
        return carry

    lax.fori_loop(1, TOK // 32, back_step, 0)

    def rest_of_plane(d):
        return lax.rem(sp + d, 16)

    gain_copies = [send(dn.at[rest_of_plane(d)], dr.at[d], spdev(d)) for d in range(1, 16)]

    def gain_sum():
        total = dn[sp]
        for d in range(1, 16):
            gain_copies[d - 1].wait_recv()
            total = total + dr[d]
        dz[cz] = total
        return [send(dz.at[cz], dz.at[cz], zdev(d)) for d in range(1, NZ)]

    def gain_pair(copies):
        for copy in copies:
            copy.wait_recv()
        total = dz[0]
        for k in range(1, NZ):
            total = total + dz[k]
        dfin[...] = total
        return send(dfin, dsib, sibling)

    def gain_out(copy):
        copy.wait_recv()
        gfull[sp] = dfin[...] + dsib[...]
        return [send(gfull.at[sp], gfull.at[sp], spdev(d)) for d in range(1, 16)]

    def taps_chunk(c, carry):
        def rows_step(i, sums):
            sums = list(sums)
            base = pl.multiple_of(i * 64, 64)
            g = [gpad[c, pl.ds(base + 8 * k, 8), :] for k in range(8)]
            for o in range(8 * 7 + TAPS):
                x = glu[c, pl.ds(base + 2 + o, 8), :]
                for k in range(8):
                    j = o - 8 * k
                    if 0 <= j < TAPS:
                        sums[j] = sums[j] + g[k] * x
            return tuple(sums)

        sums = lax.fori_loop(0, TOK // 64, rows_step, tuple(jnp.zeros((8, 128), F32) for _ in range(TAPS)))
        rows = [jnp.sum(total, axis=0, keepdims=True) for total in sums] + [jnp.zeros((1, 128), F32)]
        tg[c] = jnp.concatenate(rows, axis=0).astype(BF16)
        return carry

    part_copies = []

    def taps_group(dy):
        row = lax.rem(cy + dy, 4)
        lax.fori_loop(4 * row, 4 * row + 4, taps_chunk, 0)
        for dx in range(4):
            if dx or dy:
                x = lax.rem(cx + dx, 4)
                part_copies.append(
                    send(tg.at[4 * row + x], tr.at[4 * dy + dx], {"sp_0": row, "sp_1": x})
                )

    rs2_fin(0)
    taps_group(2)
    rs1_fin(3)
    rs2_mid(2)
    taps_group(1)
    rs2_fin(1)
    taps_group(3)
    rs2_mid(3)
    rs2_fin(2)
    gain_z = gain_sum()
    taps_group(0)
    rs3(0)
    rs2_fin(3)

    ghalo_copy.wait_recv()
    keep_g = (sp < 15).astype(F32)
    for c in range(NC):
        gpad[c, TOK:, :] = ghalo_in[:, 128 * c : 128 * c + 128].astype(F32) * keep_g

    def grad_chunk(c, carry):
        taps = [jnp.broadcast_to(tapsb[c, j : j + 1, :], (8, 128)) for j in reversed(range(TAPS))]
        lanes = pl.ds(pl.multiple_of(c * 128, 128), 128)

        def rows_step(i, carry):
            base = pl.multiple_of(i * 64, 64)
            values, gates = [], []
            for k, total in correlate(taps, lambda o: gpad[c, pl.ds(base + o, 8), :]):
                total = total.astype(BF16).astype(F32)
                values.append(total * gate_a[c, pl.ds(base + 8 * k, 8), :])
                gates.append(total * gate_b[c, pl.ds(base + 8 * k, 8), :])
                if k % 2:
                    rows = pl.ds(base + 8 * k - 8, 16)
                    gv_s[rows, lanes] = jnp.concatenate(values, axis=0).astype(BF16)
                    gt_s[rows, lanes] = jnp.concatenate(gates, axis=0).astype(BF16)
                    values, gates = [], []
            return carry

        return lax.fori_loop(0, TOK // 64, rows_step, carry)

    stores = []

    def grad_group(at):
        lax.fori_loop(4 * at, 4 * at + 4, grad_chunk, 0)
        lanes = pl.ds(512 * at, 512)
        for narrow, wide in ((gv_s, gv_hbm), (gt_s, gt_hbm)):
            copy = pltpu.make_async_copy(
                narrow.at[:, lanes], wide.at[0, :, lanes], local_sem.at[4 + len(stores)]
            )
            copy.start()
            stores.append(copy)

    grad_group(0)
    rs3(1)
    grad_group(1)
    rs3(2)
    gain_last = gain_pair(gain_z)
    total = tg[sp].astype(F32)
    for copy in part_copies:
        copy.wait_recv()
    for d in range(1, 16):
        total = total + tr[d].astype(F32)
    tz[cz] = total
    tz_copies = [send(tz.at[cz], tz.at[cz], zdev(d)) for d in range(1, NZ)]
    rs3(3)
    grad_group(2)
    gain_copies2 = gain_out(gain_last)
    grad_group(3)

    for copy in tz_copies:
        copy.wait_recv()
    total = tz[0]
    for k in range(1, NZ):
        total = total + tz[k]
    tfin[...] = total
    pair_copy = send(tfin, tsib, sibling)

    for copy in gather_copies:
        copy.wait_recv()
    for s in range(16):
        y, x = divmod(s, 4)
        for t in range(NS):
            lane = 512 * t + 128 * y
            gw_ref[16 * x : 16 * x + 16, lane : lane + 128] = fg[t, s, 0]
            lane = 512 * t + 128 * x
            gw_ref[64 + 16 * y : 80 + 16 * y, lane : lane + 128] = fg[t, s, 1]
    def store(held, target):
        copy = pltpu.make_async_copy(held, target, local_sem.at[14 + len(stores) - 8])
        copy.start()
        stores.append(copy)

    store(gw_ref, gw_hbm)
    for copy in gain_copies2:
        copy.wait_recv()
    for c in range(NC):
        dn_ref[:, 128 * c : 128 * c + 128] = jnp.sum(gfull[c], axis=0, keepdims=True)
    store(dn_ref, dn_hbm)
    pair_copy.wait_recv()
    dt_ref[...] = (tfin[...] + tsib[...])[:TAPS]
    store(dt_ref, dt_hbm)
    for copy in stores:
        copy.wait()
    for copy in started:
        copy.wait_send()


def write_out(gv, gt, gw, dt, dn, gv_out, gt_out, gw_out, dt_out, dn_out, gv_s, gt_s, gw_s, gw_wide, dt_s, dn_s, sem):
    copies = []
    for i, (source, held, target) in enumerate(
        ((gw, gw_s, gw_out), (gv, gv_s, gv_out), (gt, gt_s, gt_out), (dt, dt_s, dt_out), (dn, dn_s, dn_out))
    ):
        copy = pltpu.make_async_copy(source, held, sem.at[0, i])
        copy.start()
        copies.append((copy, held, target))
    outs = []
    for i, (copy, held, target) in enumerate(copies):
        copy.wait()
        if i == 0:
            gw_wide[...] = gw_s[...].astype(F32)
            held = gw_wide
        out = pltpu.make_async_copy(held, target, sem.at[1, i])
        out.start()
        outs.append(out)
    for out in outs:
        out.wait()


def body(value_half, gate_half, upstream, conv_taps, norm_gain, out_weight):
    hbm = pl.BlockSpec(memory_space=pl.ANY)
    grad_value, grad_gate, grad_rows, taps, gain = pl.pallas_call(
        kernel,
        out_shape=(
            jax.ShapeDtypeStruct((1, TOK, CH), BF16),
            jax.ShapeDtypeStruct((1, TOK, CH), BF16),
            jax.ShapeDtypeStruct((128, CH), BF16),
            jax.ShapeDtypeStruct((TAPS, 128), F32),
            jax.ShapeDtypeStruct((1, CH), F32),
        ),
        in_specs=[hbm] * 6,
        out_specs=[hbm] * 5,
        scratch_shapes=[
            pltpu.VMEM((1, CH), F32),
            pltpu.VMEM((128, CH), BF16),
            pltpu.VMEM((TAPS, 128), F32),
            pltpu.VMEM((1, CH), F32),
            pltpu.VMEM((TOK, CH), BF16),
            pltpu.VMEM((TOK, CH), BF16),
            pltpu.VMEM((TOK, CH), BF16),
            pltpu.VMEM((TOK, CH), BF16),
            pltpu.VMEM((NZ, 2, 128, CH), BF16),
            pltpu.VMEM((NC, 32, 128), F32),
            pltpu.VMEM((NC, TOK + 32, 128), F32),
            pltpu.VMEM((NC, TOK, 128), F32),
            pltpu.VMEM((TOK, CH), BF16),
            pltpu.VMEM((TOK, CH), BF16),
            pltpu.VMEM((NZ, 128, 512), BF16),
            pltpu.VMEM((NS, 2, 4, NZ, 16, 512), BF16),
            pltpu.VMEM((NS, 2, 2, NZ, 16, 256), BF16),
            pltpu.VMEM((NS, 2, 2, NZ, 16, 512), BF16),
            pltpu.VMEM((NS, 2, 4, NZ, 16, 128), BF16),
            pltpu.VMEM((NS, 2, 2, 4, 16, 128), BF16),
            pltpu.VMEM((NS, 2, 2, NZ, 16, 128), BF16),
            pltpu.VMEM((NS, NZ, 2, 16, 128), BF16),
            pltpu.VMEM((NS, NZ, 2, 16, 128), BF16),
            pltpu.VMEM((NS, 16, 2, 16, 128), BF16),
            pltpu.VMEM((TOK, CH), F32),
            pltpu.VMEM((NC, TOK + 32, 128), F32),
            pltpu.VMEM((TOK, 128), F32),
            pltpu.VMEM((TOK, 128), F32),
            pltpu.VMEM((NC, TOK, 128), F32),
            pltpu.VMEM((NC, TOK, 128), F32),
            pltpu.VMEM((TOK, CH), BF16),
            pltpu.VMEM((TOK, CH), BF16),
            pltpu.VMEM((32, CH), BF16),
            pltpu.VMEM((32, CH), BF16),
            pltpu.VMEM((32, CH), BF16),
            pltpu.VMEM((32, CH), BF16),
            pltpu.VMEM((NC, 8, 128), F32),
            pltpu.VMEM((NC, 32, 128), BF16),
            pltpu.VMEM((16, 32, 128), BF16),
            pltpu.VMEM((NZ, 32, 128), F32),
            pltpu.VMEM((32, 128), F32),
            pltpu.VMEM((32, 128), F32),
            pltpu.VMEM((16, 8, 128), F32),
            pltpu.VMEM((16, 8, 128), F32),
            pltpu.VMEM((NZ, 8, 128), F32),
            pltpu.VMEM((8, 128), F32),
            pltpu.VMEM((8, 128), F32),
            pltpu.SemaphoreType.DMA((17,)),
            pltpu.SemaphoreType.DMA((N_SEND,)),
            pltpu.SemaphoreType.DMA((N_SEND,)),
        ],
        compiler_params=pltpu.CompilerParams(
            collective_id=0, has_side_effects=True, vmem_limit_bytes=66_000_000
        ),
    )(value_half, gate_half, upstream, out_weight, conv_taps, norm_gain[None])
    grad_value, grad_gate, grad_rows, taps, gain = pl.pallas_call(
        write_out,
        out_shape=(
            jax.ShapeDtypeStruct((1, TOK, CH), BF16),
            jax.ShapeDtypeStruct((1, TOK, CH), BF16),
            jax.ShapeDtypeStruct((128, CH), F32),
            jax.ShapeDtypeStruct((TAPS, 128), F32),
            jax.ShapeDtypeStruct((1, CH), F32),
        ),
        in_specs=[hbm] * 5,
        out_specs=[hbm] * 5,
        scratch_shapes=[
            pltpu.VMEM((1, TOK, CH), BF16),
            pltpu.VMEM((1, TOK, CH), BF16),
            pltpu.VMEM((128, CH), BF16),
            pltpu.VMEM((128, CH), F32),
            pltpu.VMEM((TAPS, 128), F32),
            pltpu.VMEM((1, CH), F32),
            pltpu.SemaphoreType.DMA((2, 5)),
        ],
        compiler_params=pltpu.CompilerParams(vmem_limit_bytes=60_000_000),
    )(grad_value, grad_gate, grad_rows, taps, gain)
    return grad_value, grad_gate, taps, gain.reshape(CH), grad_rows


def solution(mesh):
    torus = Mesh(mesh.devices.reshape(4, 4, 8, 2), ("sp_0", "sp_1", "dp_0", "dp_1"))
    placed = (P(DP, SP, None), P(DP, SP, None), P(DP, SP, None), P(None, SP), P(), P(DP, None))
    return jax.shard_map(
        body,
        mesh=torus,
        in_specs=placed,
        out_specs=(P(DP, SP, None), P(DP, SP, None), P(None, SP), P(), P(DP, None)),
        check_vma=False,
    )
```

```python
import functools

import jax
import jax.numpy as jnp
from jax import lax
from jax.experimental import pallas as pl
from jax.experimental.pallas import tpu as pltpu
from jax.sharding import Mesh
from jax.sharding import PartitionSpec as P

DP = ("dp_0", "dp_1")
SP = ("sp_0", "sp_1")
NORM_EPS = 1e-05
MESH = pl.DeviceIdType.MESH
F32 = jnp.float32
BF16 = jnp.bfloat16

TOK = 256
CH = 2048
NC = CH // 128
TAPS = 31
ROW_ORDER = (0, 1, 3, 2)
NZ = 8
NS = 4
N_SEND = 320


def kernel(
    v_hbm, g_hbm, u_hbm, w_hbm, taps_hbm, gain_hbm,
    gv_hbm, gt_hbm, gw_hbm, dt_hbm, dn_hbm,
    gain_ref, gw_ref, dt_ref, dn_ref,
    v_s, g_s, u_s, usib, wbuf, tapsb, glu, conv, act, actsib, ut,
    pbuf, r1, r2, q, s1, s2, vz, rz, fg, gacc, gpad, mean_s, inv_s, gate_a, gate_b, gv_s, gt_s,
    halo_out, halo_in, ghalo_out, ghalo_in, dn, tg, tr, tz, tsib, tfin, gfull, dr, dz, dfin, dsib,
    local_sem, send_sem, recv_sem,
):
    cy, cx, cz, cc = (lax.axis_index(a) for a in ("sp_0", "sp_1", "dp_0", "dp_1"))
    sp = cy * 4 + cx
    other = 1 - cc
    sibling = {"dp_1": other}

    def zdev(d):
        return {"dp_0": lax.rem(cz + d + NZ, NZ)}

    def spdev(d):
        s = lax.rem(sp + d + 16, 16)
        return {"sp_0": s // 4, "sp_1": lax.rem(s, 4)}

    used = [0]
    started = []

    def send(src, dst, device):
        i = used[0]
        used[0] += 1
        copy = pltpu.make_async_remote_copy(
            src_ref=src, dst_ref=dst, send_sem=send_sem.at[i], recv_sem=recv_sem.at[i],
            device_id=device, device_id_type=MESH,
        )
        copy.start()
        started.append(copy)
        return copy

    loads = [
        pltpu.make_async_copy(w_hbm, wbuf.at[0, cc], local_sem.at[0]),
        pltpu.make_async_copy(v_hbm.at[0], v_s, local_sem.at[1]),
        pltpu.make_async_copy(g_hbm.at[0], g_s, local_sem.at[2]),
        pltpu.make_async_copy(u_hbm.at[0], u_s, local_sem.at[3]),
        pltpu.make_async_copy(taps_hbm, tapsb.at[sp, pl.ds(0, TAPS)], local_sem.at[12]),
        pltpu.make_async_copy(gain_hbm, gain_ref, local_sem.at[13]),
    ]
    for at in (1, 2, 4, 5, 0, 3):
        loads[at].start()

    barrier = pltpu.get_barrier_semaphore()
    pl.semaphore_signal(barrier, inc=1, device_id=sibling, device_id_type=MESH)
    for d in range(1, NZ):
        pl.semaphore_signal(barrier, inc=1, device_id=zdev(d), device_id_type=MESH)
    for d in range(1, 16):
        pl.semaphore_signal(barrier, inc=1, device_id=spdev(d), device_id_type=MESH)

    for load in loads[1:3]:
        load.wait()
    def glu_rows(r):
        rows = pl.ds(r, 32)
        for c in range(NC):
            lanes = slice(128 * c, 128 * c + 128)
            value = v_s[rows, lanes].astype(F32)
            sig = jax.nn.sigmoid(g_s[rows, lanes].astype(F32))
            wide = value * sig
            gate_a[c, rows, :] = sig
            gate_b[c, rows, :] = wide * (1.0 - sig)
            narrow = wide.astype(BF16)
            glu[c, pl.ds(r + 32, 32), :] = narrow.astype(F32)
            yield lanes, narrow

    for lanes, narrow in glu_rows(TOK - 32):
        halo_out[:, lanes] = narrow

    def glu_step(i, carry):
        for _ in glu_rows(pl.multiple_of(i * 32, 32)):
            pass
        return carry

    lax.fori_loop(0, TOK // 32 - 1, glu_step, 0)

    for load in loads[3:]:
        load.wait()
    tapsb[sp, TAPS:] = jnp.zeros((1, 128), F32)
    loads[0].wait()
    pl.semaphore_wait(barrier, 23)

    parity = lax.rem(cy + cx, 2)
    w_copies = {}
    w_quarters = {}
    w_pair = {}

    def arrived(copies, key):
        copy = copies.pop(key, None)
        if copy is not None:
            copy.wait_recv()

    def w_send(half, step, sub):
        at = parity if half == 0 else 1 - parity
        rows = pl.ds(pl.multiple_of(64 * at + 32 * sub, 32), 32)
        lanes = (slice(0, 1024), slice(1024, 2048)) if step == 4 else (slice(None), slice(None))
        for way, sign in ((0, 1), (1, -1)):
            src = (-sign * (step - 1)) % NZ
            dst = (-sign * step) % NZ
            w_copies[half, step, sub, way] = send(
                wbuf.at[src, cc, rows, lanes[way]], wbuf.at[dst, cc, rows, lanes[way]], zdev(sign)
            )

    def w_share(rels, half, sub):
        at = parity if half == 0 else 1 - parity
        rows = pl.ds(pl.multiple_of(64 * at + 32 * sub, 32), 32)
        for rel in rels:
            w_pair.setdefault(rel, []).append(send(wbuf.at[rel, cc, rows], wbuf.at[rel, cc, rows], sibling))

    def blocks_at(step):
        return sorted({step, NZ - step})

    def w_event(step, sub):
        for way in (0, 1):
            arrived(w_copies, (0, step, sub, way))
        if step < 4:
            w_send(0, step + 1, sub)
        name, at = (("sp_1", cx), ("sp_0", cy))[sub]
        if step < 3:
            for rel in (step, NZ - step):
                for turn, sign in ((2 * sub, 1), (2 * sub + 1, -1)):
                    rows = pl.ds(pl.multiple_of(64 * parity + 16 * turn, 16), 16)
                    w_quarters[rel, turn] = send(
                        wbuf.at[rel, cc, rows], wbuf.at[rel, cc, rows], {name: lax.rem(at + sign + 4, 4)}
                    )
        w_share(blocks_at(step), 0, sub)

    def w_rest(step, sub):
        if step < 3:
            for rel in blocks_at(step):
                for turn in (2 * sub, 2 * sub + 1):
                    arrived(w_quarters, (rel, turn))
        else:
            for way in (0, 1):
                arrived(w_copies, (1, step, sub, way))
        if step in (2, 3):
            w_send(1, step + 1, sub)
        w_share(blocks_at(step), 1, sub)

    taps_copies = {
        dy: [
            send(tapsb.at[sp], tapsb.at[sp], {"sp_0": lax.rem(cy + dy, 4), "sp_1": lax.rem(cx + dx, 4)})
            for dx in range(4)
            if dx or dy
        ]
        for dy in ROW_ORDER
    }
    w_send(0, 1, 0)
    w_send(0, 1, 1)
    halo_copy = send(halo_out, halo_in, spdev(1))
    u_copy = send(u_s, usib, sibling)
    w_pair[0] = [send(wbuf.at[0, cc], wbuf.at[0, cc], sibling)]

    u_copy.wait_recv()

    def transpose_step(k, carry):
        zb = lax.rem(cz + k, NZ)
        cols = pl.ds(pl.multiple_of(zb * 256 + cc * 128, 128), 128)
        ut[k, :, 0:256] = u_s[:, cols].T
        ut[k, :, 256:512] = usib[:, cols].T
        return carry

    lax.fori_loop(0, NZ, transpose_step, 0)

    def correlate(taps, read):
        sums = {}
        for o in range(8 * 7 + TAPS):
            x = read(o)
            for k in range(8):
                j = o - 8 * k
                if 0 <= j < TAPS:
                    term = taps[j] * x
                    key = k, j % 2
                    sums[key] = sums[key] + term if key in sums else term
                    if j == TAPS - 1:
                        yield k, sums.pop((k, 0)) + sums.pop((k, 1))

    mean_s[...] = jnp.zeros_like(mean_s)

    def conv_chunk(first, last, c, carry):
        taps = [jnp.broadcast_to(tapsb[c, j : j + 1, :], (8, 128)) for j in range(TAPS)]

        def rows_step(i, carry):
            base = pl.multiple_of(i * 64, 64)
            for k, total in correlate(taps, lambda o: glu[c, pl.ds(base + 2 + o, 8), :]):
                total = total.astype(BF16).astype(F32)
                conv[c, pl.ds(base + 8 * k, 8), :] = total
                mean_s[pl.ds(base + 8 * k, 8), :] += total
            return carry

        return lax.fori_loop(first, last, rows_step, carry)

    body_rows = functools.partial(conv_chunk, 1, TOK // 64)

    def conv_group(dy):
        for copy in taps_copies[dy]:
            copy.wait_recv()
        row = lax.rem(cy - dy + 4, 4)
        lax.fori_loop(4 * row, 4 * row + 4, body_rows, 0)

    conv_group(ROW_ORDER[0])
    w_event(1, 0)
    conv_group(ROW_ORDER[1])
    conv_group(ROW_ORDER[2])
    w_event(1, 1)
    conv_group(ROW_ORDER[3])
    halo_copy.wait_recv()
    keep = (sp > 0).astype(F32)
    for c in range(NC):
        glu[c, 0:32, :] = halo_in[:, 128 * c : 128 * c + 128].astype(F32) * keep
    lax.fori_loop(0, NC, functools.partial(conv_chunk, 0, 1), 0)

    def norm_step(i, carry):
        rows = pl.ds(pl.multiple_of(i * 32, 32), 32)
        mu = jnp.broadcast_to(jnp.sum(mean_s[rows, :], axis=1, keepdims=True) * (1.0 / CH), (32, 128))
        squares = jnp.zeros((32, 128), F32)
        for c in range(NC):
            centered = conv[c, rows, :] - mu
            squares = squares + centered * centered
        inv = lax.rsqrt(jnp.sum(squares, axis=1, keepdims=True) * (1.0 / CH) + NORM_EPS)
        inv = jnp.broadcast_to(inv, (32, 128))
        mean_s[rows, :] = mu
        inv_s[rows, :] = inv
        for c in range(NC):
            lanes = slice(128 * c, 128 * c + 128)
            scaled = (conv[c, rows, :] - mu) * inv * gain_ref[:, lanes]
            act[rows, lanes] = (scaled * jax.nn.sigmoid(scaled)).astype(BF16)
        return carry

    act_copies = []

    def norm_part(at):
        lax.fori_loop(2 * at, 2 * at + 2, norm_step, 0)
        rows = pl.ds(64 * at, 64)
        act_copies.append(send(act.at[rows], actsib.at[rows], sibling))

    norm_part(0)
    norm_part(1)
    w_event(2, 0)
    norm_part(2)
    norm_part(3)
    axes = ((("sp_1", cx), ("sp_0", cy)), (("sp_0", cy), ("sp_1", cx)))

    def near(axis, d):
        name, at = axis
        return {name: lax.rem(at + d + 4, 4)}

    def part(axis, d):
        return lax.rem(axis[1] + d + 4, 4)

    def partial_sums(stage):
        lanes = slice(512 * stage, 512 * stage + 512)
        for k in range(NZ):
            lhs = ut[k]
            total = jnp.dot(lhs[:, 0:256], act[:, lanes], preferred_element_type=F32)
            total = total + jnp.dot(lhs[:, 256:512], actsib[:, lanes], preferred_element_type=F32)
            narrow = total.astype(BF16)
            for h in range(2):
                for p in range(4):
                    first = 64 * h + 16 * p
                    pbuf[stage, h, p, k] = narrow[first : first + 16, :]

    rs_copies = {}

    def rs1_send(stage):
        for h in range(2):
            axis = axes[h][0]
            far = part(axis, 2)
            for way, sign, lanes in ((0, 1, slice(0, 256)), (1, -1, slice(256, 512))):
                rs_copies[1, stage, h, way] = send(
                    pbuf.at[stage, h, far, :, :, lanes], r1.at[stage, h, way], near(axis, sign)
                )

    def rs1_mid(stage):
        for h in range(2):
            axis = axes[h][0]
            for way, sign, lanes in ((0, 1, slice(0, 256)), (1, -1, slice(256, 512))):
                rs_copies[1, stage, h, way].wait_recv()
                to = part(axis, sign)

                def add(k, carry, h=h, to=to, way=way, lanes=lanes):
                    pbuf[stage, h, to, k, :, lanes] = (
                        pbuf[stage, h, to, k, :, lanes].astype(F32) + r1[stage, h, way, k].astype(F32)
                    ).astype(BF16)
                    return carry

                lax.fori_loop(0, NZ, add, 0)
                rs_copies[2, stage, h, way] = send(
                    pbuf.at[stage, h, to], r2.at[stage, h, way], near(axis, sign)
                )

    def rs1_fin(stage):
        for h in range(2):
            mine = part(axes[h][0], 0)
            axis = axes[h][1]
            for way in (0, 1):
                rs_copies[2, stage, h, way].wait_recv()

            def add(k, carry, h=h, mine=mine):
                for p in range(4):
                    lanes = slice(128 * p, 128 * p + 128)
                    q[stage, h, p, k] = (
                        pbuf[stage, h, mine, k, :, lanes].astype(F32)
                        + r2[stage, h, 0, k, :, lanes].astype(F32)
                        + r2[stage, h, 1, k, :, lanes].astype(F32)
                    ).astype(BF16)
                return carry

            lax.fori_loop(0, NZ, add, 0)
            far = part(axis, 2)
            for way, sign in ((0, 1), (1, -1)):
                rs_copies[3, stage, h, way] = send(
                    q.at[stage, h, far, pl.ds(4 * way, 4)], s1.at[stage, h, way], near(axis, sign)
                )

    def rs2_mid(stage):
        for h in range(2):
            axis = axes[h][1]
            for way, sign in ((0, 1), (1, -1)):
                rs_copies[3, stage, h, way].wait_recv()
                to = part(axis, sign)
                for k in range(4):
                    q[stage, h, to, 4 * way + k] = (
                        q[stage, h, to, 4 * way + k].astype(F32) + s1[stage, h, way, k].astype(F32)
                    ).astype(BF16)
                rs_copies[4, stage, h, way] = send(
                    q.at[stage, h, to], s2.at[stage, h, way], near(axis, sign)
                )

    z_copies = {}

    def rs2_fin(stage):
        for h in range(2):
            mine = part(axes[h][1], 0)
            for way in (0, 1):
                rs_copies[4, stage, h, way].wait_recv()
            for k in range(NZ):
                vz[stage, k, h] = (
                    q[stage, h, mine, k].astype(F32)
                    + s2[stage, h, 0, k].astype(F32)
                    + s2[stage, h, 1, k].astype(F32)
                ).astype(BF16)
        for k in (4, 3, 5, 2, 6, 1, 7):
            z_copies[stage, k] = send(vz.at[stage, k], rz.at[stage, k], zdev(k))

    gather_copies = []

    def rs3(stage):
        total = vz[stage, 0].astype(F32)
        for k in range(1, NZ):
            z_copies[stage, k].wait_recv()
            total = total + rz[stage, k].astype(F32)
        fg[stage, sp] = total.astype(BF16)
        for d in range(1, 16):
            gather_copies.append(send(fg.at[stage, sp], fg.at[stage, sp], spdev(d)))

    def grad_block(rels, first=False):
        for rel in rels:
            for copy in w_pair[rel]:
                copy.wait_recv()
        lhs = []
        for rel in rels:
            zb = lax.rem(cz + rel, NZ)
            lhs.append(u_s[:, pl.ds(pl.multiple_of(zb * 256, 256), 256)])

        def step(n, carry):
            lanes = pl.ds(pl.multiple_of(n * 512, 512), 512)
            total = None
            for left, rel in zip(lhs, rels):
                right = wbuf[rel, :, :, lanes].reshape(256, 512)
                term = jnp.dot(left, right, preferred_element_type=F32)
                total = term if total is None else total + term
            if first:
                gacc[:, lanes] = total
            else:
                gacc[:, lanes] += total
            return carry

        lax.fori_loop(0, 4, step, 0)

    grad_block((0,), first=True)
    w_event(2, 1)
    w_rest(1, 0)
    w_rest(1, 1)
    for copy in act_copies:
        copy.wait_recv()
    partial_sums(0)
    rs1_send(0)
    partial_sums(1)
    rs1_send(1)
    w_rest(2, 0)
    partial_sums(2)
    rs1_send(2)
    partial_sums(3)
    rs1_send(3)
    w_event(3, 0)
    w_rest(2, 1)
    rs1_mid(0)
    w_event(3, 1)
    rs1_mid(1)
    grad_block((1, 7))
    w_rest(3, 0)
    grad_block((2, 6))
    w_event(4, 0)
    w_rest(3, 1)
    rs1_fin(0)
    rs1_mid(2)
    w_event(4, 1)
    grad_block((3, 5))
    w_rest(4, 0)
    w_rest(4, 1)
    rs1_fin(1)
    rs1_mid(3)
    rs2_mid(0)
    grad_block((4,))
    rs1_fin(2)
    rs2_mid(1)

    dn[...] = jnp.zeros_like(dn)

    def back_rows(r):
        rows = pl.ds(r, 32)
        mu = mean_s[rows, :]
        inv = inv_s[rows, :]
        sum1 = jnp.zeros((32, 128), F32)
        sum2 = jnp.zeros((32, 128), F32)
        for c in range(NC):
            lanes = slice(128 * c, 128 * c + 128)
            gain = gain_ref[:, lanes]
            normed = (conv[c, rows, :] - mu) * inv
            scaled = normed * gain
            sig = jax.nn.sigmoid(scaled)
            grad_scaled = gacc[rows, lanes] * sig * (1.0 + scaled * (1.0 - sig))
            gain_term = grad_scaled * normed
            dn[c] += (gain_term[0:8] + gain_term[8:16]) + (gain_term[16:24] + gain_term[24:32])
            grad_normed = grad_scaled * gain
            gacc[rows, lanes] = grad_normed
            sum1 = sum1 + grad_normed
            sum2 = sum2 + grad_normed * normed
        m1 = jnp.broadcast_to(jnp.sum(sum1, axis=1, keepdims=True) * (1.0 / CH), (32, 128))
        m2 = jnp.broadcast_to(jnp.sum(sum2, axis=1, keepdims=True) * (1.0 / CH), (32, 128))
        for c in range(NC):
            lanes = slice(128 * c, 128 * c + 128)
            normed = (conv[c, rows, :] - mu) * inv
            narrow = (inv * (gacc[rows, lanes] - m1 - normed * m2)).astype(BF16)
            gpad[c, rows, :] = narrow.astype(F32)
            yield lanes, narrow

    for lanes, narrow in back_rows(0):
        ghalo_out[:, lanes] = narrow

    def back_step(i, carry):
        for _ in back_rows(pl.multiple_of(i * 32, 32)):
            pass
        return carry

    lax.fori_loop(1, TOK // 32, back_step, 0)

    def rest_of_plane(d):
        return lax.rem(sp + d, 16)

    gain_copies = [send(dn.at[rest_of_plane(d)], dr.at[d], spdev(d)) for d in range(1, 16)]

    def gain_sum():
        total = dn[sp]
        for d in range(1, 16):
            gain_copies[d - 1].wait_recv()
            total = total + dr[d]
        dz[cz] = total
        return [send(dz.at[cz], dz.at[cz], zdev(d)) for d in range(1, NZ)]

    def gain_pair(copies):
        for copy in copies:
            copy.wait_recv()
        total = dz[0]
        for k in range(1, NZ):
            total = total + dz[k]
        dfin[...] = total
        return send(dfin, dsib, sibling)

    def gain_out(copy):
        copy.wait_recv()
        gfull[sp] = dfin[...] + dsib[...]
        return [send(gfull.at[sp], gfull.at[sp], spdev(d)) for d in range(1, 16)]

    def taps_chunk(c, carry):
        def rows_step(i, sums):
            sums = list(sums)
            base = pl.multiple_of(i * 64, 64)
            g = [gpad[c, pl.ds(base + 8 * k, 8), :] for k in range(8)]
            for o in range(8 * 7 + TAPS):
                x = glu[c, pl.ds(base + 2 + o, 8), :]
                for k in range(8):
                    j = o - 8 * k
                    if 0 <= j < TAPS:
                        sums[j] = sums[j] + g[k] * x
            return tuple(sums)

        sums = lax.fori_loop(0, TOK // 64, rows_step, tuple(jnp.zeros((8, 128), F32) for _ in range(TAPS)))
        rows = [jnp.sum(total, axis=0, keepdims=True) for total in sums] + [jnp.zeros((1, 128), F32)]
        tg[c] = jnp.concatenate(rows, axis=0).astype(BF16)
        return carry

    part_copies = []

    def taps_group(dy):
        row = lax.rem(cy + dy, 4)
        lax.fori_loop(4 * row, 4 * row + 4, taps_chunk, 0)
        for dx in range(4):
            if dx or dy:
                x = lax.rem(cx + dx, 4)
                part_copies.append(
                    send(tg.at[4 * row + x], tr.at[4 * dy + dx], {"sp_0": row, "sp_1": x})
                )

    rs2_fin(0)
    rs1_fin(3)
    ghalo_copy = send(ghalo_out, ghalo_in, spdev(-1))
    taps_group(2)
    rs2_mid(2)
    rs2_fin(1)
    taps_group(1)
    rs2_mid(3)
    gain_z = gain_sum()
    taps_group(3)
    rs2_fin(2)
    taps_group(0)
    rs3(0)
    rs2_fin(3)

    ghalo_copy.wait_recv()
    keep_g = (sp < 15).astype(F32)
    for c in range(NC):
        gpad[c, TOK:, :] = ghalo_in[:, 128 * c : 128 * c + 128].astype(F32) * keep_g

    def grad_chunk(c, carry):
        taps = [jnp.broadcast_to(tapsb[c, j : j + 1, :], (8, 128)) for j in reversed(range(TAPS))]
        lanes = pl.ds(pl.multiple_of(c * 128, 128), 128)

        def rows_step(i, carry):
            base = pl.multiple_of(i * 64, 64)
            values, gates = [], []
            for k, total in correlate(taps, lambda o: gpad[c, pl.ds(base + o, 8), :]):
                total = total.astype(BF16).astype(F32)
                values.append(total * gate_a[c, pl.ds(base + 8 * k, 8), :])
                gates.append(total * gate_b[c, pl.ds(base + 8 * k, 8), :])
                if k % 2:
                    rows = pl.ds(base + 8 * k - 8, 16)
                    gv_s[rows, lanes] = jnp.concatenate(values, axis=0).astype(BF16)
                    gt_s[rows, lanes] = jnp.concatenate(gates, axis=0).astype(BF16)
                    values, gates = [], []
            return carry

        return lax.fori_loop(0, TOK // 64, rows_step, carry)

    stores = []

    def grad_group(at):
        lax.fori_loop(4 * at, 4 * at + 4, grad_chunk, 0)
        lanes = pl.ds(512 * at, 512)
        for narrow, wide in ((gv_s, gv_hbm), (gt_s, gt_hbm)):
            copy = pltpu.make_async_copy(
                narrow.at[:, lanes], wide.at[0, :, lanes], local_sem.at[4 + len(stores)]
            )
            copy.start()
            stores.append(copy)

    rs3(1)
    grad_group(0)
    rs3(2)
    gain_last = gain_pair(gain_z)
    total = tg[sp].astype(F32)
    for copy in part_copies:
        copy.wait_recv()
    for d in range(1, 16):
        total = total + tr[d].astype(F32)
    tz[cz] = total
    tz_copies = [send(tz.at[cz], tz.at[cz], zdev(d)) for d in range(1, NZ)]
    grad_group(1)
    rs3(3)
    grad_group(2)
    gain_copies2 = gain_out(gain_last)
    grad_group(3)
    for copy in started[:200]:
        copy.wait_send()

    for copy in tz_copies:
        copy.wait_recv()
    total = tz[0]
    for k in range(1, NZ):
        total = total + tz[k]
    tfin[...] = total
    pair_copy = send(tfin, tsib, sibling)

    for copy in gather_copies:
        copy.wait_recv()
    for s in range(16):
        y, x = divmod(s, 4)
        for t in range(NS):
            lane = 512 * t + 128 * y
            gw_ref[16 * x : 16 * x + 16, lane : lane + 128] = fg[t, s, 0]
            lane = 512 * t + 128 * x
            gw_ref[64 + 16 * y : 80 + 16 * y, lane : lane + 128] = fg[t, s, 1]
    def store(held, target):
        copy = pltpu.make_async_copy(held, target, local_sem.at[14 + len(stores) - 8])
        copy.start()
        stores.append(copy)

    store(gw_ref, gw_hbm)
    for copy in gain_copies2:
        copy.wait_recv()
    for c in range(NC):
        dn_ref[:, 128 * c : 128 * c + 128] = jnp.sum(gfull[c], axis=0, keepdims=True)
    store(dn_ref, dn_hbm)
    pair_copy.wait_recv()
    dt_ref[...] = (tfin[...] + tsib[...])[:TAPS]
    store(dt_ref, dt_hbm)
    for copy in stores:
        copy.wait()
    for copy in started[200:]:
        copy.wait_send()


def write_out(gv, gt, gw, dt, dn, gv_out, gt_out, gw_out, dt_out, dn_out, gv_s, gt_s, gw_s, gw_wide, dt_s, dn_s, sem):
    copies = []
    for i, (source, held, target) in enumerate(
        ((gw, gw_s, gw_out), (gv, gv_s, gv_out), (gt, gt_s, gt_out), (dt, dt_s, dt_out), (dn, dn_s, dn_out))
    ):
        copy = pltpu.make_async_copy(source, held, sem.at[0, i])
        copy.start()
        copies.append((copy, held, target))
    outs = []
    for i, (copy, held, target) in enumerate(copies):
        copy.wait()
        if i == 0:
            gw_wide[...] = gw_s[...].astype(F32)
            held = gw_wide
        out = pltpu.make_async_copy(held, target, sem.at[1, i])
        out.start()
        outs.append(out)
    for out in outs:
        out.wait()


def body(value_half, gate_half, upstream, conv_taps, norm_gain, out_weight):
    hbm = pl.BlockSpec(memory_space=pl.ANY)
    grad_value, grad_gate, grad_rows, taps, gain = pl.pallas_call(
        kernel,
        out_shape=(
            jax.ShapeDtypeStruct((1, TOK, CH), BF16),
            jax.ShapeDtypeStruct((1, TOK, CH), BF16),
            jax.ShapeDtypeStruct((128, CH), BF16),
            jax.ShapeDtypeStruct((TAPS, 128), F32),
            jax.ShapeDtypeStruct((1, CH), F32),
        ),
        in_specs=[hbm] * 6,
        out_specs=[hbm] * 5,
        scratch_shapes=[
            pltpu.VMEM((1, CH), F32),
            pltpu.VMEM((128, CH), BF16),
            pltpu.VMEM((TAPS, 128), F32),
            pltpu.VMEM((1, CH), F32),
            pltpu.VMEM((TOK, CH), BF16),
            pltpu.VMEM((TOK, CH), BF16),
            pltpu.VMEM((TOK, CH), BF16),
            pltpu.VMEM((TOK, CH), BF16),
            pltpu.VMEM((NZ, 2, 128, CH), BF16),
            pltpu.VMEM((NC, 32, 128), F32),
            pltpu.VMEM((NC, TOK + 32, 128), F32),
            pltpu.VMEM((NC, TOK, 128), F32),
            pltpu.VMEM((TOK, CH), BF16),
            pltpu.VMEM((TOK, CH), BF16),
            pltpu.VMEM((NZ, 128, 512), BF16),
            pltpu.VMEM((NS, 2, 4, NZ, 16, 512), BF16),
            pltpu.VMEM((NS, 2, 2, NZ, 16, 256), BF16),
            pltpu.VMEM((NS, 2, 2, NZ, 16, 512), BF16),
            pltpu.VMEM((NS, 2, 4, NZ, 16, 128), BF16),
            pltpu.VMEM((NS, 2, 2, 4, 16, 128), BF16),
            pltpu.VMEM((NS, 2, 2, NZ, 16, 128), BF16),
            pltpu.VMEM((NS, NZ, 2, 16, 128), BF16),
            pltpu.VMEM((NS, NZ, 2, 16, 128), BF16),
            pltpu.VMEM((NS, 16, 2, 16, 128), BF16),
            pltpu.VMEM((TOK, CH), F32),
            pltpu.VMEM((NC, TOK + 32, 128), F32),
            pltpu.VMEM((TOK, 128), F32),
            pltpu.VMEM((TOK, 128), F32),
            pltpu.VMEM((NC, TOK, 128), F32),
            pltpu.VMEM((NC, TOK, 128), F32),
            pltpu.VMEM((TOK, CH), BF16),
            pltpu.VMEM((TOK, CH), BF16),
            pltpu.VMEM((32, CH), BF16),
            pltpu.VMEM((32, CH), BF16),
            pltpu.VMEM((32, CH), BF16),
            pltpu.VMEM((32, CH), BF16),
            pltpu.VMEM((NC, 8, 128), F32),
            pltpu.VMEM((NC, 32, 128), BF16),
            pltpu.VMEM((16, 32, 128), BF16),
            pltpu.VMEM((NZ, 32, 128), F32),
            pltpu.VMEM((32, 128), F32),
            pltpu.VMEM((32, 128), F32),
            pltpu.VMEM((16, 8, 128), F32),
            pltpu.VMEM((16, 8, 128), F32),
            pltpu.VMEM((NZ, 8, 128), F32),
            pltpu.VMEM((8, 128), F32),
            pltpu.VMEM((8, 128), F32),
            pltpu.SemaphoreType.DMA((17,)),
            pltpu.SemaphoreType.DMA((N_SEND,)),
            pltpu.SemaphoreType.DMA((N_SEND,)),
        ],
        compiler_params=pltpu.CompilerParams(
            collective_id=0, has_side_effects=True, vmem_limit_bytes=66_000_000
        ),
    )(value_half, gate_half, upstream, out_weight, conv_taps, norm_gain[None])
    grad_value, grad_gate, grad_rows, taps, gain = pl.pallas_call(
        write_out,
        out_shape=(
            jax.ShapeDtypeStruct((1, TOK, CH), BF16),
            jax.ShapeDtypeStruct((1, TOK, CH), BF16),
            jax.ShapeDtypeStruct((128, CH), F32),
            jax.ShapeDtypeStruct((TAPS, 128), F32),
            jax.ShapeDtypeStruct((1, CH), F32),
        ),
        in_specs=[hbm] * 5,
        out_specs=[hbm] * 5,
        scratch_shapes=[
            pltpu.VMEM((1, TOK, CH), BF16),
            pltpu.VMEM((1, TOK, CH), BF16),
            pltpu.VMEM((128, CH), BF16),
            pltpu.VMEM((128, CH), F32),
            pltpu.VMEM((TAPS, 128), F32),
            pltpu.VMEM((1, CH), F32),
            pltpu.SemaphoreType.DMA((2, 5)),
        ],
        compiler_params=pltpu.CompilerParams(vmem_limit_bytes=60_000_000),
    )(grad_value, grad_gate, grad_rows, taps, gain)
    return grad_value, grad_gate, taps, gain.reshape(CH), grad_rows


def solution(mesh):
    torus = Mesh(mesh.devices.reshape(4, 4, 8, 2), ("sp_0", "sp_1", "dp_0", "dp_1"))
    placed = (P(DP, SP, None), P(DP, SP, None), P(DP, SP, None), P(None, SP), P(), P(DP, None))
    return jax.shard_map(
        body,
        mesh=torus,
        in_specs=placed,
        out_specs=(P(DP, SP, None), P(DP, SP, None), P(None, SP), P(), P(DP, None)),
        check_vma=False,
    )
```

```python
import functools

import jax
import jax.numpy as jnp
from jax import lax
from jax.experimental import pallas as pl
from jax.experimental.pallas import tpu as pltpu
from jax.sharding import Mesh
from jax.sharding import PartitionSpec as P

DP = ("dp_0", "dp_1")
SP = ("sp_0", "sp_1")
NORM_EPS = 1e-05
MESH = pl.DeviceIdType.MESH
F32 = jnp.float32
BF16 = jnp.bfloat16

TOK = 256
CH = 2048
NC = CH // 128
TAPS = 31
ROW_ORDER = (0, 1, 3, 2)
NZ = 8
NS = 4
N_SEND = 320


def kernel(
    v_hbm, g_hbm, u_hbm, w_hbm, taps_hbm, gain_hbm,
    gv_hbm, gt_hbm, gw_hbm, dt_hbm, dn_hbm,
    gain_ref, gw_ref, dt_ref, dn_ref,
    v_s, g_s, u_s, usib, wbuf, tapsb, glu, conv, act, actsib, ut,
    pbuf, r1, r2, q, s1, s2, vz, rz, fg, gacc, gpad, mean_s, inv_s, gate_a, gate_b, gv_s, gt_s,
    halo_out, halo_in, ghalo_out, ghalo_in, dn, tg, tr, tz, tsib, tfin, gfull, dr, dz, dfin, dsib,
    local_sem, send_sem, recv_sem,
):
    cy, cx, cz, cc = (lax.axis_index(a) for a in ("sp_0", "sp_1", "dp_0", "dp_1"))
    sp = cy * 4 + cx
    other = 1 - cc
    sibling = {"dp_1": other}

    def zdev(d):
        return {"dp_0": lax.rem(cz + d + NZ, NZ)}

    def spdev(d):
        s = lax.rem(sp + d + 16, 16)
        return {"sp_0": s // 4, "sp_1": lax.rem(s, 4)}

    used = [0]
    started = []

    def send(src, dst, device):
        i = used[0]
        used[0] += 1
        copy = pltpu.make_async_remote_copy(
            src_ref=src, dst_ref=dst, send_sem=send_sem.at[i], recv_sem=recv_sem.at[i],
            device_id=device, device_id_type=MESH,
        )
        copy.start()
        started.append(copy)
        return copy

    loads = [
        pltpu.make_async_copy(w_hbm, wbuf.at[0, cc], local_sem.at[0]),
        pltpu.make_async_copy(v_hbm.at[0], v_s, local_sem.at[1]),
        pltpu.make_async_copy(g_hbm.at[0], g_s, local_sem.at[2]),
        pltpu.make_async_copy(u_hbm.at[0], u_s, local_sem.at[3]),
        pltpu.make_async_copy(taps_hbm, tapsb.at[sp, pl.ds(0, TAPS)], local_sem.at[4]),
        pltpu.make_async_copy(gain_hbm, gain_ref, local_sem.at[5]),
    ]
    for at in (1, 2, 4, 5, 0, 3):
        loads[at].start()

    barrier = pltpu.get_barrier_semaphore()
    pl.semaphore_signal(barrier, inc=1, device_id=sibling, device_id_type=MESH)
    for d in range(1, NZ):
        pl.semaphore_signal(barrier, inc=1, device_id=zdev(d), device_id_type=MESH)
    for d in range(1, 16):
        pl.semaphore_signal(barrier, inc=1, device_id=spdev(d), device_id_type=MESH)

    for load in loads[1:3]:
        load.wait()
    def glu_rows(r):
        rows = pl.ds(r, 32)
        for c in range(NC):
            lanes = slice(128 * c, 128 * c + 128)
            value = v_s[rows, lanes].astype(F32)
            sig = jax.nn.sigmoid(g_s[rows, lanes].astype(F32))
            wide = value * sig
            gate_a[c, rows, :] = sig
            gate_b[c, rows, :] = wide * (1.0 - sig)
            narrow = wide.astype(BF16)
            glu[c, pl.ds(r + 32, 32), :] = narrow.astype(F32)
            yield lanes, narrow

    for lanes, narrow in glu_rows(TOK - 32):
        halo_out[:, lanes] = narrow

    def glu_step(i, carry):
        for _ in glu_rows(pl.multiple_of(i * 32, 32)):
            pass
        return carry

    lax.fori_loop(0, TOK // 32 - 1, glu_step, 0)

    for load in loads[3:]:
        load.wait()
    tapsb[sp, TAPS:] = jnp.zeros((1, 128), F32)
    loads[0].wait()
    pl.semaphore_wait(barrier, 23)

    parity = lax.rem(cy + cx, 2)
    w_copies = {}
    w_quarters = {}
    w_pair = {}

    def arrived(copies, key):
        copy = copies.pop(key, None)
        if copy is not None:
            copy.wait_recv()

    def w_send(half, step, sub):
        at = parity if half == 0 else 1 - parity
        rows = pl.ds(pl.multiple_of(64 * at + 32 * sub, 32), 32)
        lanes = (slice(0, 1024), slice(1024, 2048)) if step == 4 else (slice(None), slice(None))
        for way, sign in ((0, 1), (1, -1)):
            src = (-sign * (step - 1)) % NZ
            dst = (-sign * step) % NZ
            w_copies[half, step, sub, way] = send(
                wbuf.at[src, cc, rows, lanes[way]], wbuf.at[dst, cc, rows, lanes[way]], zdev(sign)
            )

    def w_share(rels, half, sub):
        at = parity if half == 0 else 1 - parity
        rows = pl.ds(pl.multiple_of(64 * at + 32 * sub, 32), 32)
        for rel in rels:
            w_pair.setdefault(rel, []).append(send(wbuf.at[rel, cc, rows], wbuf.at[rel, cc, rows], sibling))

    def blocks_at(step):
        return sorted({step, NZ - step})

    def w_event(step, sub):
        for way in (0, 1):
            arrived(w_copies, (0, step, sub, way))
        if step < 4:
            w_send(0, step + 1, sub)
        name, at = (("sp_1", cx), ("sp_0", cy))[sub]
        if step < 3:
            for rel in (step, NZ - step):
                for turn, sign in ((2 * sub, 1), (2 * sub + 1, -1)):
                    rows = pl.ds(pl.multiple_of(64 * parity + 16 * turn, 16), 16)
                    w_quarters[rel, turn] = send(
                        wbuf.at[rel, cc, rows], wbuf.at[rel, cc, rows], {name: lax.rem(at + sign + 4, 4)}
                    )
        w_share(blocks_at(step), 0, sub)

    def w_rest(step, sub):
        if step < 3:
            for rel in blocks_at(step):
                for turn in (2 * sub, 2 * sub + 1):
                    arrived(w_quarters, (rel, turn))
        else:
            for way in (0, 1):
                arrived(w_copies, (1, step, sub, way))
        if step in (2, 3):
            w_send(1, step + 1, sub)
        w_share(blocks_at(step), 1, sub)

    taps_copies = {
        dy: [
            send(tapsb.at[sp], tapsb.at[sp], {"sp_0": lax.rem(cy + dy, 4), "sp_1": lax.rem(cx + dx, 4)})
            for dx in range(4)
            if dx or dy
        ]
        for dy in ROW_ORDER
    }
    w_send(0, 1, 0)
    w_send(0, 1, 1)
    halo_copy = send(halo_out, halo_in, spdev(1))
    u_copy = send(u_s, usib, sibling)
    w_pair[0] = [send(wbuf.at[0, cc], wbuf.at[0, cc], sibling)]

    u_copy.wait_recv()

    def transpose_step(k, carry):
        zb = lax.rem(cz + k, NZ)
        cols = pl.ds(pl.multiple_of(zb * 256 + cc * 128, 128), 128)
        ut[k, :, 0:256] = u_s[:, cols].T
        ut[k, :, 256:512] = usib[:, cols].T
        return carry

    lax.fori_loop(0, NZ, transpose_step, 0)

    def correlate(taps, read):
        sums = {}
        for o in range(8 * 7 + TAPS):
            x = read(o)
            for k in range(8):
                j = o - 8 * k
                if 0 <= j < TAPS:
                    term = taps[j] * x
                    key = k, j % 2
                    sums[key] = sums[key] + term if key in sums else term
                    if j == TAPS - 1:
                        yield k, sums.pop((k, 0)) + sums.pop((k, 1))

    mean_s[...] = jnp.zeros_like(mean_s)

    def conv_chunk(first, last, c, carry):
        taps = [jnp.broadcast_to(tapsb[c, j : j + 1, :], (8, 128)) for j in range(TAPS)]

        def rows_step(i, carry):
            base = pl.multiple_of(i * 64, 64)
            for k, total in correlate(taps, lambda o: glu[c, pl.ds(base + 2 + o, 8), :]):
                total = total.astype(BF16).astype(F32)
                conv[c, pl.ds(base + 8 * k, 8), :] = total
                mean_s[pl.ds(base + 8 * k, 8), :] += total
            return carry

        return lax.fori_loop(first, last, rows_step, carry)

    body_rows = functools.partial(conv_chunk, 1, TOK // 64)

    def conv_group(dy):
        for copy in taps_copies[dy]:
            copy.wait_recv()
        row = lax.rem(cy - dy + 4, 4)
        lax.fori_loop(4 * row, 4 * row + 4, body_rows, 0)

    conv_group(ROW_ORDER[0])
    w_event(1, 0)
    conv_group(ROW_ORDER[1])
    conv_group(ROW_ORDER[2])
    w_event(1, 1)
    conv_group(ROW_ORDER[3])
    halo_copy.wait_recv()
    keep = (sp > 0).astype(F32)
    for c in range(NC):
        glu[c, 0:32, :] = halo_in[:, 128 * c : 128 * c + 128].astype(F32) * keep
    lax.fori_loop(0, NC, functools.partial(conv_chunk, 0, 1), 0)

    def norm_step(i, carry):
        rows = pl.ds(pl.multiple_of(i * 32, 32), 32)
        mu = jnp.broadcast_to(jnp.sum(mean_s[rows, :], axis=1, keepdims=True) * (1.0 / CH), (32, 128))
        squares = jnp.zeros((32, 128), F32)
        for c in range(NC):
            centered = conv[c, rows, :] - mu
            squares = squares + centered * centered
        inv = lax.rsqrt(jnp.sum(squares, axis=1, keepdims=True) * (1.0 / CH) + NORM_EPS)
        inv = jnp.broadcast_to(inv, (32, 128))
        mean_s[rows, :] = mu
        inv_s[rows, :] = inv
        for c in range(NC):
            lanes = slice(128 * c, 128 * c + 128)
            scaled = (conv[c, rows, :] - mu) * inv * gain_ref[:, lanes]
            act[rows, lanes] = (scaled * jax.nn.sigmoid(scaled)).astype(BF16)
        return carry

    act_copies = []

    def norm_part(at):
        lax.fori_loop(2 * at, 2 * at + 2, norm_step, 0)
        rows = pl.ds(64 * at, 64)
        act_copies.append(send(act.at[rows], actsib.at[rows], sibling))

    norm_part(0)
    norm_part(1)
    w_event(2, 0)
    norm_part(2)
    norm_part(3)
    axes = ((("sp_1", cx), ("sp_0", cy)), (("sp_0", cy), ("sp_1", cx)))

    def near(axis, d):
        name, at = axis
        return {name: lax.rem(at + d + 4, 4)}

    def part(axis, d):
        return lax.rem(axis[1] + d + 4, 4)

    def partial_sums(stage):
        lanes = slice(512 * stage, 512 * stage + 512)
        for k in range(NZ):
            lhs = ut[k]
            total = jnp.dot(lhs[:, 0:256], act[:, lanes], preferred_element_type=F32)
            total = total + jnp.dot(lhs[:, 256:512], actsib[:, lanes], preferred_element_type=F32)
            narrow = total.astype(BF16)
            for h in range(2):
                for p in range(4):
                    first = 64 * h + 16 * p
                    pbuf[stage, h, p, k] = narrow[first : first + 16, :]

    rs_copies = {}

    def rs1_send(stage):
        for h in range(2):
            axis = axes[h][0]
            far = part(axis, 2)
            for way, sign, lanes in ((0, 1, slice(0, 256)), (1, -1, slice(256, 512))):
                rs_copies[1, stage, h, way] = send(
                    pbuf.at[stage, h, far, :, :, lanes], r1.at[stage, h, way], near(axis, sign)
                )

    def rs1_mid(stage):
        for h in range(2):
            axis = axes[h][0]
            for way, sign, lanes in ((0, 1, slice(0, 256)), (1, -1, slice(256, 512))):
                rs_copies[1, stage, h, way].wait_recv()
                to = part(axis, sign)

                def add(k, carry, h=h, to=to, way=way, lanes=lanes):
                    pbuf[stage, h, to, k, :, lanes] = (
                        pbuf[stage, h, to, k, :, lanes].astype(F32) + r1[stage, h, way, k].astype(F32)
                    ).astype(BF16)
                    return carry

                lax.fori_loop(0, NZ, add, 0)
                rs_copies[2, stage, h, way] = send(
                    pbuf.at[stage, h, to], r2.at[stage, h, way], near(axis, sign)
                )

    def rs1_fin(stage):
        for h in range(2):
            mine = part(axes[h][0], 0)
            axis = axes[h][1]
            for way in (0, 1):
                rs_copies[2, stage, h, way].wait_recv()

            def add(k, carry, h=h, mine=mine):
                for p in range(4):
                    lanes = slice(128 * p, 128 * p + 128)
                    q[stage, h, p, k] = (
                        pbuf[stage, h, mine, k, :, lanes].astype(F32)
                        + r2[stage, h, 0, k, :, lanes].astype(F32)
                        + r2[stage, h, 1, k, :, lanes].astype(F32)
                    ).astype(BF16)
                return carry

            lax.fori_loop(0, NZ, add, 0)
            far = part(axis, 2)
            for way, sign in ((0, 1), (1, -1)):
                rs_copies[3, stage, h, way] = send(
                    q.at[stage, h, far, pl.ds(4 * way, 4)], s1.at[stage, h, way], near(axis, sign)
                )

    def rs2_mid(stage):
        for h in range(2):
            axis = axes[h][1]
            for way, sign in ((0, 1), (1, -1)):
                rs_copies[3, stage, h, way].wait_recv()
                to = part(axis, sign)
                for k in range(4):
                    q[stage, h, to, 4 * way + k] = (
                        q[stage, h, to, 4 * way + k].astype(F32) + s1[stage, h, way, k].astype(F32)
                    ).astype(BF16)
                rs_copies[4, stage, h, way] = send(
                    q.at[stage, h, to], s2.at[stage, h, way], near(axis, sign)
                )

    z_copies = {}

    def rs2_fin(stage):
        for h in range(2):
            mine = part(axes[h][1], 0)
            for way in (0, 1):
                rs_copies[4, stage, h, way].wait_recv()
            for k in range(NZ):
                vz[stage, k, h] = (
                    q[stage, h, mine, k].astype(F32)
                    + s2[stage, h, 0, k].astype(F32)
                    + s2[stage, h, 1, k].astype(F32)
                ).astype(BF16)
        for k in (4, 3, 5, 2, 6, 1, 7):
            z_copies[stage, k] = send(vz.at[stage, k], rz.at[stage, k], zdev(k))

    gather_copies = []

    def rs3(stage):
        total = vz[stage, 0].astype(F32)
        for k in range(1, NZ):
            z_copies[stage, k].wait_recv()
            total = total + rz[stage, k].astype(F32)
        fg[stage, sp] = total.astype(BF16)
        for d in range(1, 16):
            gather_copies.append(send(fg.at[stage, sp], fg.at[stage, sp], spdev(d)))

    def grad_block(rels, first=False):
        for rel in rels:
            for copy in w_pair[rel]:
                copy.wait_recv()
        lhs = []
        for rel in rels:
            zb = lax.rem(cz + rel, NZ)
            lhs.append(u_s[:, pl.ds(pl.multiple_of(zb * 256, 256), 256)])

        def step(n, carry):
            lanes = pl.ds(pl.multiple_of(n * 512, 512), 512)
            total = None
            for left, rel in zip(lhs, rels):
                right = wbuf[rel, :, :, lanes].reshape(256, 512)
                term = jnp.dot(left, right, preferred_element_type=F32)
                total = term if total is None else total + term
            if first:
                gacc[:, lanes] = total
            else:
                gacc[:, lanes] += total
            return carry

        lax.fori_loop(0, 4, step, 0)

    grad_block((0,), first=True)
    w_event(2, 1)
    w_rest(1, 0)
    w_rest(1, 1)
    for copy in act_copies:
        copy.wait_recv()
    partial_sums(0)
    rs1_send(0)
    partial_sums(1)
    rs1_send(1)
    w_rest(2, 0)
    partial_sums(2)
    rs1_send(2)
    partial_sums(3)
    rs1_send(3)
    w_event(3, 0)
    w_rest(2, 1)
    rs1_mid(0)
    w_event(3, 1)
    rs1_mid(1)
    grad_block((1, 7))
    w_rest(3, 0)
    grad_block((2, 6))
    w_event(4, 0)
    w_rest(3, 1)
    rs1_fin(0)
    rs1_mid(2)
    w_event(4, 1)
    grad_block((3, 5))
    w_rest(4, 0)
    w_rest(4, 1)
    rs1_fin(1)
    rs1_mid(3)
    rs2_mid(0)
    grad_block((4,))

    dn[...] = jnp.zeros_like(dn)

    def back_rows(r):
        rows = pl.ds(r, 32)
        mu = mean_s[rows, :]
        inv = inv_s[rows, :]
        sum1 = jnp.zeros((32, 128), F32)
        sum2 = jnp.zeros((32, 128), F32)
        for c in range(NC):
            lanes = slice(128 * c, 128 * c + 128)
            gain = gain_ref[:, lanes]
            normed = (conv[c, rows, :] - mu) * inv
            scaled = normed * gain
            sig = jax.nn.sigmoid(scaled)
            grad_scaled = gacc[rows, lanes] * sig * (1.0 + scaled * (1.0 - sig))
            gain_term = grad_scaled * normed
            dn[c] += (gain_term[0:8] + gain_term[8:16]) + (gain_term[16:24] + gain_term[24:32])
            grad_normed = grad_scaled * gain
            gacc[rows, lanes] = grad_normed
            sum1 = sum1 + grad_normed
            sum2 = sum2 + grad_normed * normed
        m1 = jnp.broadcast_to(jnp.sum(sum1, axis=1, keepdims=True) * (1.0 / CH), (32, 128))
        m2 = jnp.broadcast_to(jnp.sum(sum2, axis=1, keepdims=True) * (1.0 / CH), (32, 128))
        for c in range(NC):
            lanes = slice(128 * c, 128 * c + 128)
            normed = (conv[c, rows, :] - mu) * inv
            narrow = (inv * (gacc[rows, lanes] - m1 - normed * m2)).astype(BF16)
            gpad[c, rows, :] = narrow.astype(F32)
            yield lanes, narrow

    for lanes, narrow in back_rows(0):
        ghalo_out[:, lanes] = narrow

    def back_step(i, carry):
        for _ in back_rows(pl.multiple_of(i * 32, 32)):
            pass
        return carry

    lax.fori_loop(1, TOK // 32, back_step, 0)

    def rest_of_plane(d):
        return lax.rem(sp + d, 16)

    gain_copies = [send(dn.at[rest_of_plane(d)], dr.at[d], spdev(d)) for d in range(1, 16)]

    def gain_sum():
        total = dn[sp]
        for d in range(1, 16):
            gain_copies[d - 1].wait_recv()
            total = total + dr[d]
        dz[cz] = total
        return [send(dz.at[cz], dz.at[cz], zdev(d)) for d in range(1, NZ)]

    def gain_pair(copies):
        for copy in copies:
            copy.wait_recv()
        total = dz[0]
        for k in range(1, NZ):
            total = total + dz[k]
        dfin[...] = total
        return send(dfin, dsib, sibling)

    def gain_out(copy):
        copy.wait_recv()
        gfull[sp] = dfin[...] + dsib[...]
        return [send(gfull.at[sp], gfull.at[sp], spdev(d)) for d in range(1, 16)]

    def taps_chunk(c, carry):
        def rows_step(i, sums):
            sums = list(sums)
            base = pl.multiple_of(i * 64, 64)
            g = [gpad[c, pl.ds(base + 8 * k, 8), :] for k in range(8)]
            for o in range(8 * 7 + TAPS):
                x = glu[c, pl.ds(base + 2 + o, 8), :]
                for k in range(8):
                    j = o - 8 * k
                    if 0 <= j < TAPS:
                        sums[j] = sums[j] + g[k] * x
            return tuple(sums)

        sums = lax.fori_loop(0, TOK // 64, rows_step, tuple(jnp.zeros((8, 128), F32) for _ in range(TAPS)))
        rows = [jnp.sum(total, axis=0, keepdims=True) for total in sums] + [jnp.zeros((1, 128), F32)]
        tg[c] = jnp.concatenate(rows, axis=0).astype(BF16)
        return carry

    part_copies = []

    def taps_group(dy):
        row = lax.rem(cy + dy, 4)
        lax.fori_loop(4 * row, 4 * row + 4, taps_chunk, 0)
        for dx in range(4):
            if dx or dy:
                x = lax.rem(cx + dx, 4)
                part_copies.append(
                    send(tg.at[4 * row + x], tr.at[4 * dy + dx], {"sp_0": row, "sp_1": x})
                )

    rs1_fin(2)
    rs2_mid(1)
    rs1_fin(3)
    taps_group(2)
    rs2_fin(0)
    rs2_mid(2)
    taps_group(1)
    rs2_fin(1)
    rs2_mid(3)
    ghalo_copy = send(ghalo_out, ghalo_in, spdev(-1))
    gain_z = gain_sum()
    taps_group(3)
    rs2_fin(2)
    taps_group(0)
    rs2_fin(3)
    rs3(0)

    def grad_chunk(first, last, c, carry):
        taps = [jnp.broadcast_to(tapsb[c, j : j + 1, :], (8, 128)) for j in reversed(range(TAPS))]
        lanes = pl.ds(pl.multiple_of(c * 128, 128), 128)

        def rows_step(i, carry):
            base = pl.multiple_of(i * 64, 64)
            values, gates = [], []
            for k, total in correlate(taps, lambda o: gpad[c, pl.ds(base + o, 8), :]):
                total = total.astype(BF16).astype(F32)
                values.append(total * gate_a[c, pl.ds(base + 8 * k, 8), :])
                gates.append(total * gate_b[c, pl.ds(base + 8 * k, 8), :])
                if k % 2:
                    rows = pl.ds(base + 8 * k - 8, 16)
                    gv_s[rows, lanes] = jnp.concatenate(values, axis=0).astype(BF16)
                    gt_s[rows, lanes] = jnp.concatenate(gates, axis=0).astype(BF16)
                    values, gates = [], []
            return carry

        return lax.fori_loop(first, last, rows_step, carry)

    stores = []

    def store(held, target):
        copy = pltpu.make_async_copy(held, target, local_sem.at[6 + len(stores)])
        copy.start()
        stores.append(copy)

    def grad_group(at):
        lax.fori_loop(4 * at, 4 * at + 4, functools.partial(grad_chunk, 0, TOK // 64 - 1), 0)
        rows, lanes = pl.ds(0, TOK - 64), pl.ds(512 * at, 512)
        store(gv_s.at[rows, lanes], gv_hbm.at[0, rows, lanes])
        store(gt_s.at[rows, lanes], gt_hbm.at[0, rows, lanes])

    def grad_last():
        ghalo_copy.wait_recv()
        keep_g = (sp < 15).astype(F32)
        for c in range(NC):
            gpad[c, TOK:, :] = ghalo_in[:, 128 * c : 128 * c + 128].astype(F32) * keep_g
        lax.fori_loop(0, NC, functools.partial(grad_chunk, TOK // 64 - 1, TOK // 64), 0)
        rows = pl.ds(TOK - 64, 64)
        store(gv_s.at[rows], gv_hbm.at[0, rows])
        store(gt_s.at[rows], gt_hbm.at[0, rows])

    rs3(1)
    grad_group(0)
    gain_last = gain_pair(gain_z)
    rs3(2)
    total = tg[sp].astype(F32)
    for copy in part_copies:
        copy.wait_recv()
    for d in range(1, 16):
        total = total + tr[d].astype(F32)
    tz[cz] = total
    tz_copies = [send(tz.at[cz], tz.at[cz], zdev(d)) for d in range(1, NZ)]
    grad_group(1)
    rs3(3)
    gain_copies2 = gain_out(gain_last)
    grad_group(2)
    grad_group(3)
    grad_last()
    for copy in started[:200]:
        copy.wait_send()

    for copy in tz_copies:
        copy.wait_recv()
    total = tz[0]
    for k in range(1, NZ):
        total = total + tz[k]
    tfin[...] = total
    pair_copy = send(tfin, tsib, sibling)

    for copy in gather_copies:
        copy.wait_recv()
    for s in range(16):
        y, x = divmod(s, 4)
        for t in range(NS):
            lane = 512 * t + 128 * y
            gw_ref[16 * x : 16 * x + 16, lane : lane + 128] = fg[t, s, 0]
            lane = 512 * t + 128 * x
            gw_ref[64 + 16 * y : 80 + 16 * y, lane : lane + 128] = fg[t, s, 1]
    store(gw_ref, gw_hbm)
    for copy in gain_copies2:
        copy.wait_recv()
    for c in range(NC):
        dn_ref[:, 128 * c : 128 * c + 128] = jnp.sum(gfull[c], axis=0, keepdims=True)
    store(dn_ref, dn_hbm)
    pair_copy.wait_recv()
    dt_ref[...] = (tfin[...] + tsib[...])[:TAPS]
    store(dt_ref, dt_hbm)
    for copy in stores:
        copy.wait()
    for copy in started[200:]:
        copy.wait_send()


def write_out(gv, gt, gw, dt, dn, gv_out, gt_out, gw_out, dt_out, dn_out, gv_s, gt_s, gw_s, gw_wide, dt_s, dn_s, sem):
    copies = []
    for i, (source, held, target) in enumerate(
        ((gw, gw_s, gw_out), (gv, gv_s, gv_out), (gt, gt_s, gt_out), (dt, dt_s, dt_out), (dn, dn_s, dn_out))
    ):
        copy = pltpu.make_async_copy(source, held, sem.at[0, i])
        copy.start()
        copies.append((copy, held, target))
    outs = []
    for i, (copy, held, target) in enumerate(copies):
        copy.wait()
        if i == 0:
            gw_wide[...] = gw_s[...].astype(F32)
            held = gw_wide
        out = pltpu.make_async_copy(held, target, sem.at[1, i])
        out.start()
        outs.append(out)
    for out in outs:
        out.wait()


def body(value_half, gate_half, upstream, conv_taps, norm_gain, out_weight):
    hbm = pl.BlockSpec(memory_space=pl.ANY)
    grad_value, grad_gate, grad_rows, taps, gain = pl.pallas_call(
        kernel,
        out_shape=(
            jax.ShapeDtypeStruct((1, TOK, CH), BF16),
            jax.ShapeDtypeStruct((1, TOK, CH), BF16),
            jax.ShapeDtypeStruct((128, CH), BF16),
            jax.ShapeDtypeStruct((TAPS, 128), F32),
            jax.ShapeDtypeStruct((1, CH), F32),
        ),
        in_specs=[hbm] * 6,
        out_specs=[hbm] * 5,
        scratch_shapes=[
            pltpu.VMEM((1, CH), F32),
            pltpu.VMEM((128, CH), BF16),
            pltpu.VMEM((TAPS, 128), F32),
            pltpu.VMEM((1, CH), F32),
            pltpu.VMEM((TOK, CH), BF16),
            pltpu.VMEM((TOK, CH), BF16),
            pltpu.VMEM((TOK, CH), BF16),
            pltpu.VMEM((TOK, CH), BF16),
            pltpu.VMEM((NZ, 2, 128, CH), BF16),
            pltpu.VMEM((NC, 32, 128), F32),
            pltpu.VMEM((NC, TOK + 32, 128), F32),
            pltpu.VMEM((NC, TOK, 128), F32),
            pltpu.VMEM((TOK, CH), BF16),
            pltpu.VMEM((TOK, CH), BF16),
            pltpu.VMEM((NZ, 128, 512), BF16),
            pltpu.VMEM((NS, 2, 4, NZ, 16, 512), BF16),
            pltpu.VMEM((NS, 2, 2, NZ, 16, 256), BF16),
            pltpu.VMEM((NS, 2, 2, NZ, 16, 512), BF16),
            pltpu.VMEM((NS, 2, 4, NZ, 16, 128), BF16),
            pltpu.VMEM((NS, 2, 2, 4, 16, 128), BF16),
            pltpu.VMEM((NS, 2, 2, NZ, 16, 128), BF16),
            pltpu.VMEM((NS, NZ, 2, 16, 128), BF16),
            pltpu.VMEM((NS, NZ, 2, 16, 128), BF16),
            pltpu.VMEM((NS, 16, 2, 16, 128), BF16),
            pltpu.VMEM((TOK, CH), F32),
            pltpu.VMEM((NC, TOK + 32, 128), F32),
            pltpu.VMEM((TOK, 128), F32),
            pltpu.VMEM((TOK, 128), F32),
            pltpu.VMEM((NC, TOK, 128), F32),
            pltpu.VMEM((NC, TOK, 128), F32),
            pltpu.VMEM((TOK, CH), BF16),
            pltpu.VMEM((TOK, CH), BF16),
            pltpu.VMEM((32, CH), BF16),
            pltpu.VMEM((32, CH), BF16),
            pltpu.VMEM((32, CH), BF16),
            pltpu.VMEM((32, CH), BF16),
            pltpu.VMEM((NC, 8, 128), F32),
            pltpu.VMEM((NC, 32, 128), BF16),
            pltpu.VMEM((16, 32, 128), BF16),
            pltpu.VMEM((NZ, 32, 128), F32),
            pltpu.VMEM((32, 128), F32),
            pltpu.VMEM((32, 128), F32),
            pltpu.VMEM((16, 8, 128), F32),
            pltpu.VMEM((16, 8, 128), F32),
            pltpu.VMEM((NZ, 8, 128), F32),
            pltpu.VMEM((8, 128), F32),
            pltpu.VMEM((8, 128), F32),
            pltpu.SemaphoreType.DMA((19,)),
            pltpu.SemaphoreType.DMA((N_SEND,)),
            pltpu.SemaphoreType.DMA((N_SEND,)),
        ],
        compiler_params=pltpu.CompilerParams(
            collective_id=0, has_side_effects=True, vmem_limit_bytes=66_000_000
        ),
    )(value_half, gate_half, upstream, out_weight, conv_taps, norm_gain[None])
    grad_value, grad_gate, grad_rows, taps, gain = pl.pallas_call(
        write_out,
        out_shape=(
            jax.ShapeDtypeStruct((1, TOK, CH), BF16),
            jax.ShapeDtypeStruct((1, TOK, CH), BF16),
            jax.ShapeDtypeStruct((128, CH), F32),
            jax.ShapeDtypeStruct((TAPS, 128), F32),
            jax.ShapeDtypeStruct((1, CH), F32),
        ),
        in_specs=[hbm] * 5,
        out_specs=[hbm] * 5,
        scratch_shapes=[
            pltpu.VMEM((1, TOK, CH), BF16),
            pltpu.VMEM((1, TOK, CH), BF16),
            pltpu.VMEM((128, CH), BF16),
            pltpu.VMEM((128, CH), F32),
            pltpu.VMEM((TAPS, 128), F32),
            pltpu.VMEM((1, CH), F32),
            pltpu.SemaphoreType.DMA((2, 5)),
        ],
        compiler_params=pltpu.CompilerParams(vmem_limit_bytes=60_000_000),
    )(grad_value, grad_gate, grad_rows, taps, gain)
    return grad_value, grad_gate, taps, gain.reshape(CH), grad_rows


def solution(mesh):
    torus = Mesh(mesh.devices.reshape(4, 4, 8, 2), ("sp_0", "sp_1", "dp_0", "dp_1"))
    placed = (P(DP, SP, None), P(DP, SP, None), P(DP, SP, None), P(None, SP), P(), P(DP, None))
    return jax.shard_map(
        body,
        mesh=torus,
        in_specs=placed,
        out_specs=(P(DP, SP, None), P(DP, SP, None), P(None, SP), P(), P(DP, None)),
        check_vma=False,
    )
```

```python
import functools

import jax
import jax.numpy as jnp
from jax import lax
from jax.experimental import pallas as pl
from jax.experimental.pallas import tpu as pltpu
from jax.sharding import Mesh
from jax.sharding import PartitionSpec as P

DP = ("dp_0", "dp_1")
SP = ("sp_0", "sp_1")
NORM_EPS = 1e-05
MESH = pl.DeviceIdType.MESH
F32 = jnp.float32
BF16 = jnp.bfloat16

TOK = 256
CH = 2048
NC = CH // 128
TAPS = 31
ROW_ORDER = (0, 1, 3, 2)
NZ = 8
NS = 4
N_SEND = 320


def kernel(
    v_hbm, g_hbm, u_hbm, w_hbm, taps_hbm, gain_hbm,
    gv_hbm, gt_hbm, gw_hbm, dt_hbm, dn_hbm,
    gain_ref, gw_ref, dt_ref, dn_ref,
    v_s, g_s, u_s, usib, wbuf, tapsb, glu, conv, act, actsib, ut,
    pbuf, r1, r2, q, s1, s2, vz, rz, fg, gacc, gpad, mean_s, inv_s, gate_a, gate_b, gv_s, gt_s,
    halo_out, halo_in, ghalo_out, ghalo_in, dn, tg, tr, tz, tsib, tfin, gfull, dr, dz, dfin, dsib,
    local_sem, send_sem, recv_sem,
):
    cy, cx, cz, cc = (lax.axis_index(a) for a in ("sp_0", "sp_1", "dp_0", "dp_1"))
    sp = cy * 4 + cx
    other = 1 - cc
    sibling = {"dp_1": other}

    def zdev(d):
        return {"dp_0": lax.rem(cz + d + NZ, NZ)}

    def spdev(d):
        s = lax.rem(sp + d + 16, 16)
        return {"sp_0": s // 4, "sp_1": lax.rem(s, 4)}

    used = [0]
    started = []

    def send(src, dst, device):
        i = used[0]
        used[0] += 1
        copy = pltpu.make_async_remote_copy(
            src_ref=src, dst_ref=dst, send_sem=send_sem.at[i], recv_sem=recv_sem.at[i],
            device_id=device, device_id_type=MESH,
        )
        copy.start()
        started.append(copy)
        return copy

    loads = [
        pltpu.make_async_copy(w_hbm, wbuf.at[0, cc], local_sem.at[0]),
        pltpu.make_async_copy(v_hbm.at[0], v_s, local_sem.at[1]),
        pltpu.make_async_copy(g_hbm.at[0], g_s, local_sem.at[2]),
        pltpu.make_async_copy(u_hbm.at[0], u_s, local_sem.at[3]),
        pltpu.make_async_copy(taps_hbm, tapsb.at[sp, pl.ds(0, TAPS)], local_sem.at[4]),
        pltpu.make_async_copy(gain_hbm, gain_ref, local_sem.at[5]),
    ]
    for at in (1, 2, 4, 5, 0, 3):
        loads[at].start()

    barrier = pltpu.get_barrier_semaphore()
    pl.semaphore_signal(barrier, inc=1, device_id=sibling, device_id_type=MESH)
    for d in range(1, NZ):
        pl.semaphore_signal(barrier, inc=1, device_id=zdev(d), device_id_type=MESH)
    for d in range(1, 16):
        pl.semaphore_signal(barrier, inc=1, device_id=spdev(d), device_id_type=MESH)

    for load in loads[1:3]:
        load.wait()
    def glu_rows(r):
        rows = pl.ds(r, 32)
        for c in range(NC):
            lanes = slice(128 * c, 128 * c + 128)
            value = v_s[rows, lanes].astype(F32)
            sig = jax.nn.sigmoid(g_s[rows, lanes].astype(F32))
            wide = value * sig
            gate_a[c, rows, :] = sig
            gate_b[c, rows, :] = wide * (1.0 - sig)
            narrow = wide.astype(BF16)
            glu[c, pl.ds(r + 32, 32), :] = narrow.astype(F32)
            yield lanes, narrow

    for lanes, narrow in glu_rows(TOK - 32):
        halo_out[:, lanes] = narrow

    def glu_step(i, carry):
        for _ in glu_rows(pl.multiple_of(i * 32, 32)):
            pass
        return carry

    lax.fori_loop(0, TOK // 32 - 1, glu_step, 0)

    for load in loads[3:]:
        load.wait()
    tapsb[sp, TAPS:] = jnp.zeros((1, 128), F32)
    loads[0].wait()
    pl.semaphore_wait(barrier, 23)

    parity = lax.rem(cy + cx, 2)
    w_copies = {}
    w_quarters = {}
    w_pair = {}

    def arrived(copies, key):
        copy = copies.pop(key, None)
        if copy is not None:
            copy.wait_recv()

    def w_send(half, step, sub):
        at = parity if half == 0 else 1 - parity
        rows = pl.ds(pl.multiple_of(64 * at + 32 * sub, 32), 32)
        lanes = (slice(0, 1024), slice(1024, 2048)) if step == 4 else (slice(None), slice(None))
        for way, sign in ((0, 1), (1, -1)):
            src = (-sign * (step - 1)) % NZ
            dst = (-sign * step) % NZ
            w_copies[half, step, sub, way] = send(
                wbuf.at[src, cc, rows, lanes[way]], wbuf.at[dst, cc, rows, lanes[way]], zdev(sign)
            )

    def w_share(rels, half, sub):
        at = parity if half == 0 else 1 - parity
        rows = pl.ds(pl.multiple_of(64 * at + 32 * sub, 32), 32)
        for rel in rels:
            w_pair.setdefault(rel, []).append(send(wbuf.at[rel, cc, rows], wbuf.at[rel, cc, rows], sibling))

    def blocks_at(step):
        return sorted({step, NZ - step})

    def w_event(step, sub):
        for way in (0, 1):
            arrived(w_copies, (0, step, sub, way))
        if step < 4:
            w_send(0, step + 1, sub)
        name, at = (("sp_1", cx), ("sp_0", cy))[sub]
        if step < 3:
            for rel in (step, NZ - step):
                for turn, sign in ((2 * sub, 1), (2 * sub + 1, -1)):
                    rows = pl.ds(pl.multiple_of(64 * parity + 16 * turn, 16), 16)
                    w_quarters[rel, turn] = send(
                        wbuf.at[rel, cc, rows], wbuf.at[rel, cc, rows], {name: lax.rem(at + sign + 4, 4)}
                    )
        w_share(blocks_at(step), 0, sub)

    def w_rest(step, sub):
        if step < 3:
            for rel in blocks_at(step):
                for turn in (2 * sub, 2 * sub + 1):
                    arrived(w_quarters, (rel, turn))
        else:
            for way in (0, 1):
                arrived(w_copies, (1, step, sub, way))
        if step in (2, 3):
            w_send(1, step + 1, sub)
        w_share(blocks_at(step), 1, sub)

    taps_copies = {
        dy: [
            send(tapsb.at[sp], tapsb.at[sp], {"sp_0": lax.rem(cy + dy, 4), "sp_1": lax.rem(cx + dx, 4)})
            for dx in range(4)
            if dx or dy
        ]
        for dy in ROW_ORDER
    }
    w_send(0, 1, 0)
    w_send(0, 1, 1)
    halo_copy = send(halo_out, halo_in, spdev(1))
    u_copy = send(u_s, usib, sibling)
    w_pair[0] = [send(wbuf.at[0, cc], wbuf.at[0, cc], sibling)]

    u_copy.wait_recv()

    def transpose_step(k, carry):
        zb = lax.rem(cz + k, NZ)
        cols = pl.ds(pl.multiple_of(zb * 256 + cc * 128, 128), 128)
        ut[k, :, 0:256] = u_s[:, cols].T
        ut[k, :, 256:512] = usib[:, cols].T
        return carry

    lax.fori_loop(0, NZ, transpose_step, 0)

    def correlate(taps, read):
        sums = {}
        for o in range(8 * 7 + TAPS):
            x = read(o)
            for k in range(8):
                j = o - 8 * k
                if 0 <= j < TAPS:
                    term = taps[j] * x
                    key = k, j % 2
                    sums[key] = sums[key] + term if key in sums else term
                    if j == TAPS - 1:
                        yield k, sums.pop((k, 0)) + sums.pop((k, 1))

    mean_s[...] = jnp.zeros_like(mean_s)

    def conv_chunk(first, last, c, carry):
        taps = [jnp.broadcast_to(tapsb[c, j : j + 1, :], (8, 128)) for j in range(TAPS)]

        def rows_step(i, carry):
            base = pl.multiple_of(i * 64, 64)
            for k, total in correlate(taps, lambda o: glu[c, pl.ds(base + 2 + o, 8), :]):
                total = total.astype(BF16).astype(F32)
                conv[c, pl.ds(base + 8 * k, 8), :] = total
                mean_s[pl.ds(base + 8 * k, 8), :] += total
            return carry

        return lax.fori_loop(first, last, rows_step, carry)

    body_rows = functools.partial(conv_chunk, 1, TOK // 64)

    def conv_group(dy):
        for copy in taps_copies[dy]:
            copy.wait_recv()
        row = lax.rem(cy - dy + 4, 4)
        lax.fori_loop(4 * row, 4 * row + 4, body_rows, 0)

    conv_group(ROW_ORDER[0])
    w_event(1, 0)
    conv_group(ROW_ORDER[1])
    conv_group(ROW_ORDER[2])
    w_event(1, 1)
    conv_group(ROW_ORDER[3])
    halo_copy.wait_recv()
    keep = (sp > 0).astype(F32)
    for c in range(NC):
        glu[c, 0:32, :] = halo_in[:, 128 * c : 128 * c + 128].astype(F32) * keep
    lax.fori_loop(0, NC, functools.partial(conv_chunk, 0, 1), 0)

    def norm_step(i, carry):
        rows = pl.ds(pl.multiple_of(i * 32, 32), 32)
        mu = jnp.broadcast_to(jnp.sum(mean_s[rows, :], axis=1, keepdims=True) * (1.0 / CH), (32, 128))
        squares = jnp.zeros((32, 128), F32)
        for c in range(NC):
            centered = conv[c, rows, :] - mu
            squares = squares + centered * centered
        inv = lax.rsqrt(jnp.sum(squares, axis=1, keepdims=True) * (1.0 / CH) + NORM_EPS)
        inv = jnp.broadcast_to(inv, (32, 128))
        mean_s[rows, :] = mu
        inv_s[rows, :] = inv
        for c in range(NC):
            lanes = slice(128 * c, 128 * c + 128)
            scaled = (conv[c, rows, :] - mu) * inv * gain_ref[:, lanes]
            act[rows, lanes] = (scaled * jax.nn.sigmoid(scaled)).astype(BF16)
        return carry

    act_copies = []

    def norm_part(at):
        lax.fori_loop(2 * at, 2 * at + 2, norm_step, 0)
        rows = pl.ds(64 * at, 64)
        act_copies.append(send(act.at[rows], actsib.at[rows], sibling))

    norm_part(0)
    norm_part(1)
    w_event(2, 0)
    norm_part(2)
    norm_part(3)
    axes = ((("sp_1", cx), ("sp_0", cy)), (("sp_0", cy), ("sp_1", cx)))

    def near(axis, d):
        name, at = axis
        return {name: lax.rem(at + d + 4, 4)}

    def part(axis, d):
        return lax.rem(axis[1] + d + 4, 4)

    def partial_sums(stage):
        lanes = slice(512 * stage, 512 * stage + 512)
        for k in range(NZ):
            lhs = ut[k]
            total = jnp.dot(lhs[:, 0:256], act[:, lanes], preferred_element_type=F32)
            total = total + jnp.dot(lhs[:, 256:512], actsib[:, lanes], preferred_element_type=F32)
            narrow = total.astype(BF16)
            for h in range(2):
                for p in range(4):
                    first = 64 * h + 16 * p
                    pbuf[stage, h, p, k] = narrow[first : first + 16, :]

    rs_copies = {}

    def rs1_send(stage):
        for h in range(2):
            axis = axes[h][0]
            far = part(axis, 2)
            for way, sign, lanes in ((0, 1, slice(0, 256)), (1, -1, slice(256, 512))):
                rs_copies[1, stage, h, way] = send(
                    pbuf.at[stage, h, far, :, :, lanes], r1.at[stage, h, way], near(axis, sign)
                )

    def rs1_mid(stage):
        for h in range(2):
            axis = axes[h][0]
            for way, sign, lanes in ((0, 1, slice(0, 256)), (1, -1, slice(256, 512))):
                rs_copies[1, stage, h, way].wait_recv()
                to = part(axis, sign)

                def add(k, carry, h=h, to=to, way=way, lanes=lanes):
                    pbuf[stage, h, to, k, :, lanes] = (
                        pbuf[stage, h, to, k, :, lanes].astype(F32) + r1[stage, h, way, k].astype(F32)
                    ).astype(BF16)
                    return carry

                lax.fori_loop(0, NZ, add, 0)
                rs_copies[2, stage, h, way] = send(
                    pbuf.at[stage, h, to], r2.at[stage, h, way], near(axis, sign)
                )

    def rs1_fin(stage):
        for h in range(2):
            mine = part(axes[h][0], 0)
            axis = axes[h][1]
            for way in (0, 1):
                rs_copies[2, stage, h, way].wait_recv()

            def add(k, carry, h=h, mine=mine):
                for p in range(4):
                    lanes = slice(128 * p, 128 * p + 128)
                    q[stage, h, p, k] = (
                        pbuf[stage, h, mine, k, :, lanes].astype(F32)
                        + r2[stage, h, 0, k, :, lanes].astype(F32)
                        + r2[stage, h, 1, k, :, lanes].astype(F32)
                    ).astype(BF16)
                return carry

            lax.fori_loop(0, NZ, add, 0)
            far = part(axis, 2)
            for way, sign in ((0, 1), (1, -1)):
                rs_copies[3, stage, h, way] = send(
                    q.at[stage, h, far, pl.ds(4 * way, 4)], s1.at[stage, h, way], near(axis, sign)
                )

    def rs2_mid(stage):
        for h in range(2):
            axis = axes[h][1]
            for way, sign in ((0, 1), (1, -1)):
                rs_copies[3, stage, h, way].wait_recv()
                to = part(axis, sign)
                for k in range(4):
                    q[stage, h, to, 4 * way + k] = (
                        q[stage, h, to, 4 * way + k].astype(F32) + s1[stage, h, way, k].astype(F32)
                    ).astype(BF16)
                rs_copies[4, stage, h, way] = send(
                    q.at[stage, h, to], s2.at[stage, h, way], near(axis, sign)
                )

    z_copies = {}

    def rs2_fin(stage):
        for h in range(2):
            mine = part(axes[h][1], 0)
            for way in (0, 1):
                rs_copies[4, stage, h, way].wait_recv()
            for k in range(NZ):
                vz[stage, k, h] = (
                    q[stage, h, mine, k].astype(F32)
                    + s2[stage, h, 0, k].astype(F32)
                    + s2[stage, h, 1, k].astype(F32)
                ).astype(BF16)
        for k in (4, 3, 5, 2, 6, 1, 7):
            z_copies[stage, k] = send(vz.at[stage, k], rz.at[stage, k], zdev(k))

    gather_copies = []

    def rs3(stage):
        total = vz[stage, 0].astype(F32)
        for k in range(1, NZ):
            z_copies[stage, k].wait_recv()
            total = total + rz[stage, k].astype(F32)
        fg[stage, sp] = total.astype(BF16)
        for d in range(1, 16):
            gather_copies.append(send(fg.at[stage, sp], fg.at[stage, sp], spdev(d)))

    def grad_block(rels, first=False):
        for rel in rels:
            for copy in w_pair[rel]:
                copy.wait_recv()
        lhs = []
        for rel in rels:
            zb = lax.rem(cz + rel, NZ)
            lhs.append(u_s[:, pl.ds(pl.multiple_of(zb * 256, 256), 256)])

        def step(n, carry):
            lanes = pl.ds(pl.multiple_of(n * 512, 512), 512)
            total = None
            for left, rel in zip(lhs, rels):
                right = wbuf[rel, :, :, lanes].reshape(256, 512)
                term = jnp.dot(left, right, preferred_element_type=F32)
                total = term if total is None else total + term
            if first:
                gacc[:, lanes] = total
            else:
                gacc[:, lanes] += total
            return carry

        lax.fori_loop(0, 4, step, 0)

    grad_block((0,), first=True)
    w_event(2, 1)
    w_rest(1, 0)
    w_rest(1, 1)
    for copy in act_copies:
        copy.wait_recv()
    partial_sums(0)
    rs1_send(0)
    partial_sums(1)
    rs1_send(1)
    w_rest(2, 0)
    partial_sums(2)
    rs1_send(2)
    partial_sums(3)
    rs1_send(3)
    w_event(3, 0)
    w_rest(2, 1)
    rs1_mid(0)
    w_event(3, 1)
    rs1_mid(1)
    grad_block((1, 7))
    w_rest(3, 0)
    grad_block((2, 6))
    w_event(4, 0)
    w_rest(3, 1)
    rs1_fin(0)
    rs1_mid(2)
    w_event(4, 1)
    grad_block((3, 5))
    w_rest(4, 0)
    w_rest(4, 1)
    rs1_fin(1)
    rs1_mid(3)
    rs2_mid(0)
    grad_block((4,))

    dn[...] = jnp.zeros_like(dn)

    def back_rows(r):
        rows = pl.ds(r, 32)
        mu = mean_s[rows, :]
        inv = inv_s[rows, :]
        sum1 = jnp.zeros((32, 128), F32)
        sum2 = jnp.zeros((32, 128), F32)
        for c in range(NC):
            lanes = slice(128 * c, 128 * c + 128)
            gain = gain_ref[:, lanes]
            normed = (conv[c, rows, :] - mu) * inv
            scaled = normed * gain
            sig = jax.nn.sigmoid(scaled)
            grad_scaled = gacc[rows, lanes] * sig * (1.0 + scaled * (1.0 - sig))
            gain_term = grad_scaled * normed
            dn[c] += (gain_term[0:8] + gain_term[8:16]) + (gain_term[16:24] + gain_term[24:32])
            grad_normed = grad_scaled * gain
            gacc[rows, lanes] = grad_normed
            sum1 = sum1 + grad_normed
            sum2 = sum2 + grad_normed * normed
        m1 = jnp.broadcast_to(jnp.sum(sum1, axis=1, keepdims=True) * (1.0 / CH), (32, 128))
        m2 = jnp.broadcast_to(jnp.sum(sum2, axis=1, keepdims=True) * (1.0 / CH), (32, 128))
        for c in range(NC):
            lanes = slice(128 * c, 128 * c + 128)
            normed = (conv[c, rows, :] - mu) * inv
            narrow = (inv * (gacc[rows, lanes] - m1 - normed * m2)).astype(BF16)
            gpad[c, rows, :] = narrow.astype(F32)
            yield lanes, narrow

    for lanes, narrow in back_rows(0):
        ghalo_out[:, lanes] = narrow

    def back_step(i, carry):
        for _ in back_rows(pl.multiple_of(i * 32, 32)):
            pass
        return carry

    lax.fori_loop(1, TOK // 32, back_step, 0)

    def rest_of_plane(d):
        return lax.rem(sp + d, 16)

    gain_copies = [send(dn.at[rest_of_plane(d)], dr.at[d], spdev(d)) for d in range(1, 16)]

    def gain_sum():
        total = dn[sp]
        for d in range(1, 16):
            gain_copies[d - 1].wait_recv()
            total = total + dr[d]
        dz[cz] = total
        return [send(dz.at[cz], dz.at[cz], zdev(d)) for d in range(1, NZ)]

    def gain_pair(copies):
        for copy in copies:
            copy.wait_recv()
        total = dz[0]
        for k in range(1, NZ):
            total = total + dz[k]
        dfin[...] = total
        return send(dfin, dsib, sibling)

    def gain_out(copy):
        copy.wait_recv()
        gfull[sp] = dfin[...] + dsib[...]
        return [send(gfull.at[sp], gfull.at[sp], spdev(d)) for d in range(1, 16)]

    def taps_chunk(c, carry):
        def rows_step(i, sums):
            sums = list(sums)
            base = pl.multiple_of(i * 64, 64)
            g = [gpad[c, pl.ds(base + 8 * k, 8), :] for k in range(8)]
            for o in range(8 * 7 + TAPS):
                x = glu[c, pl.ds(base + 2 + o, 8), :]
                for k in range(8):
                    j = o - 8 * k
                    if 0 <= j < TAPS:
                        sums[j] = sums[j] + g[k] * x
            return tuple(sums)

        sums = lax.fori_loop(0, TOK // 64, rows_step, tuple(jnp.zeros((8, 128), F32) for _ in range(TAPS)))
        rows = [jnp.sum(total, axis=0, keepdims=True) for total in sums] + [jnp.zeros((1, 128), F32)]
        tg[c] = jnp.concatenate(rows, axis=0).astype(BF16)
        return carry

    part_copies = []

    def taps_group(dy):
        row = lax.rem(cy + dy, 4)
        lax.fori_loop(4 * row, 4 * row + 4, taps_chunk, 0)
        for dx in range(4):
            if dx or dy:
                x = lax.rem(cx + dx, 4)
                part_copies.append(
                    send(tg.at[4 * row + x], tr.at[4 * dy + dx], {"sp_0": row, "sp_1": x})
                )

    rs1_fin(2)
    rs2_mid(1)
    rs1_fin(3)
    taps_group(2)
    rs2_fin(0)
    rs2_mid(2)
    taps_group(1)
    rs2_fin(1)
    rs2_mid(3)
    ghalo_copy = send(ghalo_out, ghalo_in, spdev(-1))
    gain_z = gain_sum()
    taps_group(3)
    rs2_fin(2)
    taps_group(0)
    rs2_fin(3)
    rs3(0)

    def grad_chunk(first, last, c, carry):
        taps = [jnp.broadcast_to(tapsb[c, j : j + 1, :], (8, 128)) for j in reversed(range(TAPS))]
        lanes = pl.ds(pl.multiple_of(c * 128, 128), 128)

        def rows_step(i, carry):
            base = pl.multiple_of(i * 64, 64)
            values, gates = [], []
            for k, total in correlate(taps, lambda o: gpad[c, pl.ds(base + o, 8), :]):
                total = total.astype(BF16).astype(F32)
                values.append(total * gate_a[c, pl.ds(base + 8 * k, 8), :])
                gates.append(total * gate_b[c, pl.ds(base + 8 * k, 8), :])
                if k % 2:
                    rows = pl.ds(base + 8 * k - 8, 16)
                    gv_s[rows, lanes] = jnp.concatenate(values, axis=0).astype(BF16)
                    gt_s[rows, lanes] = jnp.concatenate(gates, axis=0).astype(BF16)
                    values, gates = [], []
            return carry

        return lax.fori_loop(first, last, rows_step, carry)

    stores = []

    def store(held, target):
        copy = pltpu.make_async_copy(held, target, local_sem.at[6 + len(stores)])
        copy.start()
        stores.append(copy)

    def grad_group(at):
        lax.fori_loop(4 * at, 4 * at + 4, functools.partial(grad_chunk, 0, TOK // 64 - 1), 0)
        rows, lanes = pl.ds(0, TOK - 64), pl.ds(512 * at, 512)
        store(gv_s.at[rows, lanes], gv_hbm.at[0, rows, lanes])
        store(gt_s.at[rows, lanes], gt_hbm.at[0, rows, lanes])

    def grad_last():
        ghalo_copy.wait_recv()
        keep_g = (sp < 15).astype(F32)
        for c in range(NC):
            gpad[c, TOK:, :] = ghalo_in[:, 128 * c : 128 * c + 128].astype(F32) * keep_g
        lax.fori_loop(0, NC, functools.partial(grad_chunk, TOK // 64 - 1, TOK // 64), 0)
        rows = pl.ds(TOK - 64, 64)
        store(gv_s.at[rows], gv_hbm.at[0, rows])
        store(gt_s.at[rows], gt_hbm.at[0, rows])

    rs3(1)
    grad_group(0)
    gain_last = gain_pair(gain_z)
    rs3(2)
    total = tg[sp].astype(F32)
    for copy in part_copies:
        copy.wait_recv()
    for d in range(1, 16):
        total = total + tr[d].astype(F32)
    tz[cz] = total
    tz_copies = [send(tz.at[cz], tz.at[cz], zdev(d)) for d in range(1, NZ)]
    grad_group(1)
    rs3(3)
    gain_copies2 = gain_out(gain_last)
    grad_group(2)
    grad_group(3)
    grad_last()
    for copy in started[:200]:
        copy.wait_send()

    for copy in tz_copies:
        copy.wait_recv()
    total = tz[0]
    for k in range(1, NZ):
        total = total + tz[k]
    tfin[...] = total
    pair_copy = send(tfin, tsib, sibling)

    for copy in gather_copies:
        copy.wait_recv()
    for s in range(16):
        y, x = divmod(s, 4)
        for t in range(NS):
            lane = 512 * t + 128 * y
            gw_ref[16 * x : 16 * x + 16, lane : lane + 128] = fg[t, s, 0]
            lane = 512 * t + 128 * x
            gw_ref[64 + 16 * y : 80 + 16 * y, lane : lane + 128] = fg[t, s, 1]
    store(gw_ref, gw_hbm)
    for copy in gain_copies2:
        copy.wait_recv()
    for c in range(NC):
        dn_ref[:, 128 * c : 128 * c + 128] = jnp.sum(gfull[c], axis=0, keepdims=True)
    store(dn_ref, dn_hbm)
    pair_copy.wait_recv()
    dt_ref[...] = (tfin[...] + tsib[...])[:TAPS]
    store(dt_ref, dt_hbm)
    for copy in stores:
        copy.wait()
    for copy in started[200:]:
        copy.wait_send()


def write_out(gv, gt, gw, dt, dn, gv_out, gt_out, gw_out, dt_out, dn_out, gv_s, gt_s, gw_s, gw_wide, dt_s, dn_s, sem):
    copies = []
    for i, (source, held, target) in enumerate(
        [(gw, gw_s, gw_out)]
        + [
            tuple(ref.at[:, pl.ds(128 * half, 128)] for ref in refs)
            for refs in ((gv, gv_s, gv_out), (gt, gt_s, gt_out))
            for half in range(2)
        ]
        + [(dt, dt_s, dt_out), (dn, dn_s, dn_out)]
    ):
        copy = pltpu.make_async_copy(source, held, sem.at[0, i])
        copy.start()
        copies.append((copy, held, target))
    outs = []
    for i, (copy, held, target) in enumerate(copies):
        copy.wait()
        if i == 0:
            gw_wide[...] = gw_s[...].astype(F32)
            held = gw_wide
        out = pltpu.make_async_copy(held, target, sem.at[1, i])
        out.start()
        outs.append(out)
    for out in outs:
        out.wait()


def body(value_half, gate_half, upstream, conv_taps, norm_gain, out_weight):
    hbm = pl.BlockSpec(memory_space=pl.ANY)
    grad_value, grad_gate, grad_rows, taps, gain = pl.pallas_call(
        kernel,
        out_shape=(
            jax.ShapeDtypeStruct((1, TOK, CH), BF16),
            jax.ShapeDtypeStruct((1, TOK, CH), BF16),
            jax.ShapeDtypeStruct((128, CH), BF16),
            jax.ShapeDtypeStruct((TAPS, 128), F32),
            jax.ShapeDtypeStruct((1, CH), F32),
        ),
        in_specs=[hbm] * 6,
        out_specs=[hbm] * 5,
        scratch_shapes=[
            pltpu.VMEM((1, CH), F32),
            pltpu.VMEM((128, CH), BF16),
            pltpu.VMEM((TAPS, 128), F32),
            pltpu.VMEM((1, CH), F32),
            pltpu.VMEM((TOK, CH), BF16),
            pltpu.VMEM((TOK, CH), BF16),
            pltpu.VMEM((TOK, CH), BF16),
            pltpu.VMEM((TOK, CH), BF16),
            pltpu.VMEM((NZ, 2, 128, CH), BF16),
            pltpu.VMEM((NC, 32, 128), F32),
            pltpu.VMEM((NC, TOK + 32, 128), F32),
            pltpu.VMEM((NC, TOK, 128), F32),
            pltpu.VMEM((TOK, CH), BF16),
            pltpu.VMEM((TOK, CH), BF16),
            pltpu.VMEM((NZ, 128, 512), BF16),
            pltpu.VMEM((NS, 2, 4, NZ, 16, 512), BF16),
            pltpu.VMEM((NS, 2, 2, NZ, 16, 256), BF16),
            pltpu.VMEM((NS, 2, 2, NZ, 16, 512), BF16),
            pltpu.VMEM((NS, 2, 4, NZ, 16, 128), BF16),
            pltpu.VMEM((NS, 2, 2, 4, 16, 128), BF16),
            pltpu.VMEM((NS, 2, 2, NZ, 16, 128), BF16),
            pltpu.VMEM((NS, NZ, 2, 16, 128), BF16),
            pltpu.VMEM((NS, NZ, 2, 16, 128), BF16),
            pltpu.VMEM((NS, 16, 2, 16, 128), BF16),
            pltpu.VMEM((TOK, CH), F32),
            pltpu.VMEM((NC, TOK + 32, 128), F32),
            pltpu.VMEM((TOK, 128), F32),
            pltpu.VMEM((TOK, 128), F32),
            pltpu.VMEM((NC, TOK, 128), F32),
            pltpu.VMEM((NC, TOK, 128), F32),
            pltpu.VMEM((TOK, CH), BF16),
            pltpu.VMEM((TOK, CH), BF16),
            pltpu.VMEM((32, CH), BF16),
            pltpu.VMEM((32, CH), BF16),
            pltpu.VMEM((32, CH), BF16),
            pltpu.VMEM((32, CH), BF16),
            pltpu.VMEM((NC, 8, 128), F32),
            pltpu.VMEM((NC, 32, 128), BF16),
            pltpu.VMEM((16, 32, 128), BF16),
            pltpu.VMEM((NZ, 32, 128), F32),
            pltpu.VMEM((32, 128), F32),
            pltpu.VMEM((32, 128), F32),
            pltpu.VMEM((16, 8, 128), F32),
            pltpu.VMEM((16, 8, 128), F32),
            pltpu.VMEM((NZ, 8, 128), F32),
            pltpu.VMEM((8, 128), F32),
            pltpu.VMEM((8, 128), F32),
            pltpu.SemaphoreType.DMA((19,)),
            pltpu.SemaphoreType.DMA((N_SEND,)),
            pltpu.SemaphoreType.DMA((N_SEND,)),
        ],
        compiler_params=pltpu.CompilerParams(
            collective_id=0, has_side_effects=True, vmem_limit_bytes=66_000_000
        ),
    )(value_half, gate_half, upstream, out_weight, conv_taps, norm_gain[None])
    grad_value, grad_gate, grad_rows, taps, gain = pl.pallas_call(
        write_out,
        out_shape=(
            jax.ShapeDtypeStruct((1, TOK, CH), BF16),
            jax.ShapeDtypeStruct((1, TOK, CH), BF16),
            jax.ShapeDtypeStruct((128, CH), F32),
            jax.ShapeDtypeStruct((TAPS, 128), F32),
            jax.ShapeDtypeStruct((1, CH), F32),
        ),
        in_specs=[hbm] * 5,
        out_specs=[hbm] * 5,
        scratch_shapes=[
            pltpu.VMEM((1, TOK, CH), BF16),
            pltpu.VMEM((1, TOK, CH), BF16),
            pltpu.VMEM((128, CH), BF16),
            pltpu.VMEM((128, CH), F32),
            pltpu.VMEM((TAPS, 128), F32),
            pltpu.VMEM((1, CH), F32),
            pltpu.SemaphoreType.DMA((2, 7)),
        ],
        compiler_params=pltpu.CompilerParams(vmem_limit_bytes=60_000_000),
    )(grad_value, grad_gate, grad_rows, taps, gain)
    return grad_value, grad_gate, taps, gain.reshape(CH), grad_rows


def solution(mesh):
    torus = Mesh(mesh.devices.reshape(4, 4, 8, 2), ("sp_0", "sp_1", "dp_0", "dp_1"))
    placed = (P(DP, SP, None), P(DP, SP, None), P(DP, SP, None), P(None, SP), P(), P(DP, None))
    return jax.shard_map(
        body,
        mesh=torus,
        in_specs=placed,
        out_specs=(P(DP, SP, None), P(DP, SP, None), P(None, SP), P(), P(DP, None)),
        check_vma=False,
    )
```
